32 devices in a mesh: sp: 8 (over z, y), tp: 4 (over x, core).
Axes of the slice: x: 2, y: 2, z: 4, core: 2. Of those that a mesh axis runs over, the one named last changes fastest.
Arguments:
- tokens: bfloat16 [4096, 2048], P(('sp', 'tp')), may hold values from -6 to 6
- norm_gain: float32 [2048], replicated, may hold values from 0.1 to 1.9
- query_weight: bfloat16 [2048, 2048], P('sp', 'tp'), may hold values from -0.125 to 0.125
- key_weight: bfloat16 [2048, 2048], P('sp', 'tp'), may hold values from -0.125 to 0.125
- value_weight: bfloat16 [2048, 4096], P('sp', 'tp'), may hold values from -0.125 to 0.125
- retain_gate: bfloat16 [2048, 4096], P('sp', 'tp'), may hold values from -0.125 to 0.125
- unit_value: bfloat16 [2048, 2048], P('sp', 'tp'), may hold values from -0.125 to 0.125
- unit_gate: bfloat16 [2048, 2048], P('sp', 'tp'), may hold values from -0.125 to 0.125
- convolve_gate: bfloat16 [2048, 2048], P('sp', 'tp'), may hold values from -0.125 to 0.125
- filter_taps: float32 [31, 2048], replicated, may hold values from -1 to 1
- layer_gain: float32 [2048], replicated, may hold values from 0.1 to 1.9
- layer_shift: float32 [2048], replicated, may hold values from -3 to 3
- retain_output: bfloat16 [2048, 4096], P('sp', 'tp'), may hold values from -0.09375 to 0.09375
- convolve_output: bfloat16 [2048, 2048], P('sp', 'tp'), may hold values from -0.125 to 0.125
Outputs:
- mixed: bfloat16 [4096, 2048], P(('sp', 'tp'))
The draws below stay inside these ranges and needn't reach their ends.
All inputs are finite; a program needn't handle non-finite values.
Results may differ from the reference program's by a relative error of at most 0.018.
Values may be sent and summed in bfloat16 or wider, within the bound.
A program may use at most 128 MiB of HBM per device.

```python
import jax
import jax.numpy as jnp
from jax import lax

D = 2048
HEADS = 8
KEY = 256
VAL = 512
CONV = 2048
GROUP = 512
KW = 31
TOK_DEV = 512
QK = 2048
VW = 4096
SEQ = 4096


def steps_of(stream_key, shape, cuts, smallest, top_value):
    gain, own = 1.0, jax.random.fold_in(stream_key, 6)
    for dim, shards_of in cuts:
        draws = jnp.exp(jax.random.uniform(jax.random.fold_in(own, dim), (shards_of,), jnp.float32, smallest / len(cuts), top_value / len(cuts)))
        gain = gain * jnp.repeat(draws, shape[dim] // shards_of).reshape([-1 if axis == dim else 1 for axis in range(len(shape))])
    return gain


def centred(own_key, extent, scale, most, shards=(), kind=jnp.bfloat16):
    drawn = jax.random.normal(own_key, extent, jnp.float32) * scale
    if len(shards) > 0:
        drawn = steps_of(own_key, extent, shards, -0.22, 0.18) * drawn
    return jnp.clip(drawn, min=-most, max=most).astype(kind)


def setup_inputs(seed: int = 0) -> dict:
    keys = jax.random.split(jax.random.key(seed), 15)
    return {
        "tokens": centred(keys[0], (SEQ, D), 1.0, 6.0, ((0, 32),)),
        "norm_gain": jnp.clip(1.0 + 0.18 * jax.random.normal(keys[1], (D,), jnp.float32), 0.1, 1.9),
        "query_weight": centred(keys[2], (D, QK), D ** -0.5, 0.125, ((0, 8), (1, 4))),
        "key_weight": centred(keys[3], (D, QK), D ** -0.5, 0.125, ((0, 8), (1, 4))),
        "value_weight": centred(keys[4], (D, VW), D ** -0.5, 0.125, ((0, 8), (1, 4))),
        "retain_gate": centred(keys[5], (D, VW), D ** -0.5, 0.125, ((0, 8), (1, 4))),
        "unit_value": centred(keys[6], (D, CONV), D ** -0.5, 0.125, ((0, 8), (1, 4))),
        "unit_gate": centred(keys[7], (D, CONV), D ** -0.5, 0.125, ((0, 8), (1, 4))),
        "convolve_gate": centred(keys[8], (D, CONV), D ** -0.5, 0.125, ((0, 8), (1, 4))),
        "filter_taps": centred(keys[9], (KW, CONV), KW ** -0.5, 1.0, (), jnp.float32),
        "layer_gain": jnp.clip(1.0 + 0.18 * jax.random.normal(keys[10], (CONV,), jnp.float32), 0.1, 1.9),
        "layer_shift": centred(keys[11], (CONV,), 0.5, 3.0, (), jnp.float32),
        "retain_output": centred(keys[12], (D, VW), VW ** -0.5, 0.09375, ((0, 8), (1, 4))),
        "convolve_output": centred(keys[13], (D, CONV), CONV ** -0.5, 0.125, ((0, 8), (1, 4))),
    }


rms_eps = 1e-06
group_eps = 1.0
layer_eps = 0.001
rope_base = 10000.0
highest = lax.Precision.HIGHEST

def rms_normalize(tokens, norm_gain):
    widened = tokens.astype(jnp.float32)
    scaled = widened * lax.rsqrt(lax.optimization_barrier(jnp.mean(widened * widened, axis=-1, keepdims=True)) + rms_eps)
    return (scaled * norm_gain).astype(jnp.bfloat16)

def widen(narrow_value):
    return lax.optimization_barrier(narrow_value.astype(jnp.bfloat16)).astype(jnp.float32)

def rotate(vectors, positions):
    half_width = vectors.shape[-1] // 2
    frequency = rope_base ** (-jnp.arange(half_width, dtype=jnp.float32) / half_width)
    angles = positions.astype(jnp.float32)[:, None] * frequency
    cosine = jnp.cos(angles)[:, None, :]
    sine_part = jnp.sin(angles)[:, None, :]
    front_half = vectors[..., :half_width]
    back_half = vectors[..., half_width:]
    return jnp.concatenate([front_half * cosine - back_half * sine_part, front_half * sine_part + back_half * cosine], axis=-1)

def prepare(queries, key_rows, values, positions):
    row_count = queries.shape[0]
    rotated_query = widen(rotate(queries.astype(jnp.float32).reshape(row_count, -1, KEY), positions))
    rotated_keys = widen(rotate(key_rows.astype(jnp.float32).reshape(row_count, -1, KEY), positions) * KEY ** (-0.5))
    value_heads = values.astype(jnp.float32).reshape(row_count, -1, VAL)
    return (rotated_query, rotated_keys, value_heads)

def decay_logs(first_head, head_total, all_heads, seq_length):
    ratio = (first_head + jnp.arange(head_total)).astype(jnp.float32) / (all_heads - 1)
    return (jnp.log(0.05) + ratio * jnp.log(18.0)) / seq_length

def local_parts(queries, key_rows, values, log_decay):
    row_count = queries.shape[0]
    indices = jnp.arange(row_count, dtype=jnp.float32)
    offsets = indices[:, None] - indices[None, :]
    causal = offsets >= 0
    weight = jnp.where(causal[None], jnp.exp(log_decay[:, None, None] * jnp.where(causal, offsets, 0.0)[None]), 0.0)
    scores = widen(jnp.einsum('ihd,jhd->hij', queries, key_rows) * weight)
    within = jnp.einsum('hij,jhe->ihe', scores, values)
    trailing = jnp.exp(log_decay[None, :] * (row_count - 1.0 - indices)[:, None])
    weighted = widen(key_rows * trailing[:, :, None])
    contribution = jnp.einsum('jhd,jhe->hde', weighted, values)
    return (within, contribution)

def cross_part(queries, carry_state, log_decay):
    row_count = queries.shape[0]
    indices = jnp.arange(row_count, dtype=jnp.float32)
    leading = jnp.exp(log_decay[None, :] * (indices + 1.0)[:, None])
    return jnp.einsum('ihd,hde->ihe', queries, carry_state, precision=highest) * leading[:, :, None]

def retain_finish(raw, switch):
    average = lax.optimization_barrier(jnp.mean(raw, axis=-1, keepdims=True))
    spread = lax.optimization_barrier(jnp.mean(jnp.square(raw - average), axis=-1, keepdims=True))
    normalized = ((raw - average) * lax.rsqrt(spread + group_eps)).reshape(raw.shape[0], -1)
    return (normalized * jax.nn.silu(switch.astype(jnp.float32))).astype(jnp.bfloat16)

def convolve_branch(gated_input, before, tap_slice, gain_slice, shift_slice, switch):
    padded = jnp.concatenate([before, gated_input], axis=0)
    row_count = gated_input.shape[0]
    summed = jnp.zeros(gated_input.shape, jnp.float32)
    for tap_index in range(tap_slice.shape[0]):
        summed = summed + padded[tap_index:tap_index + row_count].astype(jnp.float32) * tap_slice[tap_index]
    grouped = summed.reshape(row_count, -1, GROUP)
    average = lax.optimization_barrier(jnp.mean(grouped, axis=-1, keepdims=True))
    spread = lax.optimization_barrier(jnp.mean(jnp.square(grouped - average), axis=-1, keepdims=True))
    normalized = ((grouped - average) * lax.rsqrt(spread + layer_eps)).reshape(row_count, -1)
    normalized = normalized * gain_slice + shift_slice
    return (jax.nn.silu(normalized) * jax.nn.silu(switch.astype(jnp.float32))).astype(jnp.bfloat16)

def contract(hidden, matrix):
    return lax.dot_general(hidden, matrix, (((1,), (1,)), ((), ())), preferred_element_type=jnp.float32)

def reference(tokens, norm_gain, query_weight, key_weight, value_weight, retain_gate, unit_value, unit_gate, convolve_gate, filter_taps, layer_gain, layer_shift, retain_output, convolve_output):
    seq_total = tokens.shape[0]
    normed = rms_normalize(tokens, norm_gain)

    def project(matrix):
        return jnp.dot(normed, matrix, preferred_element_type=jnp.float32).astype(jnp.bfloat16)
    queries = project(query_weight)
    key_rows = project(key_weight)
    values = project(value_weight)
    retain_switch = project(retain_gate)
    glu_value = project(unit_value)
    glu_switch = project(unit_gate)
    convolve_switch = project(convolve_gate)
    positions = jnp.arange(seq_total, dtype=jnp.int32)
    rotated_query, rotated_keys, value_heads = prepare(queries, key_rows, values, positions)
    log_decay = decay_logs(0, HEADS, HEADS, seq_total)
    totals = jnp.exp(log_decay * TOK_DEV)
    blocks = seq_total // TOK_DEV

    def advance(carry_state, block):
        block_query, block_keys, block_values = block
        within, contribution = local_parts(block_query, block_keys, block_values, log_decay)
        result = within + cross_part(block_query, carry_state, log_decay)
        return (carry_state * totals[:, None, None] + contribution, result)
    start_state = jnp.zeros((HEADS, KEY, VAL), jnp.float32)
    final_state, outputs = lax.scan(advance, start_state, (rotated_query.reshape(blocks, TOK_DEV, HEADS, KEY), rotated_keys.reshape(blocks, TOK_DEV, HEADS, KEY), value_heads.reshape(blocks, TOK_DEV, HEADS, VAL)))
    raw = outputs.reshape(seq_total, HEADS, VAL)
    retain_hidden = retain_finish(raw, retain_switch)
    gated_input = (glu_value.astype(jnp.float32) * jax.nn.sigmoid(glu_switch.astype(jnp.float32))).astype(jnp.bfloat16)
    before = jnp.zeros((KW - 1, CONV), jnp.bfloat16)
    convolve_hidden = convolve_branch(gated_input, before, filter_taps, layer_gain, layer_shift, convolve_switch)
    summed = contract(retain_hidden, retain_output) + contract(convolve_hidden, convolve_output)
    return summed.astype(jnp.bfloat16)
```

```python
import jax
import jax.numpy as jnp
from jax import lax
from jax.experimental import pallas as pl
from jax.experimental.pallas import tpu as pltpu
from jax.sharding import Mesh
from jax.sharding import PartitionSpec as P

KEY = 256
VAL = 512
GROUP = 512
KW = 31


rms_eps = 1e-06
group_eps = 1.0
layer_eps = 0.001
rope_base = 10000.0


SPANS = ("tp", "lo")


def swap_planes(x):
    size = lax.axis_size("tp")
    pairs = [(h * size + t, t * size + h) for h in range(size) for t in range(size)]
    return lax.ppermute(x, ("hi", "tp"), pairs)


def from_behind(x, by):
    outer, inner = lax.axis_size("tp"), lax.axis_size("lo")
    spot = [(i % inner) * outer + i // inner for i in range(outer * inner)]
    return lax.ppermute(x, ("lo", "tp"), list(zip(spot[:-by], spot[by:])))


def carried_in(contribution, log_span_decay):
    length = lax.axis_size(SPANS)
    state = from_behind(contribution.astype(jnp.bfloat16), 1).astype(jnp.float32)
    by = 1
    while by < length:
        earlier = from_behind(state.astype(jnp.bfloat16), by).astype(jnp.float32)
        state = state + jnp.exp(log_span_decay * by)[:, None, None] * earlier
        by *= 2
    return state


def rms_normalize(tokens, norm_gain):
    widened = tokens.astype(jnp.float32)
    scaled = widened * lax.rsqrt(jnp.mean(widened * widened, axis=-1, keepdims=True) + rms_eps)
    return (scaled * norm_gain).astype(jnp.bfloat16)


def rotate(vectors, positions):
    half_width = vectors.shape[-1] // 2
    frequency = rope_base ** (-jnp.arange(half_width, dtype=jnp.float32) / half_width)
    angles = positions.astype(jnp.float32)[:, None] * frequency
    cosine = jnp.cos(angles)[:, None, :]
    sine_part = jnp.sin(angles)[:, None, :]
    front_half = vectors[..., :half_width]
    back_half = vectors[..., half_width:]
    return jnp.concatenate(
        [front_half * cosine - back_half * sine_part, front_half * sine_part + back_half * cosine],
        axis=-1,
    )


def prepare(queries, key_rows, values, positions):
    row_count = queries.shape[0]
    rotated_query = rotate(
        queries.astype(jnp.float32).reshape(row_count, -1, KEY), positions
    ).astype(jnp.bfloat16)
    rotated_keys = (
        rotate(key_rows.astype(jnp.float32).reshape(row_count, -1, KEY), positions) * KEY ** (-0.5)
    ).astype(jnp.bfloat16)
    value_heads = values.reshape(row_count, -1, VAL)
    return (rotated_query, rotated_keys, value_heads)


def decay_logs(first_head, head_total, all_heads, seq_length):
    ratio = (first_head + jnp.arange(head_total)).astype(jnp.float32) / (all_heads - 1)
    return (jnp.log(0.05) + ratio * jnp.log(18.0)) / seq_length


def local_parts(queries, key_rows, values, log_decay):
    row_count = queries.shape[0]
    indices = jnp.arange(row_count, dtype=jnp.float32)
    offsets = indices[:, None] - indices[None, :]
    causal = offsets >= 0
    weight = jnp.where(
        causal[None], jnp.exp(log_decay[:, None, None] * jnp.where(causal, offsets, 0.0)[None]), 0.0
    )
    scores = (
        jnp.einsum("ihd,jhd->hij", queries, key_rows, preferred_element_type=jnp.float32) * weight
    ).astype(jnp.bfloat16)
    within = jnp.einsum("hij,jhe->ihe", scores, values, preferred_element_type=jnp.float32)
    trailing = jnp.exp(log_decay[None, :] * (row_count - 1.0 - indices)[:, None])
    weighted = (key_rows.astype(jnp.float32) * trailing[:, :, None]).astype(jnp.bfloat16)
    contribution = jnp.einsum("jhd,jhe->hde", weighted, values, preferred_element_type=jnp.float32)
    return (within, contribution)


def cross_part(queries, carry_state, log_decay):
    row_count = queries.shape[0]
    indices = jnp.arange(row_count, dtype=jnp.float32)
    leading = jnp.exp(log_decay[None, :] * (indices + 1.0)[:, None])
    return (
        jnp.einsum(
            "ihd,hde->ihe",
            queries,
            carry_state.astype(jnp.bfloat16),
            preferred_element_type=jnp.float32,
        )
        * leading[:, :, None]
    )


def retain_finish(raw, switch):
    average = jnp.mean(raw, axis=-1, keepdims=True)
    spread = jnp.mean(jnp.square(raw - average), axis=-1, keepdims=True)
    normalized = ((raw - average) * lax.rsqrt(spread + group_eps)).reshape(raw.shape[0], -1)
    return (normalized * jax.nn.silu(switch.astype(jnp.float32))).astype(jnp.bfloat16)


def convolve_branch(gated_input, before, tap_slice, gain_slice, shift_slice, switch):
    padded = jnp.concatenate([before, gated_input], axis=0)
    row_count = gated_input.shape[0]
    summed = jnp.zeros(gated_input.shape, jnp.float32)
    for tap_index in range(tap_slice.shape[0]):
        summed = (
            summed
            + padded[tap_index : tap_index + row_count].astype(jnp.float32) * tap_slice[tap_index]
        )
    grouped = summed.reshape(row_count, -1, GROUP)
    average = jnp.mean(grouped, axis=-1, keepdims=True)
    spread = jnp.mean(jnp.square(grouped - average), axis=-1, keepdims=True)
    normalized = ((grouped - average) * lax.rsqrt(spread + layer_eps)).reshape(row_count, -1)
    normalized = normalized * gain_slice + shift_slice
    return (jax.nn.silu(normalized) * jax.nn.silu(switch.astype(jnp.float32))).astype(jnp.bfloat16)


def contract(hidden, matrix):
    return lax.dot_general(
        hidden, matrix, (((1,), (1,)), ((), ())), preferred_element_type=jnp.float32
    )


def local(
    tokens,
    norm_gain,
    query_weight,
    key_weight,
    value_weight,
    retain_gate,
    unit_value,
    unit_gate,
    convolve_gate,
    filter_taps,
    layer_gain,
    layer_shift,
    retain_output,
    convolve_output,
):
    head_groups = lax.axis_size("hi")
    chain_length = lax.axis_size(SPANS)
    head_rank = lax.axis_index("hi")
    chain_rank = lax.axis_index(SPANS)
    def project(rows, merged, *matrices):
        product = jnp.dot(rows, merged, preferred_element_type=jnp.float32).astype(jnp.bfloat16)
        ends = [sum(m.shape[1] for m in matrices[: k + 1]) for k in range(len(matrices) - 1)]
        return jnp.split(product, ends, axis=1)

    first = (key_weight, value_weight, query_weight)
    second = (unit_value, unit_gate, convolve_gate, retain_gate)
    third = (retain_output, convolve_output)
    groups = (first, second, third)
    merged = [jnp.concatenate(group, axis=1) for group in groups]
    normed = rms_normalize(tokens, norm_gain)
    normed = lax.all_gather(swap_planes(normed), "hi", axis=0, tiled=True)
    merged = [lax.all_gather(swap_planes(m), SPANS, axis=0, tiled=True) for m in merged]
    key_rows, values, queries = project(normed, merged[0], *first)
    glu_value, glu_switch, convolve_switch, retain_switch = project(normed, merged[1], *second)
    out_full = merged[2]
    row_count = normed.shape[0]
    local_heads = queries.shape[1] // KEY
    positions = chain_rank * row_count + jnp.arange(row_count, dtype=jnp.int32)
    rotated_query, rotated_keys, value_heads = prepare(queries, key_rows, values, positions)
    log_decay = decay_logs(
        head_rank * local_heads, local_heads, local_heads * head_groups, row_count * chain_length
    )
    within, contribution = local_parts(rotated_query, rotated_keys, value_heads, log_decay)
    gated_input = (
        glu_value.astype(jnp.float32) * jax.nn.sigmoid(glu_switch.astype(jnp.float32))
    ).astype(jnp.bfloat16)
    channels = gated_input.shape[1]
    before = from_behind(gated_input[row_count - (KW - 1) :], 1)
    incoming = carried_in(contribution, log_decay * row_count)
    raw = within + cross_part(rotated_query, incoming, log_decay)
    retain_hidden = retain_finish(raw, retain_switch)
    tap_slice = lax.dynamic_slice_in_dim(filter_taps, head_rank * channels, channels, 1)
    gain_slice = lax.dynamic_slice_in_dim(layer_gain, head_rank * channels, channels, 0)
    shift_slice = lax.dynamic_slice_in_dim(layer_shift, head_rank * channels, channels, 0)
    convolve_hidden = convolve_branch(
        gated_input, before, tap_slice, gain_slice, shift_slice, convolve_switch
    )
    hidden = jnp.concatenate([retain_hidden, convolve_hidden], axis=1)
    mixed = contract(hidden, out_full).astype(jnp.bfloat16)
    return swap_planes(lax.psum_scatter(mixed, "hi", scatter_dimension=0, tiled=True))


UNITS_IN = 9
AHEAD = 3
MESH = pl.DeviceIdType.MESH
SQUARE = ("zh", "zl", "y", "x", "c")
CHAIN = ("c", "zl", "y")


def remote(source, target, out_sem, in_sem, device):
    return pltpu.make_async_remote_copy(
        src_ref=source,
        dst_ref=target,
        send_sem=out_sem,
        recv_sem=in_sem,
        device_id=device,
        device_id_type=MESH,
    )


def place():
    return tuple(lax.axis_index(name) for name in SQUARE)


class Gather:
    def __init__(self, source, full, near, send, arrive, beside):
        self.source, self.full, self.near = source, full, near
        self.send, self.arrive, self.beside = send, arrive, beside
        zh, zl, y, x, c = self.at = place()
        self.depth = source.shape[1]
        self.half = self.depth // 2
        self.outer = zl * zh + (1 - zl) * (1 - zh)
        self.mine = self.index(zh, self.outer, y)
        self.is_own = c == zh

    def index(self, zh, outer, y):
        zl = outer * zh + (1 - outer) * (1 - zh)
        return (zh * 2 + zl) * 2 + y

    def own(self, outer, flip):
        return self.index(self.at[0], outer, self.at[2] if not flip else 1 - self.at[2])

    def far(self, outer, flip):
        return self.index(1 - self.at[0], outer, self.at[2] if not flip else 1 - self.at[2])

    def rows(self, k, s, half):
        start = pl.multiple_of(s * self.depth + half * self.half, self.half)
        return self.full.at[k, pl.ds(start, self.half)]

    def whole(self, k, s):
        return self.full.at[k, pl.ds(pl.multiple_of(s * self.depth, self.depth), self.depth)]

    def z_mate(self, core):
        zh, zl, y, x, c = self.at
        return (zh, 1 - zl, y, x, core)

    def y_mate(self, core):
        zh, zl, y, x, c = self.at
        return (zh, zl, 1 - y, x, core)

    def sibling(self):
        zh, zl, y, x, c = self.at
        return (zh, zl, y, x, 1 - c)

    def load(self, k, ref, first):
        part = ref.at[:, pl.ds(first, self.source.shape[2])]

        @pl.when(self.is_own)
        def _():
            pltpu.make_async_copy(part, self.whole(k, self.mine), self.near.at[k]).start()

        @pl.when(jnp.logical_not(self.is_own))
        def _():
            pltpu.make_async_copy(part, self.source.at[k], self.near.at[k]).start()

    def own_sends(self, k):
        zh, zl, y, x, c = self.at
        part = self.whole(k, self.mine)
        copies = [remote(part, part, self.send.at[k, 16], self.beside.at[k], self.sibling())]
        for r in range(2):
            piece = self.rows(k, self.mine, r)
            arrive = self.arrive.at[k, self.mine, r]
            copies.append(remote(piece, piece, self.send.at[k, 12 + r], arrive, self.z_mate(r)))
            copies.append(remote(piece, piece, self.send.at[k, 14 + r], arrive, self.y_mate(r)))
        return copies

    def far_sends(self, k):
        zh, zl, y, x, c = self.at
        copies = []
        for r in range(2):
            piece = self.source.at[k, pl.ds(r * self.half, self.half)]
            copies.append(
                remote(
                    piece,
                    self.rows(k, self.mine, r),
                    self.send.at[k, 12 + r],
                    self.arrive.at[k, self.mine, r],
                    (c, 1 - c, y, x, r),
                )
            )
        return copies

    def begin(self, k):
        pltpu.make_async_copy(self.source.at[k], self.source.at[k], self.near.at[k]).wait()

        @pl.when(self.is_own)
        def _():
            for copy in self.own_sends(k):
                copy.start()

        @pl.when(jnp.logical_not(self.is_own))
        def _():
            for copy in self.far_sends(k):
                copy.start()

    def onward(self, k, s, device, slot):
        piece = self.rows(k, s, self.at[4])
        return remote(piece, piece, self.send.at[k, slot], self.arrive.at[k, s, self.at[4]], device)

    def landed(self, k, s, half):
        piece = self.rows(k, s, half)
        remote(
            piece, piece, self.send.at[k, 0], self.arrive.at[k, s, half], self.sibling()
        ).wait_recv()

    def table(self):
        c = self.at[4]
        z_mate, y_mate, sibling = self.z_mate(c), self.y_mate(c), self.sibling()
        inner = (
            (
                (self.far(0, 0), ((z_mate, 0, None), (y_mate, 1, None), (sibling, 2, None))),
                (self.far(1, 0), ((z_mate, 3, None), (y_mate, 4, None), (sibling, 5, None))),
                (self.own(0, 1), ((z_mate, 8, 0), (sibling, 7, None))),
                (self.own(1, 0), ((sibling, 6, None),)),
            ),
            (
                (self.far(0, 1), ((sibling, 9, None),)),
                (self.far(1, 1), ((sibling, 10, None),)),
                (self.own(1, 1), ((sibling, 11, None),)),
            ),
            (),
        )
        outer = (
            (
                (self.own(1, 1), ((z_mate, 2, None), (sibling, 3, None))),
                (self.own(0, 0), ((y_mate, 1, 1), (sibling, 0, None))),
            ),
            (
                (self.far(0, 0), ((y_mate, 4, None), (sibling, 5, None))),
                (self.far(1, 0), ((y_mate, 6, None), (sibling, 7, None))),
            ),
            (
                (self.own(0, 1), ((sibling, 10, None),)),
                (self.far(0, 1), ((sibling, 8, None),)),
                (self.far(1, 1), ((sibling, 9, None),)),
            ),
        )
        return inner, outer

    def stage(self, k, number):
        for role, moves in enumerate(self.table()):
            if not moves[number]:
                continue

            @pl.when(self.outer == role)
            def _():
                for s, targets in moves[number]:
                    self.landed(k, s, self.at[4])
                    for device, slot, lane in targets:
                        copy = self.onward(k, s, device, slot)
                        if lane is None:
                            copy.start()
                        else:
                            pl.when(self.at[4] == lane)(copy.start)

    def complete(self, k):
        other = 1 - self.at[4]
        for s in (
            self.own(1 - self.outer, 0),
            self.own(self.outer, 1),
            self.own(1 - self.outer, 1),
            self.far(0, 0),
            self.far(1, 0),
            self.far(0, 1),
            self.far(1, 1),
        ):
            self.landed(k, s, other)

        @pl.when(jnp.logical_not(self.is_own))
        def _():
            part = self.whole(k, self.mine)
            remote(
                part, part, self.send.at[k, 0], self.beside.at[k], self.sibling()
            ).wait_recv()

    def drain(self, k):
        @pl.when(self.is_own)
        def _():
            for copy in self.own_sends(k):
                copy.wait_send()

        @pl.when(jnp.logical_not(self.is_own))
        def _():
            for copy in self.far_sends(k):
                copy.wait_send()

        for role, moves in enumerate(self.table()):

            @pl.when(self.outer == role)
            def _():
                for number in range(3):
                    for s, targets in moves[number]:
                        for device, slot, lane in targets:
                            copy = self.onward(k, s, device, slot)
                            if lane is None:
                                copy.wait_send()
                            else:
                                pl.when(self.at[4] == lane)(copy.wait_send)


def gather_scratch(units, depth, width, shares, dtype):
    return [
        pltpu.VMEM((units, depth, width), dtype),
        pltpu.VMEM((units, shares * depth, width), dtype),
        pltpu.SemaphoreType.DMA((units,)),
        pltpu.SemaphoreType.DMA((units, 17)),
        pltpu.SemaphoreType.DMA((units, shares, 2)),
        pltpu.SemaphoreType.DMA((units,)),
    ]


def gather_kernel(layout, units, *refs):
    rows_ref, blocks = refs[0], refs[1:10]
    product_ref, out_ref = refs[10:12]
    normed = refs[12]
    source, full, near, send, arrive, beside = refs[13:19]
    rows_send, rows_arrive, out_sem = refs[19:]
    zh, zl, y, x, c = place()
    gather = Gather(source, full, near, send, arrive, beside)
    count = rows_ref.shape[0]
    mine = normed.at[pl.ds(pl.multiple_of((x * 2 + c) * count, count), count)]

    def rows_copy(dz, dx):
        to_z = zh if not dz else 1 - zh
        to_x = x if not dx else 1 - x
        return remote(
            rows_ref,
            mine,
            rows_send.at[dz * 2 + dx],
            rows_arrive.at[x * 2 + c],
            (to_z, zl, y, to_x, zh),
        )

    far_rows = ((0, 1), (1, 0), (1, 1))
    for dz, dx in far_rows:
        rows_copy(dz, dx).start()

    @pl.when(c == zh)
    def _():
        pltpu.make_async_copy(rows_ref, mine, rows_arrive.at[x * 2 + c]).start()

    @pl.when(c != zh)
    def _():
        rows_copy(0, 0).start()

    for k, (which, first) in enumerate(layout):
        gather.load(k, blocks[which], first)

    for k in range(AHEAD):
        gather.begin(k)

    for j in range(4):
        part = normed.at[pl.ds(j * count, count)]
        remote(part, part, rows_send.at[0], rows_arrive.at[j], gather.sibling()).wait_recv()

    def when_unit(k, limit, what):
        @pl.when(jnp.logical_and(k >= 0, k < limit))
        def _():
            what(k)

    def project(k):
        wide = full.shape[2] // 2
        for part in range(2):
            columns = pl.ds(part * wide, wide)
            product_ref[k, :, columns] = jnp.dot(
                normed[...], full[k, :, columns], preferred_element_type=jnp.float32
            ).astype(product_ref.dtype)

    def write_out(k):
        pltpu.make_async_copy(full.at[k], out_ref.at[k - UNITS_IN], out_sem.at[k - UNITS_IN]).start()

    def step(i, carry):
        when_unit(i, units, lambda k: gather.stage(k, 0))
        when_unit(i - 1, units, lambda k: gather.stage(k, 1))
        when_unit(i - 2, units, lambda k: gather.stage(k, 2))
        when_unit(i + AHEAD, units, gather.begin)
        when_unit(i - 3, units, gather.complete)
        when_unit(i - 3, UNITS_IN, project)

        @pl.when(i - 3 >= UNITS_IN)
        def _():
            write_out(i - 3)

        return carry

    lax.fori_loop(0, units + 3, step, 0)

    def finish(k, carry):
        gather.drain(k)
        return carry

    lax.fori_loop(0, units, finish, 0)
    for dz, dx in far_rows:
        rows_copy(dz, dx).wait_send()

    @pl.when(c != zh)
    def _():
        rows_copy(0, 0).wait_send()

    for k in range(units - UNITS_IN):
        pltpu.make_async_copy(full.at[UNITS_IN + k], out_ref.at[k], out_sem.at[k]).wait()


def gather_and_project(rows, blocks, width):
    layout = [(n, first) for n, b in enumerate(blocks) for first in range(0, b.shape[1], width)]
    units = len(layout)
    depth, shares, dtype = blocks[0].shape[0], 8, rows.dtype
    span = 4 * rows.shape[0]
    return pl.pallas_call(
        lambda *refs: gather_kernel(layout, units, *refs),
        out_shape=[
            jax.ShapeDtypeStruct((UNITS_IN, span, width), dtype),
            jax.ShapeDtypeStruct((units - UNITS_IN, shares * depth, width), dtype),
        ],
        in_specs=[pl.BlockSpec(memory_space=pl.ANY)] * (1 + len(blocks)),
        out_specs=[pl.BlockSpec(memory_space=pltpu.VMEM), pl.BlockSpec(memory_space=pl.ANY)],
        scratch_shapes=[pltpu.VMEM((span, rows.shape[1]), dtype)]
        + gather_scratch(units, depth, width, shares, dtype)
        + [
            pltpu.SemaphoreType.DMA((4,)),
            pltpu.SemaphoreType.DMA((4,)),
            pltpu.SemaphoreType.DMA((units - UNITS_IN,)),
        ],
        compiler_params=pltpu.CompilerParams(has_side_effects=True, vmem_limit_bytes=56 << 20),
        name="gather_project",
    )(rows, *blocks)


def finish_kernel(tile, first, second, third, matrix, out, kept, sent, got, half, here, there, sems):
    hidden = (first, second, third)
    zh, zl, y, x, c = place()
    tiles = matrix.shape[1] // tile
    share = out.shape[0]
    pair = 2 * share
    to_x, from_x, to_near, from_near, to_far, from_far = (sems.at[k] for k in range(6))
    across, sibling = (zh, zl, y, 1 - x, c), (zh, zl, y, x, 1 - c)
    stays = c == zh

    def x_copy(n):
        return remote(sent.at[n], got.at[n], to_x.at[n], from_x.at[n], across)

    def near_copy(n):
        part = half.at[n, pl.ds(pl.multiple_of((1 - c) * share, share), share)]
        return remote(part, here.at[n], to_near.at[n], from_near.at[n], sibling)

    def far_copy(n, core):
        part = half.at[n, pl.ds(core * share, share)]
        out_sem = (to_near if core == 0 else to_far).at[n]
        return remote(part, there.at[n], out_sem, from_far.at[n], (c, zl, y, x, core))

    def multiply(n):
        lines = pl.ds(pl.multiple_of(n * tile, tile), tile)
        total = contract(hidden[0][...], matrix[0, lines])
        total += contract(hidden[1][...], matrix[1, lines])
        total += contract(hidden[2][...], matrix[2, lines])
        low, high = total[:pair], total[pair:]
        kept[n] = jnp.where(x == 0, low, high)
        sent[n] = jnp.where(x == 0, high, low).astype(sent.dtype)
        x_copy(n).start()

    def join(n):
        x_copy(n).wait_recv()
        half[n] = (kept[n] + got[n].astype(jnp.float32)).astype(half.dtype)

        @pl.when(stays)
        def _():
            near_copy(n).start()

        @pl.when(jnp.logical_not(stays))
        def _():
            far_copy(n, 0).start()
            far_copy(n, 1).start()

    def close(n):
        remote(there.at[n], there.at[n], to_far.at[n], from_far.at[n], across).wait_recv()
        lines = pl.ds(pl.multiple_of(n * tile, tile), tile)
        far_part = there[n].astype(jnp.float32)

        @pl.when(stays)
        def _():
            mine = half[n, pl.ds(pl.multiple_of(c * share, share), share)].astype(jnp.float32)
            out[:, lines] = (mine + far_part).astype(out.dtype)

        @pl.when(jnp.logical_not(stays))
        def _():
            near_copy(n).wait_recv()
            out[:, lines] = (here[n].astype(jnp.float32) + far_part).astype(out.dtype)

    def when_tile(n, what):
        @pl.when(jnp.logical_and(n >= 0, n < tiles))
        def _():
            what(n)

    def step(i, carry):
        when_tile(i, multiply)
        when_tile(i - 3, join)
        when_tile(i - 6, close)
        return carry

    lax.fori_loop(0, tiles + 6, step, 0)

    def drain(n, carry):
        x_copy(n).wait_send()

        @pl.when(stays)
        def _():
            near_copy(n).wait_send()

        @pl.when(jnp.logical_not(stays))
        def _():
            far_copy(n, 0).wait_send()
            far_copy(n, 1).wait_send()

        return carry

    lax.fori_loop(0, tiles, drain, 0)


def finish_outputs(hidden, matrix, tile):
    span = hidden[0].shape[0]
    share = span // 4
    tiles = matrix.shape[1] // tile
    dtype = matrix.dtype
    return pl.pallas_call(
        lambda *refs: finish_kernel(tile, *refs),
        out_shape=jax.ShapeDtypeStruct((share, matrix.shape[1]), dtype),
        in_specs=[pl.BlockSpec(memory_space=pltpu.VMEM)] * 4,
        out_specs=pl.BlockSpec(memory_space=pltpu.VMEM),
        scratch_shapes=[
            pltpu.VMEM((tiles, 2 * share, tile), jnp.float32),
            pltpu.VMEM((tiles, 2 * share, tile), dtype),
            pltpu.VMEM((tiles, 2 * share, tile), dtype),
            pltpu.VMEM((tiles, 2 * share, tile), dtype),
            pltpu.VMEM((tiles, share, tile), dtype),
            pltpu.VMEM((tiles, share, tile), dtype),
            pltpu.SemaphoreType.DMA((6, tiles)),
        ],
        compiler_params=pltpu.CompilerParams(has_side_effects=True, vmem_limit_bytes=56 << 20),
        name="finish",
    )(*hidden, matrix)


def shifted(x, by):
    length, cores = lax.axis_size(CHAIN), lax.axis_size("c")
    inner = length // cores
    spot = [(i % inner) * cores + i // inner for i in range(length)]
    return lax.ppermute(x, ("zl", "y", "c"), list(zip(spot[:-by], spot[by:])))


def local_squares(
    tokens,
    norm_gain,
    query_weight,
    key_weight,
    value_weight,
    retain_gate,
    unit_value,
    unit_gate,
    convolve_gate,
    filter_taps,
    layer_gain,
    layer_shift,
    retain_output,
    convolve_output,
):
    rank = lax.axis_index("x") * 2 + lax.axis_index("zh")
    groups = 4
    chain_length = lax.axis_size(CHAIN)
    chain_rank = lax.axis_index(CHAIN)
    normed = rms_normalize(tokens, norm_gain)
    blocks = (key_weight, value_weight, query_weight, unit_value, unit_gate, convolve_gate)
    blocks += (retain_gate, retain_output, convolve_output)
    products, matrix = gather_and_project(normed, blocks, key_weight.shape[1])
    keys, value_0, value_1, queries, glu_value, glu_switch, convolve_switch, gate_0, gate_1 = (
        products[k] for k in range(UNITS_IN)
    )
    row_count = keys.shape[0]
    local_heads = 2
    positions = chain_rank * row_count + jnp.arange(row_count, dtype=jnp.int32)
    log_decay = decay_logs(
        rank * local_heads, local_heads, local_heads * groups, row_count * chain_length
    )
    values = jnp.concatenate([value_0, value_1], axis=1)
    rotated_query, rotated_keys, value_heads = prepare(queries, keys, values, positions)
    within, contribution = local_parts(rotated_query, rotated_keys, value_heads, log_decay)
    gated_input = (
        glu_value.astype(jnp.float32) * jax.nn.sigmoid(glu_switch.astype(jnp.float32))
    ).astype(jnp.bfloat16)
    channels = gated_input.shape[1]
    before = shifted(gated_input[row_count - (KW - 1) :], 1)
    log_span = log_decay * row_count
    state = shifted(contribution.astype(jnp.bfloat16), 1).astype(jnp.float32)
    by = 1
    while by < chain_length:
        earlier = shifted(state.astype(jnp.bfloat16), by).astype(jnp.float32)
        state = state + jnp.exp(log_span * by)[:, None, None] * earlier
        by *= 2
    raw = within + cross_part(rotated_query, state, log_decay)
    retain_hidden = retain_finish(raw, jnp.concatenate([gate_0, gate_1], axis=1))
    tap_slice = lax.dynamic_slice_in_dim(filter_taps, rank * channels, channels, 1)
    gain_slice = lax.dynamic_slice_in_dim(layer_gain, rank * channels, channels, 0)
    shift_slice = lax.dynamic_slice_in_dim(layer_shift, rank * channels, channels, 0)
    convolve_hidden = convolve_branch(
        gated_input, before, tap_slice, gain_slice, shift_slice, convolve_switch
    )
    hidden = (retain_hidden[:, :VAL], retain_hidden[:, VAL:], convolve_hidden)
    return finish_outputs(hidden, matrix, 256)


def squares(mesh):
    boxes = Mesh(mesh.devices.reshape(2, 2, 2, 2, 2), SQUARE)
    rows, blocks = P(SQUARE, None), P(("zh", "zl", "y"), ("x", "c"))
    return jax.shard_map(
        local_squares,
        mesh=boxes,
        in_specs=(rows, P()) + (blocks,) * 7 + (P(),) * 3 + (blocks,) * 2,
        out_specs=rows,
        check_vma=False,
    )


def solution(mesh):
    sp, tp = mesh.shape["sp"], mesh.shape["tp"]
    if (sp, tp) == (8, 4):
        return squares(mesh)
    planes = Mesh(mesh.devices.reshape(tp, sp // tp, tp), ("hi", "lo", "tp"))
    return jax.shard_map(
        local,
        mesh=planes,
        in_specs=(
            P(("hi", "lo", "tp"), None),
            P(),
            P(("hi", "lo"), "tp"),
            P(("hi", "lo"), "tp"),
            P(("hi", "lo"), "tp"),
            P(("hi", "lo"), "tp"),
            P(("hi", "lo"), "tp"),
            P(("hi", "lo"), "tp"),
            P(("hi", "lo"), "tp"),
            P(),
            P(),
            P(),
            P(("hi", "lo"), "tp"),
            P(("hi", "lo"), "tp"),
        ),
        out_specs=P(("hi", "lo", "tp"), None),
        check_vma=False,
    )
```

```python
import math

import jax
import jax.numpy as jnp
from jax import lax
from jax.experimental import pallas as pl
from jax.experimental.pallas import tpu as pltpu
from jax.sharding import Mesh
from jax.sharding import PartitionSpec as P

KEY = 256
VAL = 512
GROUP = 512
KW = 31


rms_eps = 1e-06
group_eps = 1.0
layer_eps = 0.001
rope_base = 10000.0


SPANS = ("tp", "lo")


def swap_planes(x):
    size = lax.axis_size("tp")
    pairs = [(h * size + t, t * size + h) for h in range(size) for t in range(size)]
    return lax.ppermute(x, ("hi", "tp"), pairs)


def from_behind(x, by):
    outer, inner = lax.axis_size("tp"), lax.axis_size("lo")
    spot = [(i % inner) * outer + i // inner for i in range(outer * inner)]
    return lax.ppermute(x, ("lo", "tp"), list(zip(spot[:-by], spot[by:])))


def carried_in(contribution, log_span_decay):
    length = lax.axis_size(SPANS)
    state = from_behind(contribution.astype(jnp.bfloat16), 1).astype(jnp.float32)
    by = 1
    while by < length:
        earlier = from_behind(state.astype(jnp.bfloat16), by).astype(jnp.float32)
        state = state + jnp.exp(log_span_decay * by)[:, None, None] * earlier
        by *= 2
    return state


def rms_normalize(tokens, norm_gain):
    widened = tokens.astype(jnp.float32)
    scaled = widened * lax.rsqrt(jnp.mean(widened * widened, axis=-1, keepdims=True) + rms_eps)
    return (scaled * norm_gain).astype(jnp.bfloat16)


def rotate(vectors, positions):
    half_width = vectors.shape[-1] // 2
    frequency = rope_base ** (-jnp.arange(half_width, dtype=jnp.float32) / half_width)
    angles = positions.astype(jnp.float32)[:, None] * frequency
    cosine = jnp.cos(angles)[:, None, :]
    sine_part = jnp.sin(angles)[:, None, :]
    front_half = vectors[..., :half_width]
    back_half = vectors[..., half_width:]
    return jnp.concatenate(
        [front_half * cosine - back_half * sine_part, front_half * sine_part + back_half * cosine],
        axis=-1,
    )


def prepare(queries, key_rows, values, positions):
    row_count = queries.shape[0]
    rotated_query = rotate(
        queries.astype(jnp.float32).reshape(row_count, -1, KEY), positions
    ).astype(jnp.bfloat16)
    rotated_keys = (
        rotate(key_rows.astype(jnp.float32).reshape(row_count, -1, KEY), positions) * KEY ** (-0.5)
    ).astype(jnp.bfloat16)
    value_heads = values.reshape(row_count, -1, VAL)
    return (rotated_query, rotated_keys, value_heads)


def decay_logs(first_head, head_total, all_heads, seq_length):
    ratio = (first_head + jnp.arange(head_total)).astype(jnp.float32) / (all_heads - 1)
    return (jnp.log(0.05) + ratio * jnp.log(18.0)) / seq_length


def local_parts(queries, key_rows, values, log_decay):
    row_count = queries.shape[0]
    indices = jnp.arange(row_count, dtype=jnp.float32)
    offsets = indices[:, None] - indices[None, :]
    causal = offsets >= 0
    weight = jnp.where(
        causal[None], jnp.exp(log_decay[:, None, None] * jnp.where(causal, offsets, 0.0)[None]), 0.0
    )
    scores = (
        jnp.einsum("ihd,jhd->hij", queries, key_rows, preferred_element_type=jnp.float32) * weight
    ).astype(jnp.bfloat16)
    within = jnp.einsum("hij,jhe->ihe", scores, values, preferred_element_type=jnp.float32)
    trailing = jnp.exp(log_decay[None, :] * (row_count - 1.0 - indices)[:, None])
    weighted = (key_rows.astype(jnp.float32) * trailing[:, :, None]).astype(jnp.bfloat16)
    contribution = jnp.einsum("jhd,jhe->hde", weighted, values, preferred_element_type=jnp.float32)
    return (within, contribution)


def cross_part(queries, carry_state, log_decay):
    row_count = queries.shape[0]
    indices = jnp.arange(row_count, dtype=jnp.float32)
    leading = jnp.exp(log_decay[None, :] * (indices + 1.0)[:, None])
    return (
        jnp.einsum(
            "ihd,hde->ihe",
            queries,
            carry_state.astype(jnp.bfloat16),
            preferred_element_type=jnp.float32,
        )
        * leading[:, :, None]
    )


def retain_finish(raw, switch):
    average = jnp.mean(raw, axis=-1, keepdims=True)
    spread = jnp.mean(jnp.square(raw - average), axis=-1, keepdims=True)
    normalized = ((raw - average) * lax.rsqrt(spread + group_eps)).reshape(raw.shape[0], -1)
    return (normalized * jax.nn.silu(switch.astype(jnp.float32))).astype(jnp.bfloat16)


def convolve_branch(gated_input, before, tap_slice, gain_slice, shift_slice, switch):
    padded = jnp.concatenate([before, gated_input], axis=0)
    row_count = gated_input.shape[0]
    summed = jnp.zeros(gated_input.shape, jnp.float32)
    for tap_index in range(tap_slice.shape[0]):
        summed = (
            summed
            + padded[tap_index : tap_index + row_count].astype(jnp.float32) * tap_slice[tap_index]
        )
    grouped = summed.reshape(row_count, -1, GROUP)
    average = jnp.mean(grouped, axis=-1, keepdims=True)
    spread = jnp.mean(jnp.square(grouped - average), axis=-1, keepdims=True)
    normalized = ((grouped - average) * lax.rsqrt(spread + layer_eps)).reshape(row_count, -1)
    normalized = normalized * gain_slice + shift_slice
    return (jax.nn.silu(normalized) * jax.nn.silu(switch.astype(jnp.float32))).astype(jnp.bfloat16)


def contract(hidden, matrix):
    return lax.dot_general(
        hidden, matrix, (((1,), (1,)), ((), ())), preferred_element_type=jnp.float32
    )


def local(
    tokens,
    norm_gain,
    query_weight,
    key_weight,
    value_weight,
    retain_gate,
    unit_value,
    unit_gate,
    convolve_gate,
    filter_taps,
    layer_gain,
    layer_shift,
    retain_output,
    convolve_output,
):
    head_groups = lax.axis_size("hi")
    chain_length = lax.axis_size(SPANS)
    head_rank = lax.axis_index("hi")
    chain_rank = lax.axis_index(SPANS)
    def project(rows, merged, *matrices):
        product = jnp.dot(rows, merged, preferred_element_type=jnp.float32).astype(jnp.bfloat16)
        ends = [sum(m.shape[1] for m in matrices[: k + 1]) for k in range(len(matrices) - 1)]
        return jnp.split(product, ends, axis=1)

    first = (key_weight, value_weight, query_weight)
    second = (unit_value, unit_gate, convolve_gate, retain_gate)
    third = (retain_output, convolve_output)
    groups = (first, second, third)
    merged = [jnp.concatenate(group, axis=1) for group in groups]
    normed = rms_normalize(tokens, norm_gain)
    normed = lax.all_gather(swap_planes(normed), "hi", axis=0, tiled=True)
    merged = [lax.all_gather(swap_planes(m), SPANS, axis=0, tiled=True) for m in merged]
    key_rows, values, queries = project(normed, merged[0], *first)
    glu_value, glu_switch, convolve_switch, retain_switch = project(normed, merged[1], *second)
    out_full = merged[2]
    row_count = normed.shape[0]
    local_heads = queries.shape[1] // KEY
    positions = chain_rank * row_count + jnp.arange(row_count, dtype=jnp.int32)
    rotated_query, rotated_keys, value_heads = prepare(queries, key_rows, values, positions)
    log_decay = decay_logs(
        head_rank * local_heads, local_heads, local_heads * head_groups, row_count * chain_length
    )
    within, contribution = local_parts(rotated_query, rotated_keys, value_heads, log_decay)
    gated_input = (
        glu_value.astype(jnp.float32) * jax.nn.sigmoid(glu_switch.astype(jnp.float32))
    ).astype(jnp.bfloat16)
    channels = gated_input.shape[1]
    before = from_behind(gated_input[row_count - (KW - 1) :], 1)
    incoming = carried_in(contribution, log_decay * row_count)
    raw = within + cross_part(rotated_query, incoming, log_decay)
    retain_hidden = retain_finish(raw, retain_switch)
    tap_slice = lax.dynamic_slice_in_dim(filter_taps, head_rank * channels, channels, 1)
    gain_slice = lax.dynamic_slice_in_dim(layer_gain, head_rank * channels, channels, 0)
    shift_slice = lax.dynamic_slice_in_dim(layer_shift, head_rank * channels, channels, 0)
    convolve_hidden = convolve_branch(
        gated_input, before, tap_slice, gain_slice, shift_slice, convolve_switch
    )
    hidden = jnp.concatenate([retain_hidden, convolve_hidden], axis=1)
    mixed = contract(hidden, out_full).astype(jnp.bfloat16)
    return swap_planes(lax.psum_scatter(mixed, "hi", scatter_dimension=0, tiled=True))


AHEAD = 5
LAGS = (0, 2, 3, 4)
ROWS_AFTER = 2
ROWS_RELAY = 3
MESH = pl.DeviceIdType.MESH
SQUARE = ("zh", "zl", "y", "x", "c")
CHAIN = ("c", "zl", "y")


def remote(source, target, out_sem, in_sem, device):
    return pltpu.make_async_remote_copy(
        src_ref=source,
        dst_ref=target,
        send_sem=out_sem,
        recv_sem=in_sem,
        device_id=device,
        device_id_type=MESH,
    )


def place():
    return tuple(lax.axis_index(name) for name in SQUARE)


class Gather:
    def __init__(self, source, full, near, send, arrive, beside):
        self.source, self.full, self.near = source, full, near
        self.send, self.arrive, self.beside = send, arrive, beside
        zh, zl, y, x, c = self.at = place()
        self.depth = source.shape[1]
        self.half = self.depth // 2
        self.outer = zl * zh + (1 - zl) * (1 - zh)
        self.mine = self.index(zh, self.outer, y)
        self.is_own = c == zh

    def index(self, zh, outer, y):
        zl = outer * zh + (1 - outer) * (1 - zh)
        return (zh * 2 + zl) * 2 + y

    def own(self, outer, flip):
        return self.index(self.at[0], outer, self.at[2] if not flip else 1 - self.at[2])

    def far(self, outer, flip):
        return self.index(1 - self.at[0], outer, self.at[2] if not flip else 1 - self.at[2])

    def rows(self, k, s, half):
        start = pl.multiple_of(s * self.depth + half * self.half, self.half)
        return self.full.at[k, pl.ds(start, self.half)]

    def whole(self, k, s):
        return self.full.at[k, pl.ds(pl.multiple_of(s * self.depth, self.depth), self.depth)]

    def z_mate(self, core):
        zh, zl, y, x, c = self.at
        return (zh, 1 - zl, y, x, core)

    def y_mate(self, core):
        zh, zl, y, x, c = self.at
        return (zh, zl, 1 - y, x, core)

    def sibling(self):
        zh, zl, y, x, c = self.at
        return (zh, zl, y, x, 1 - c)

    def load(self, k, part, columns):
        columns = pl.ds(0, self.source.shape[2]) if columns is None else columns

        @pl.when(self.is_own)
        def _():
            target = self.whole(k, self.mine).at[:, columns]
            pltpu.make_async_copy(part, target, self.near.at[k]).start()

        @pl.when(jnp.logical_not(self.is_own))
        def _():
            target = self.source.at[k].at[:, columns]
            pltpu.make_async_copy(part, target, self.near.at[k]).start()

    def own_sends(self, k):
        zh, zl, y, x, c = self.at
        part = self.whole(k, self.mine)
        copies = [remote(part, part, self.send.at[k, 16], self.beside.at[k], self.sibling())]
        for r in range(2):
            piece = self.rows(k, self.mine, r)
            arrive = self.arrive.at[k, self.mine, r]
            copies.append(remote(piece, piece, self.send.at[k, 12 + r], arrive, self.z_mate(r)))
            copies.append(remote(piece, piece, self.send.at[k, 14 + r], arrive, self.y_mate(r)))
        return copies

    def far_sends(self, k):
        zh, zl, y, x, c = self.at
        copies = []
        for r in range(2):
            piece = self.source.at[k, pl.ds(r * self.half, self.half)]
            copies.append(
                remote(
                    piece,
                    self.rows(k, self.mine, r),
                    self.send.at[k, 12 + r],
                    self.arrive.at[k, self.mine, r],
                    (c, 1 - c, y, x, r),
                )
            )
        return copies

    def begin(self, k):
        pltpu.make_async_copy(self.source.at[k], self.source.at[k], self.near.at[k]).wait()

        @pl.when(self.is_own)
        def _():
            for copy in self.own_sends(k):
                copy.start()

        @pl.when(jnp.logical_not(self.is_own))
        def _():
            for copy in self.far_sends(k):
                copy.start()

    def onward(self, k, s, device, slot):
        piece = self.rows(k, s, self.at[4])
        return remote(piece, piece, self.send.at[k, slot], self.arrive.at[k, s, self.at[4]], device)

    def landed(self, k, s, half):
        piece = self.rows(k, s, half)
        remote(
            piece, piece, self.send.at[k, 0], self.arrive.at[k, s, half], self.sibling()
        ).wait_recv()

    def table(self):
        c = self.at[4]
        z_mate, y_mate, sibling = self.z_mate(c), self.y_mate(c), self.sibling()
        inner = (
            (
                (self.far(0, 0), ((z_mate, 0, None), (y_mate, 1, None), (sibling, 2, None))),
                (self.far(1, 0), ((z_mate, 3, None), (y_mate, 4, None), (sibling, 5, None))),
                (self.own(0, 1), ((z_mate, 8, 0), (sibling, 7, None))),
                (self.own(1, 0), ((sibling, 6, None),)),
            ),
            (
                (self.far(0, 1), ((sibling, 9, None),)),
                (self.far(1, 1), ((sibling, 10, None),)),
                (self.own(1, 1), ((sibling, 11, None),)),
            ),
            (),
        )
        outer = (
            (
                (self.own(1, 1), ((z_mate, 2, None), (sibling, 3, None))),
                (self.own(0, 0), ((y_mate, 1, 1), (sibling, 0, None))),
            ),
            (
                (self.far(0, 0), ((y_mate, 4, None), (sibling, 5, None))),
                (self.far(1, 0), ((y_mate, 6, None), (sibling, 7, None))),
            ),
            (
                (self.own(0, 1), ((sibling, 10, None),)),
                (self.far(0, 1), ((sibling, 8, None),)),
                (self.far(1, 1), ((sibling, 9, None),)),
            ),
        )
        return inner, outer

    def stage(self, k, number):
        for role, moves in enumerate(self.table()):
            if not moves[number]:
                continue

            @pl.when(self.outer == role)
            def _():
                for s, targets in moves[number]:
                    self.landed(k, s, self.at[4])
                    for device, slot, lane in targets:
                        copy = self.onward(k, s, device, slot)
                        if lane is None:
                            copy.start()
                        else:
                            pl.when(self.at[4] == lane)(copy.start)

    def complete(self, k):
        other = 1 - self.at[4]
        for s in (
            self.own(1 - self.outer, 0),
            self.own(self.outer, 1),
            self.own(1 - self.outer, 1),
            self.far(0, 0),
            self.far(1, 0),
            self.far(0, 1),
            self.far(1, 1),
        ):
            self.landed(k, s, other)

        @pl.when(jnp.logical_not(self.is_own))
        def _():
            part = self.whole(k, self.mine)
            remote(
                part, part, self.send.at[k, 0], self.beside.at[k], self.sibling()
            ).wait_recv()

    def drain(self, k):
        @pl.when(self.is_own)
        def _():
            for copy in self.own_sends(k):
                copy.wait_send()

        @pl.when(jnp.logical_not(self.is_own))
        def _():
            for copy in self.far_sends(k):
                copy.wait_send()

        for role, moves in enumerate(self.table()):

            @pl.when(self.outer == role)
            def _():
                for number in range(3):
                    for s, targets in moves[number]:
                        for device, slot, lane in targets:
                            copy = self.onward(k, s, device, slot)
                            if lane is None:
                                copy.wait_send()
                            else:
                                pl.when(self.at[4] == lane)(copy.wait_send)


def gather_scratch(units, depth, width, shares, dtype):
    return [
        pltpu.VMEM((units, depth, width), dtype),
        pltpu.VMEM((units, shares * depth, width), dtype),
        pltpu.SemaphoreType.DMA((units,)),
        pltpu.SemaphoreType.DMA((units, 17)),
        pltpu.SemaphoreType.DMA((units, shares, 2)),
        pltpu.SemaphoreType.DMA((units,)),
    ]


class Layer:
    def __init__(self, refs):
        names = (
            "rows",
            "cosine",
            "sine",
            "taps",
            "gain",
            "shift",
            "out",
            "normed",
            "products",
            "keys",
            "queries",
            "within",
            "sending",
            "got",
            "prefix",
            "state",
            "padded",
            "halo_out",
            "halo_in",
            "summed",
            "hidden",
            "kept",
            "sent",
            "crossed",
            "half",
            "here",
            "there",
        )
        for name, ref in zip(names, refs):
            setattr(self, name, ref)
        sems = refs[len(names) :]
        (
            self.rows_send,
            self.rows_arrive,
            self.slice_sems,
            self.prefix_sems,
            self.halo_sems,
            self.out_sems,
        ) = sems
        zh, zl, y, x, c = self.at = place()
        self.count = self.normed.shape[0]
        self.heads = self.keys.shape[1] // KEY
        self.rank = x * 2 + zh
        self.link = (c * 2 + zl) * 2 + y
        self.links = 8
        self.groups = 4

    def chain(self, s):
        zh, zl, y, x, c = self.at
        return (zh, (s // 2) % 2, s % 2, x, s // 4)

    def log_decay(self, head):
        ratio = (self.rank * self.heads + head).astype(jnp.float32) / (
            self.heads * self.groups - 1
        )
        return (math.log(0.05) + ratio * math.log(18.0)) / (self.count * self.links)

    def by_rows(self, size, what):
        def body(n, carry):
            what(pl.multiple_of(n * size, size))
            return carry

        lax.fori_loop(0, self.count // size, body, 0)

    def position(self, first, size):
        rows = lax.broadcasted_iota(jnp.int32, (size, 1), 0) + first
        return rows.astype(jnp.float32)


    def block(self, j):
        share = self.rows.shape[0]
        return self.normed.at[pl.ds(pl.multiple_of(j * share, share), share)]

    def rows_copy(self, dz, dx):
        zh, zl, y, x, c = self.at
        j = x * 2 + c
        to = (1 - zh if dz else zh, zl, y, 1 - x if dx else x, zh)
        return remote(
            self.rows, self.block(j), self.rows_send.at[dz * 2 + dx], self.rows_arrive.at[j], to
        )

    def block_arrived(self, j):
        part = self.block(j)
        remote(
            part, part, self.rows_send.at[0], self.rows_arrive.at[j], self.chain(0)
        ).wait_recv()

    def rows_onward(self, core):
        zh, zl, y, x, c = self.at
        j = x * 2 + core
        part = self.block(j)
        return remote(
            part, part, self.rows_send.at[3 + core], self.rows_arrive.at[j], (zh, zl, y, 1 - x, c)
        )

    def near_rows(self):
        zh, zl, y, x, c = self.at
        j = x * 2 + c
        self.rows_copy(0, 1).start()

        @pl.when(c == zh)
        def _():
            pltpu.make_async_copy(self.rows, self.block(j), self.rows_arrive.at[j]).start()

        @pl.when(c != zh)
        def _():
            self.rows_copy(0, 0).start()

    def relay_rows(self):
        zh, zl, y, x, c = self.at

        @pl.when(c != zh)
        def _():
            for core in range(2):
                self.block_arrived(x * 2 + core)
                self.rows_onward(core).start()

    def all_rows(self):
        zh, zl, y, x, c = self.at
        for j in range(4):
            pl.when(jnp.logical_or(c == zh, x != j // 2))(lambda: self.block_arrived(j))

    def drain_rows(self):
        zh, zl, y, x, c = self.at
        self.rows_copy(0, 1).wait_send()
        self.rows_copy(1, 0).wait_send()

        @pl.when(c != zh)
        def _():
            self.rows_copy(0, 0).wait_send()
            self.rows_onward(0).wait_send()
            self.rows_onward(1).wait_send()


    def project(self, k, weights):
        wide = weights.shape[2] // 2
        for part in range(2):
            columns = pl.ds(part * wide, wide)
            self.products[k, :, columns] = jnp.dot(
                self.normed[...], weights[k, :, columns], preferred_element_type=jnp.float32
            ).astype(self.products.dtype)

    def rotate(self, unit, target, scale):
        wide = KEY // 2

        def rows(first):
            lines = pl.ds(first, 128)
            cosine, sine = self.cosine[lines], self.sine[lines]
            for head in range(self.heads):
                low = pl.ds(head * KEY, wide)
                high = pl.ds(head * KEY + wide, wide)
                front = self.products[unit, lines, low].astype(jnp.float32)
                back = self.products[unit, lines, high].astype(jnp.float32)
                target[lines, low] = ((front * cosine - back * sine) * scale).astype(target.dtype)
                target[lines, high] = ((front * sine + back * cosine) * scale).astype(target.dtype)

        self.by_rows(128, rows)

    def contribute(self, head):
        columns = pl.ds(head * KEY, KEY)
        left = self.count - 1.0 - self.position(0, self.count)
        trailing = jnp.exp(self.log_decay(head) * left)
        weighted = (self.keys[:, columns].astype(jnp.float32) * trailing).astype(jnp.bfloat16)
        total = lax.dot_general(
            weighted,
            self.products[1 + head],
            (((0,), (0,)), ((), ())),
            preferred_element_type=jnp.float32,
        )
        self.sending[pl.ds(head * KEY, KEY)] = total.astype(self.sending.dtype)

    def slice_copy(self, s):
        size = self.got.shape[1]
        part = self.sending.at[pl.ds(s * size, size)]
        return remote(
            part,
            self.got.at[self.link],
            self.slice_sems.at[0, s],
            self.slice_sems.at[1, self.link],
            self.chain(s),
        )

    def prefix_copy(self, s):
        size = self.got.shape[1]
        lines = pl.ds(pl.multiple_of(self.link * size, size), size)
        return remote(
            self.prefix.at[s],
            self.state.at[lines],
            self.prefix_sems.at[0, s],
            self.prefix_sems.at[1, self.link],
            self.chain(s),
        )

    def others(self, what):
        for s in range(self.links):
            pl.when(self.link != s)(lambda: what(s))

    def send_slices(self):
        self.others(lambda s: self.slice_copy(s).start())
        size = self.got.shape[1]
        lines = pl.ds(pl.multiple_of(self.link * size, size), size)
        self.got[self.link] = self.sending[lines]

    def scan(self):
        size = self.got.shape[1]

        def arrived(s):
            part = self.got.at[s]
            remote(
                part, part, self.slice_sems.at[0, s], self.slice_sems.at[1, s], self.chain(s)
            ).wait_recv()

        self.others(arrived)
        step = jnp.exp(
            jnp.full((1, 1), self.log_decay(self.link * size // KEY) * self.count, jnp.float32)
        )
        state = jnp.zeros(self.got.shape[1:], jnp.float32)
        for s in range(self.links):
            self.prefix[s] = state.astype(self.prefix.dtype)
            state = state * step + self.got[s].astype(jnp.float32)
        self.others(lambda s: self.prefix_copy(s).start())
        lines = pl.ds(pl.multiple_of(self.link * size, size), size)
        self.state[lines] = self.prefix[self.link]

    def state_arrived(self):
        size = self.got.shape[1]

        def arrived(s):
            part = self.state.at[pl.ds(s * size, size)]
            remote(
                part, part, self.prefix_sems.at[0, s], self.prefix_sems.at[1, s], self.chain(s)
            ).wait_recv()

        self.others(arrived)

    def inside(self, head):
        columns = pl.ds(head * KEY, KEY)
        decay = self.log_decay(head)

        def rows(first):
            lines = pl.ds(first, 128)
            scores = contract(self.queries[lines, columns], self.keys[:, columns])
            later = lax.broadcasted_iota(jnp.int32, scores.shape, 0) + first
            ahead = later - lax.broadcasted_iota(jnp.int32, scores.shape, 1)
            weight = jnp.exp(decay * jnp.maximum(ahead, 0).astype(jnp.float32))
            scores = jnp.where(ahead >= 0, scores * weight, 0.0).astype(jnp.bfloat16)
            self.within[head, lines] = jnp.dot(
                scores, self.products[1 + head], preferred_element_type=jnp.float32
            )

        self.by_rows(128, rows)

    def finish_head(self, head):
        columns = pl.ds(head * KEY, KEY)
        decay = self.log_decay(head)

        def rows(first):
            lines = pl.ds(first, 128)
            cross = jnp.dot(
                self.queries[lines, columns],
                self.state[pl.ds(head * KEY, KEY)],
                preferred_element_type=jnp.float32,
            )
            leading = jnp.exp(decay * (self.position(first, 128) + 1.0))
            raw = self.within[head, lines] + cross * leading
            average = jnp.mean(raw, axis=-1, keepdims=True)
            centred = raw - average
            wide = jnp.mean(jnp.square(centred), axis=-1, keepdims=True)
            switch = self.products[7 + head, lines].astype(jnp.float32)
            result = centred * lax.rsqrt(wide + group_eps) * jax.nn.silu(switch)
            self.hidden[lines, pl.ds(head * VAL, VAL)] = result.astype(self.hidden.dtype)

        self.by_rows(128, rows)


    def glu(self):
        lead = self.halo_in.shape[0]

        def rows(first):
            lines = pl.ds(first, 128)
            value = self.products[4, lines].astype(jnp.float32)
            switch = self.products[5, lines].astype(jnp.float32)
            gated = (value * jax.nn.sigmoid(switch)).astype(jnp.bfloat16)
            self.padded[pl.ds(pl.multiple_of(first + lead, 8), 128)] = gated.astype(jnp.float32)

        self.by_rows(128, rows)
        self.halo_out[...] = self.padded[pl.ds(self.count, lead)].astype(jnp.bfloat16)
        self.padded[pl.ds(self.count + lead, 8)] = jnp.zeros(
            (8, self.padded.shape[1]), jnp.float32
        )
        pl.when(self.link < self.links - 1)(lambda: self.halo_copy().start())

    def halo_copy(self):
        following = jnp.minimum(self.link + 1, self.links - 1)
        return remote(
            self.halo_out,
            self.halo_in,
            self.halo_sems.at[0],
            self.halo_sems.at[1],
            self.chain(following),
        )

    def convolve(self):
        lead = self.halo_in.shape[0]
        channels = self.padded.shape[1]

        @pl.when(self.link > 0)
        def _():
            self.halo_copy().wait_recv()
            self.padded[pl.ds(0, lead)] = self.halo_in[...].astype(jnp.float32)

        @pl.when(self.link == 0)
        def _():
            self.padded[pl.ds(0, lead)] = jnp.zeros((lead, channels), jnp.float32)

        size = 64
        lanes = 128

        def body(n, carry):
            first = pl.multiple_of(n * size, size)
            for part in range(channels // lanes):
                columns = pl.ds(part * lanes, lanes)
                spot = pl.multiple_of(self.rank * channels + part * lanes, lanes)
                weights = self.taps[:, pl.ds(spot, lanes)]
                source = self.padded[pl.ds(first, size + lead + 8), columns]
                total = None
                for low in range(8):
                    group = None
                    for high in range(lead // 8 + 1):
                        tap = high * 8 + low - (lead - KW + 1)
                        if not 0 <= tap < KW:
                            continue
                        term = source[high * 8 : high * 8 + size + 8] * weights[tap : tap + 1]
                        group = term if group is None else group + term
                    if low:
                        group = pltpu.roll(group, size + 8 - low, 0)
                    total = group[:size] if total is None else total + group[:size]
                self.summed[pl.ds(first, size), columns] = total
            return carry

        lax.fori_loop(0, self.count // size, body, 0)

    def finish_convolution(self):
        channels = self.padded.shape[1]
        spot = pl.ds(pl.multiple_of(self.rank * channels, channels), channels)
        gain, shift = self.gain[:, spot], self.shift[:, spot]

        def rows(first):
            lines = pl.ds(first, 128)
            total = self.summed[lines]
            average = jnp.mean(total, axis=-1, keepdims=True)
            centred = total - average
            wide = jnp.mean(jnp.square(centred), axis=-1, keepdims=True)
            normalized = centred * lax.rsqrt(wide + layer_eps) * gain + shift
            switch = self.products[6, lines].astype(jnp.float32)
            result = jax.nn.silu(normalized) * jax.nn.silu(switch)
            target = pl.ds(self.heads * VAL, channels)
            self.hidden[lines, target] = result.astype(self.hidden.dtype)

        self.by_rows(128, rows)


    def x_copy(self, n):
        zh, zl, y, x, c = self.at
        return remote(
            self.sent.at[n],
            self.crossed.at[n],
            self.out_sems.at[0, n],
            self.out_sems.at[1, n],
            (zh, zl, y, 1 - x, c),
        )

    def near_copy(self, n):
        zh, zl, y, x, c = self.at
        share = self.out.shape[0]
        part = self.half.at[n, pl.ds(pl.multiple_of((1 - c) * share, share), share)]
        return remote(
            part,
            self.here.at[n],
            self.out_sems.at[2, n],
            self.out_sems.at[3, n],
            (zh, zl, y, x, 1 - c),
        )

    def far_copy(self, n, core):
        zh, zl, y, x, c = self.at
        share = self.out.shape[0]
        return remote(
            self.half.at[n, pl.ds(core * share, share)],
            self.there.at[n],
            self.out_sems.at[2 + 2 * core, n],
            self.out_sems.at[5, n],
            (c, zl, y, x, core),
        )

    def multiply(self, j, q, weights):
        x = self.at[3]
        tile = self.sent.shape[2]
        n = j * 4 + q
        pair = self.sent.shape[1]
        total = contract(self.hidden[...], weights[j, pl.ds(q * tile, tile)])
        low, high = total[:pair], total[pair:]
        self.kept[n] = jnp.where(x == 0, low, high)
        self.sent[n] = jnp.where(x == 0, high, low).astype(self.sent.dtype)
        self.x_copy(n).start()

    def join(self, n):
        zh, zl, y, x, c = self.at
        self.x_copy(n).wait_recv()
        total = self.kept[n] + self.crossed[n].astype(jnp.float32)
        self.half[n] = total.astype(self.half.dtype)

        @pl.when(c == zh)
        def _():
            self.near_copy(n).start()

        @pl.when(c != zh)
        def _():
            self.far_copy(n, 0).start()
            self.far_copy(n, 1).start()

    def close(self, j, q):
        zh, zl, y, x, c = self.at
        n = j * 4 + q
        share = self.out.shape[0]
        wide = self.sent.shape[2] // 2
        part = self.there.at[n]
        remote(
            part, part, self.out_sems.at[4, n], self.out_sems.at[5, n], (zh, zl, y, 1 - x, c)
        ).wait_recv()
        far_part = self.there[n].astype(jnp.float32)

        def store(near_part):
            total = (near_part.astype(jnp.float32) + far_part).astype(self.out.dtype)
            for k in range(2):
                spot = ((2 * q + k) * 2 + j) * wide
                self.out[:, pl.ds(spot, wide)] = total[:, k * wide : (k + 1) * wide]

        @pl.when(c == zh)
        def _():
            store(self.half[n, pl.ds(pl.multiple_of(c * share, share), share)])

        @pl.when(c != zh)
        def _():
            self.near_copy(n).wait_recv()
            store(self.here[n])

    def drain(self):
        zh, zl, y, x, c = self.at
        self.drain_rows()
        self.others(lambda s: self.slice_copy(s).wait_send())
        self.others(lambda s: self.prefix_copy(s).wait_send())
        pl.when(self.link < self.links - 1)(lambda: self.halo_copy().wait_send())
        for n in range(self.sent.shape[0]):
            self.x_copy(n).wait_send()

            @pl.when(c == zh)
            def _():
                self.near_copy(n).wait_send()

            @pl.when(c != zh)
            def _():
                self.far_copy(n, 0).wait_send()
                self.far_copy(n, 1).wait_send()


def layer_kernel(layout, out_layout, *refs):
    blocks, refs = refs[:9], refs[9:]
    first_gather, refs = refs[-12:-6], refs[:-12] + refs[-6:]
    second_gather, refs = refs[-6:], refs[:-6]
    layer = Layer(refs)
    inward, outward = Gather(*first_gather), Gather(*second_gather)
    units = len(layout)
    total = units + 2

    layer.near_rows()
    for k, (which, first) in enumerate(layout):
        inward.load(k, blocks[which].at[:, pl.ds(first, inward.source.shape[2])], None)
    for k, parts in enumerate(out_layout):
        for which, row, column in parts:
            ref = blocks[which]
            lines = pl.ds(row, outward.depth)
            outward.load(k, ref.at[lines], pl.ds(column, ref.shape[1]))

    for k in range(AHEAD):
        inward.begin(k)
        if k == ROWS_AFTER:
            layer.rows_copy(1, 0).start()

    def at_unit(k, what):
        @pl.when(jnp.logical_and(k >= 0, k < units))
        def _():
            what(inward, k)

        @pl.when(jnp.logical_and(k >= units, k < total))
        def _():
            what(outward, k - units)

    after = (
        (lambda: layer.rotate(0, layer.keys, KEY ** (-0.5)),),
        (lambda: layer.contribute(0),),
        (lambda: layer.contribute(1), layer.send_slices),
        (lambda: layer.rotate(3, layer.queries, 1.0), layer.scan),
        (lambda: layer.inside(0),),
        (layer.glu, lambda: layer.inside(1)),
        (layer.convolve,),
        (layer.finish_convolution, layer.state_arrived, lambda: layer.finish_head(0)),
        (lambda: layer.finish_head(1),),
    )

    def step(i, carry):
        for number in range(3):
            at_unit(i - LAGS[number], lambda gather, k: gather.stage(k, number))
        at_unit(i + AHEAD, lambda gather, k: gather.begin(k))
        pl.when(i == ROWS_RELAY)(layer.relay_rows)
        done = i - LAGS[3]
        pl.when(done == 0)(layer.all_rows)

        @pl.when(jnp.logical_and(done >= 0, done < units))
        def _():
            inward.complete(done)
            layer.project(done, inward.full)

        for k, events in enumerate(after):

            @pl.when(done == k)
            def _():
                for event in events:
                    event()

        return carry

    lax.fori_loop(0, units + LAGS[3], step, 0)

    def output(j):
        outward.complete(j)
        for q in range(4):
            layer.multiply(j, q, outward.full)

    def late_stages(j):
        for number in range(3):
            if units + j + LAGS[number] >= units + LAGS[3]:
                outward.stage(j, number)

    late_stages(0)
    output(0)
    late_stages(1)
    for n in range(4):
        layer.join(n)
    output(1)
    for q in range(4):
        layer.close(0, q)
    for n in range(4, 8):
        layer.join(n)
    for q in range(4):
        layer.close(1, q)

    def finish(gather):
        def body(k, carry):
            gather.drain(k)
            return carry

        lax.fori_loop(0, gather.source.shape[0], body, 0)

    finish(inward)
    finish(outward)
    layer.drain()


def whole_layer(rows, cosine, sine, taps, gain, shift, blocks):
    depth, width = blocks[0].shape
    share, model = rows.shape
    layout = []
    for which, block in enumerate(blocks[:7]):
        layout += [(which, first) for first in range(0, block.shape[1], width)]
    units = len(layout)
    shares, dtype = 8, rows.dtype
    span = 4 * share
    inner_width = blocks[7].shape[1] + blocks[8].shape[1]
    half_depth = depth // 2
    out_layout = [
        ((7, j * half_depth, 0), (8, j * half_depth, blocks[7].shape[1])) for j in range(2)
    ]
    heads = width // KEY
    channels = blocks[8].shape[1]
    lead = (KW + 7) // 8 * 8
    tile = 2 * half_depth
    tiles = model // tile
    sem = pltpu.SemaphoreType.DMA
    slice_rows = heads * KEY // shares
    return pl.pallas_call(
        lambda *refs: layer_kernel(layout, out_layout, *refs),
        out_shape=jax.ShapeDtypeStruct((share, model), dtype),
        in_specs=[pl.BlockSpec(memory_space=pl.ANY)] * 10
        + [pl.BlockSpec(memory_space=pltpu.VMEM)] * 5,
        out_specs=pl.BlockSpec(memory_space=pltpu.VMEM),
        scratch_shapes=[
            pltpu.VMEM((span, model), dtype),
            pltpu.VMEM((units, span, width), dtype),
            pltpu.VMEM((span, width), dtype),
            pltpu.VMEM((span, width), dtype),
            pltpu.VMEM((heads, span, VAL), jnp.float32),
            pltpu.VMEM((heads * KEY, VAL), dtype),
            pltpu.VMEM((shares, slice_rows, VAL), dtype),
            pltpu.VMEM((shares, slice_rows, VAL), dtype),
            pltpu.VMEM((heads * KEY, VAL), dtype),
            pltpu.VMEM((span + lead + 8, channels), jnp.float32),
            pltpu.VMEM((lead, channels), dtype),
            pltpu.VMEM((lead, channels), dtype),
            pltpu.VMEM((span, channels), jnp.float32),
            pltpu.VMEM((span, inner_width), dtype),
            pltpu.VMEM((tiles, 2 * share, tile), jnp.float32),
            pltpu.VMEM((tiles, 2 * share, tile), dtype),
            pltpu.VMEM((tiles, 2 * share, tile), dtype),
            pltpu.VMEM((tiles, 2 * share, tile), dtype),
            pltpu.VMEM((tiles, share, tile), dtype),
            pltpu.VMEM((tiles, share, tile), dtype),
            sem((5,)),
            sem((4,)),
            sem((2, shares)),
            sem((2, shares)),
            sem((2,)),
            sem((6, tiles)),
        ]
        + gather_scratch(units, depth, width, shares, dtype)
        + gather_scratch(2, half_depth, inner_width, shares, dtype),
        compiler_params=pltpu.CompilerParams(has_side_effects=True, vmem_limit_bytes=60 << 20),
        name="layer",
    )(*blocks, rows, cosine, sine, taps, gain, shift)


def local_squares(
    tokens,
    norm_gain,
    query_weight,
    key_weight,
    value_weight,
    retain_gate,
    unit_value,
    unit_gate,
    convolve_gate,
    filter_taps,
    layer_gain,
    layer_shift,
    retain_output,
    convolve_output,
):
    chain_rank = lax.axis_index(CHAIN)
    normed = rms_normalize(tokens, norm_gain)
    row_count = normed.shape[0] * 4
    half_width = KEY // 2
    frequency = rope_base ** (-jnp.arange(half_width, dtype=jnp.float32) / half_width)
    positions = chain_rank * row_count + jnp.arange(row_count, dtype=jnp.int32)
    angles = positions.astype(jnp.float32)[:, None] * frequency
    blocks = (key_weight, value_weight, query_weight, unit_value, unit_gate, convolve_gate)
    blocks += (retain_gate, retain_output, convolve_output)
    return whole_layer(
        normed,
        jnp.cos(angles),
        jnp.sin(angles),
        filter_taps,
        layer_gain[None],
        layer_shift[None],
        blocks,
    )


def squares(mesh):
    boxes = Mesh(mesh.devices.reshape(2, 2, 2, 2, 2), SQUARE)
    rows, blocks = P(SQUARE, None), P(("zh", "zl", "y"), ("x", "c"))
    return jax.shard_map(
        local_squares,
        mesh=boxes,
        in_specs=(rows, P()) + (blocks,) * 7 + (P(),) * 3 + (blocks,) * 2,
        out_specs=rows,
        check_vma=False,
    )


def solution(mesh):
    sp, tp = mesh.shape["sp"], mesh.shape["tp"]
    if (sp, tp) == (8, 4):
        return squares(mesh)
    planes = Mesh(mesh.devices.reshape(tp, sp // tp, tp), ("hi", "lo", "tp"))
    return jax.shard_map(
        local,
        mesh=planes,
        in_specs=(
            P(("hi", "lo", "tp"), None),
            P(),
            P(("hi", "lo"), "tp"),
            P(("hi", "lo"), "tp"),
            P(("hi", "lo"), "tp"),
            P(("hi", "lo"), "tp"),
            P(("hi", "lo"), "tp"),
            P(("hi", "lo"), "tp"),
            P(("hi", "lo"), "tp"),
            P(),
            P(),
            P(),
            P(("hi", "lo"), "tp"),
            P(("hi", "lo"), "tp"),
        ),
        out_specs=P(("hi", "lo", "tp"), None),
        check_vma=False,
    )
```

```python
import math

import jax
import jax.numpy as jnp
import numpy as np
from jax import lax
from jax.experimental import pallas as pl
from jax.experimental.pallas import tpu as pltpu
from jax.sharding import Mesh
from jax.sharding import PartitionSpec as P

KEY = 256
VAL = 512
GROUP = 512
KW = 31


rms_eps = 1e-06
group_eps = 1.0
layer_eps = 0.001
rope_base = 10000.0


SPANS = ("tp", "lo")


def swap_planes(x):
    size = lax.axis_size("tp")
    pairs = [(h * size + t, t * size + h) for h in range(size) for t in range(size)]
    return lax.ppermute(x, ("hi", "tp"), pairs)


def from_behind(x, by):
    outer, inner = lax.axis_size("tp"), lax.axis_size("lo")
    spot = [(i % inner) * outer + i // inner for i in range(outer * inner)]
    return lax.ppermute(x, ("lo", "tp"), list(zip(spot[:-by], spot[by:])))


def carried_in(contribution, log_span_decay):
    length = lax.axis_size(SPANS)
    state = from_behind(contribution.astype(jnp.bfloat16), 1).astype(jnp.float32)
    by = 1
    while by < length:
        earlier = from_behind(state.astype(jnp.bfloat16), by).astype(jnp.float32)
        state = state + jnp.exp(log_span_decay * by)[:, None, None] * earlier
        by *= 2
    return state


def rms_normalize(tokens, norm_gain):
    widened = tokens.astype(jnp.float32)
    scaled = widened * lax.rsqrt(jnp.mean(widened * widened, axis=-1, keepdims=True) + rms_eps)
    return (scaled * norm_gain).astype(jnp.bfloat16)


def rotate(vectors, positions):
    half_width = vectors.shape[-1] // 2
    frequency = rope_base ** (-jnp.arange(half_width, dtype=jnp.float32) / half_width)
    angles = positions.astype(jnp.float32)[:, None] * frequency
    cosine = jnp.cos(angles)[:, None, :]
    sine_part = jnp.sin(angles)[:, None, :]
    front_half = vectors[..., :half_width]
    back_half = vectors[..., half_width:]
    return jnp.concatenate(
        [front_half * cosine - back_half * sine_part, front_half * sine_part + back_half * cosine],
        axis=-1,
    )


def prepare(queries, key_rows, values, positions):
    row_count = queries.shape[0]
    rotated_query = rotate(
        queries.astype(jnp.float32).reshape(row_count, -1, KEY), positions
    ).astype(jnp.bfloat16)
    rotated_keys = (
        rotate(key_rows.astype(jnp.float32).reshape(row_count, -1, KEY), positions) * KEY ** (-0.5)
    ).astype(jnp.bfloat16)
    value_heads = values.reshape(row_count, -1, VAL)
    return (rotated_query, rotated_keys, value_heads)


def decay_logs(first_head, head_total, all_heads, seq_length):
    ratio = (first_head + jnp.arange(head_total)).astype(jnp.float32) / (all_heads - 1)
    return (jnp.log(0.05) + ratio * jnp.log(18.0)) / seq_length


def local_parts(queries, key_rows, values, log_decay):
    row_count = queries.shape[0]
    indices = jnp.arange(row_count, dtype=jnp.float32)
    offsets = indices[:, None] - indices[None, :]
    causal = offsets >= 0
    weight = jnp.where(
        causal[None], jnp.exp(log_decay[:, None, None] * jnp.where(causal, offsets, 0.0)[None]), 0.0
    )
    scores = (
        jnp.einsum("ihd,jhd->hij", queries, key_rows, preferred_element_type=jnp.float32) * weight
    ).astype(jnp.bfloat16)
    within = jnp.einsum("hij,jhe->ihe", scores, values, preferred_element_type=jnp.float32)
    trailing = jnp.exp(log_decay[None, :] * (row_count - 1.0 - indices)[:, None])
    weighted = (key_rows.astype(jnp.float32) * trailing[:, :, None]).astype(jnp.bfloat16)
    contribution = jnp.einsum("jhd,jhe->hde", weighted, values, preferred_element_type=jnp.float32)
    return (within, contribution)


def cross_part(queries, carry_state, log_decay):
    row_count = queries.shape[0]
    indices = jnp.arange(row_count, dtype=jnp.float32)
    leading = jnp.exp(log_decay[None, :] * (indices + 1.0)[:, None])
    return (
        jnp.einsum(
            "ihd,hde->ihe",
            queries,
            carry_state.astype(jnp.bfloat16),
            preferred_element_type=jnp.float32,
        )
        * leading[:, :, None]
    )


def retain_finish(raw, switch):
    average = jnp.mean(raw, axis=-1, keepdims=True)
    spread = jnp.mean(jnp.square(raw - average), axis=-1, keepdims=True)
    normalized = ((raw - average) * lax.rsqrt(spread + group_eps)).reshape(raw.shape[0], -1)
    return (normalized * jax.nn.silu(switch.astype(jnp.float32))).astype(jnp.bfloat16)


def convolve_branch(gated_input, before, tap_slice, gain_slice, shift_slice, switch):
    padded = jnp.concatenate([before, gated_input], axis=0)
    row_count = gated_input.shape[0]
    summed = jnp.zeros(gated_input.shape, jnp.float32)
    for tap_index in range(tap_slice.shape[0]):
        summed = (
            summed
            + padded[tap_index : tap_index + row_count].astype(jnp.float32) * tap_slice[tap_index]
        )
    grouped = summed.reshape(row_count, -1, GROUP)
    average = jnp.mean(grouped, axis=-1, keepdims=True)
    spread = jnp.mean(jnp.square(grouped - average), axis=-1, keepdims=True)
    normalized = ((grouped - average) * lax.rsqrt(spread + layer_eps)).reshape(row_count, -1)
    normalized = normalized * gain_slice + shift_slice
    return (jax.nn.silu(normalized) * jax.nn.silu(switch.astype(jnp.float32))).astype(jnp.bfloat16)


def contract(hidden, matrix):
    return lax.dot_general(
        hidden, matrix, (((1,), (1,)), ((), ())), preferred_element_type=jnp.float32
    )


def local(
    tokens,
    norm_gain,
    query_weight,
    key_weight,
    value_weight,
    retain_gate,
    unit_value,
    unit_gate,
    convolve_gate,
    filter_taps,
    layer_gain,
    layer_shift,
    retain_output,
    convolve_output,
):
    head_groups = lax.axis_size("hi")
    chain_length = lax.axis_size(SPANS)
    head_rank = lax.axis_index("hi")
    chain_rank = lax.axis_index(SPANS)
    def project(rows, merged, *matrices):
        product = jnp.dot(rows, merged, preferred_element_type=jnp.float32).astype(jnp.bfloat16)
        ends = [sum(m.shape[1] for m in matrices[: k + 1]) for k in range(len(matrices) - 1)]
        return jnp.split(product, ends, axis=1)

    first = (key_weight, value_weight, query_weight)
    second = (unit_value, unit_gate, convolve_gate, retain_gate)
    third = (retain_output, convolve_output)
    groups = (first, second, third)
    merged = [jnp.concatenate(group, axis=1) for group in groups]
    normed = rms_normalize(tokens, norm_gain)
    normed = lax.all_gather(swap_planes(normed), "hi", axis=0, tiled=True)
    merged = [lax.all_gather(swap_planes(m), SPANS, axis=0, tiled=True) for m in merged]
    key_rows, values, queries = project(normed, merged[0], *first)
    glu_value, glu_switch, convolve_switch, retain_switch = project(normed, merged[1], *second)
    out_full = merged[2]
    row_count = normed.shape[0]
    local_heads = queries.shape[1] // KEY
    positions = chain_rank * row_count + jnp.arange(row_count, dtype=jnp.int32)
    rotated_query, rotated_keys, value_heads = prepare(queries, key_rows, values, positions)
    log_decay = decay_logs(
        head_rank * local_heads, local_heads, local_heads * head_groups, row_count * chain_length
    )
    within, contribution = local_parts(rotated_query, rotated_keys, value_heads, log_decay)
    gated_input = (
        glu_value.astype(jnp.float32) * jax.nn.sigmoid(glu_switch.astype(jnp.float32))
    ).astype(jnp.bfloat16)
    channels = gated_input.shape[1]
    before = from_behind(gated_input[row_count - (KW - 1) :], 1)
    incoming = carried_in(contribution, log_decay * row_count)
    raw = within + cross_part(rotated_query, incoming, log_decay)
    retain_hidden = retain_finish(raw, retain_switch)
    tap_slice = lax.dynamic_slice_in_dim(filter_taps, head_rank * channels, channels, 1)
    gain_slice = lax.dynamic_slice_in_dim(layer_gain, head_rank * channels, channels, 0)
    shift_slice = lax.dynamic_slice_in_dim(layer_shift, head_rank * channels, channels, 0)
    convolve_hidden = convolve_branch(
        gated_input, before, tap_slice, gain_slice, shift_slice, convolve_switch
    )
    hidden = jnp.concatenate([retain_hidden, convolve_hidden], axis=1)
    mixed = contract(hidden, out_full).astype(jnp.bfloat16)
    return swap_planes(lax.psum_scatter(mixed, "hi", scatter_dimension=0, tiled=True))


OWN_AHEAD = 4
FAR_AHEAD = 2
LEADS = (1, 1, 0, -1, 0)
STRIPS = 4
ROWS_RELAY = 1
START = 4
BEHIND = 1
MESH = pl.DeviceIdType.MESH
SQUARE = ("zh", "zl", "y", "x", "c")
CHAIN = ("c", "zl", "y")


def remote(source, target, out_sem, in_sem, device):
    return pltpu.make_async_remote_copy(
        src_ref=source,
        dst_ref=target,
        send_sem=out_sem,
        recv_sem=in_sem,
        device_id=device,
        device_id_type=MESH,
    )


def place():
    return tuple(lax.axis_index(name) for name in SQUARE)


class Gather:
    def __init__(self, source, full, near, send, arrive, beside):
        self.source, self.full, self.near = source, full, near
        self.send, self.arrive, self.beside = send, arrive, beside
        zh, zl, y, x, c = self.at = place()
        self.depth = source.shape[1]
        self.half = self.depth // 2
        self.outer = zl * zh + (1 - zl) * (1 - zh)
        self.mine = self.index(zh, self.outer, y)
        self.is_own = c == zh

    def index(self, zh, outer, y):
        zl = outer * zh + (1 - outer) * (1 - zh)
        return (zh * 2 + zl) * 2 + y

    def own(self, outer, flip):
        return self.index(self.at[0], outer, self.at[2] if not flip else 1 - self.at[2])

    def far(self, outer, flip):
        return self.index(1 - self.at[0], outer, self.at[2] if not flip else 1 - self.at[2])

    def rows(self, k, s, half):
        start = pl.multiple_of(s * self.depth + half * self.half, self.half)
        return self.full.at[k, pl.ds(start, self.half)]

    def whole(self, k, s):
        return self.full.at[k, pl.ds(pl.multiple_of(s * self.depth, self.depth), self.depth)]

    def z_mate(self, core):
        zh, zl, y, x, c = self.at
        return (zh, 1 - zl, y, x, core)

    def y_mate(self, core):
        zh, zl, y, x, c = self.at
        return (zh, zl, 1 - y, x, core)

    def sibling(self):
        zh, zl, y, x, c = self.at
        return (zh, zl, y, x, 1 - c)

    def load(self, k, part, columns):
        columns = pl.ds(0, self.source.shape[2]) if columns is None else columns

        @pl.when(self.is_own)
        def _():
            target = self.whole(k, self.mine).at[:, columns]
            pltpu.make_async_copy(part, target, self.near.at[k]).start()

        @pl.when(jnp.logical_not(self.is_own))
        def _():
            target = self.source.at[k].at[:, columns]
            pltpu.make_async_copy(part, target, self.near.at[k]).start()

    def own_sends(self, k):
        zh, zl, y, x, c = self.at
        part = self.whole(k, self.mine)
        copies = [remote(part, part, self.send.at[k, 16], self.beside.at[k], self.sibling())]
        for r in range(2):
            piece = self.rows(k, self.mine, r)
            arrive = self.arrive.at[k, self.mine, r]
            copies.append(remote(piece, piece, self.send.at[k, 12 + r], arrive, self.z_mate(r)))
            copies.append(remote(piece, piece, self.send.at[k, 14 + r], arrive, self.y_mate(r)))
        return copies

    def far_sends(self, k):
        zh, zl, y, x, c = self.at
        copies = []
        for r in range(2):
            piece = self.source.at[k, pl.ds(r * self.half, self.half)]
            copies.append(
                remote(
                    piece,
                    self.rows(k, self.mine, r),
                    self.send.at[k, 12 + r],
                    self.arrive.at[k, self.mine, r],
                    (c, 1 - c, y, x, r),
                )
            )
        return copies

    def begin(self, k, own):
        pltpu.make_async_copy(self.source.at[k], self.source.at[k], self.near.at[k]).wait()
        for copy in self.own_sends(k) if own else self.far_sends(k):
            copy.start()

    def onward(self, k, s, device, slot):
        piece = self.rows(k, s, self.at[4])
        return remote(piece, piece, self.send.at[k, slot], self.arrive.at[k, s, self.at[4]], device)

    def landed(self, k, s, half):
        piece = self.rows(k, s, half)
        remote(
            piece, piece, self.send.at[k, 0], self.arrive.at[k, s, half], self.sibling()
        ).wait_recv()

    def table(self):
        c = self.at[4]
        z_mate, y_mate, sibling = self.z_mate(c), self.y_mate(c), self.sibling()
        inner = (
            (
                (self.far(0, 0), ((z_mate, 0, None), (y_mate, 1, None), (sibling, 2, None))),
                (self.far(1, 0), ((z_mate, 3, None), (y_mate, 4, None), (sibling, 5, None))),
            ),
            (
                (self.own(0, 1), ((z_mate, 8, 0), (sibling, 7, None))),
                (self.own(1, 0), ((sibling, 6, None),)),
            ),
            (
                (self.far(0, 1), ((sibling, 9, None),)),
                (self.far(1, 1), ((sibling, 10, None),)),
            ),
            (),
            ((self.own(1, 1), ((sibling, 11, None),)),),
        )
        outer = (
            (),
            (
                (self.own(1, 1), ((z_mate, 2, None), (sibling, 3, None))),
                (self.own(0, 0), ((y_mate, 1, 1), (sibling, 0, None))),
            ),
            (
                (self.far(0, 0), ((y_mate, 4, None), (sibling, 5, None))),
                (self.far(1, 0), ((y_mate, 6, None), (sibling, 7, None))),
            ),
            (
                (self.far(0, 1), ((sibling, 8, None),)),
                (self.far(1, 1), ((sibling, 9, None),)),
            ),
            ((self.own(0, 1), ((sibling, 10, None),)),),
        )
        return inner, outer

    def stage(self, k, number):
        for role, moves in enumerate(self.table()):
            if not moves[number]:
                continue

            @pl.when(self.outer == role)
            def _():
                for s, targets in moves[number]:
                    self.landed(k, s, self.at[4])
                    for device, slot, lane in targets:
                        copy = self.onward(k, s, device, slot)
                        if lane is None:
                            copy.start()
                        else:
                            pl.when(self.at[4] == lane)(copy.start)

    def complete_own(self, k):
        other = 1 - self.at[4]
        for outer, flip in ((1 - self.outer, 0), (self.outer, 1), (1 - self.outer, 1)):
            self.landed(k, self.own(outer, flip), other)

        @pl.when(jnp.logical_not(self.is_own))
        def _():
            part = self.whole(k, self.mine)
            remote(
                part, part, self.send.at[k, 0], self.beside.at[k], self.sibling()
            ).wait_recv()

    def complete_far(self, k):
        other = 1 - self.at[4]
        for outer, flip in ((0, 0), (1, 0), (0, 1), (1, 1)):
            self.landed(k, self.far(outer, flip), other)

    def drain(self, k):
        @pl.when(self.is_own)
        def _():
            for copy in self.own_sends(k):
                copy.wait_send()

        @pl.when(jnp.logical_not(self.is_own))
        def _():
            for copy in self.far_sends(k):
                copy.wait_send()

        for role, moves in enumerate(self.table()):

            @pl.when(self.outer == role)
            def _():
                for number in range(len(moves)):
                    for s, targets in moves[number]:
                        for device, slot, lane in targets:
                            copy = self.onward(k, s, device, slot)
                            if lane is None:
                                copy.wait_send()
                            else:
                                pl.when(self.at[4] == lane)(copy.wait_send)


def gather_scratch(units, depth, width, shares, dtype):
    return [
        pltpu.VMEM((units, depth, width), dtype),
        pltpu.VMEM((units, shares * depth, width), dtype),
        pltpu.SemaphoreType.DMA((units,)),
        pltpu.SemaphoreType.DMA((units, 17)),
        pltpu.SemaphoreType.DMA((units, shares, 2)),
        pltpu.SemaphoreType.DMA((units,)),
    ]


class Layer:
    def __init__(self, refs):
        names = (
            "tokens_in",
            "angles_in",
            "turns",
            "taps_in",
            "norm_gain",
            "gain",
            "shift",
            "out",
            "tokens",
            "angles",
            "taps",
            "rows",
            "cosine",
            "sine",
            "normed",
            "products",
            "keys",
            "queries",
            "within",
            "sending",
            "got",
            "prefix",
            "state",
            "padded",
            "halo_out",
            "halo_in",
            "summed",
            "hidden",
            "kept",
            "sent",
            "crossed",
            "half",
            "here",
            "there",
        )
        for name, ref in zip(names, refs):
            setattr(self, name, ref)
        sems = refs[len(names) :]
        (
            self.rows_send,
            self.rows_arrive,
            self.slice_sems,
            self.prefix_sems,
            self.halo_sems,
            self.out_sems,
            self.load_sems,
        ) = sems
        zh, zl, y, x, c = self.at = place()
        self.count = self.normed.shape[0]
        self.heads = self.keys.shape[1] // KEY
        self.rank = x * 2 + zh
        self.link = (c * 2 + zl) * 2 + y
        self.links = 8
        self.groups = 4

    def chain(self, s):
        zh, zl, y, x, c = self.at
        return (zh, (s // 2) % 2, s % 2, x, s // 4)

    def log_decay(self, head):
        ratio = (self.rank * self.heads + head).astype(jnp.float32) / (
            self.heads * self.groups - 1
        )
        return (math.log(0.05) + ratio * math.log(18.0)) / (self.count * self.links)

    def by_rows(self, what, slot=0, slots=1, size=128):
        steps = self.count // size // slots

        def body(n, carry):
            what(pl.multiple_of(n * size, size))
            return carry

        lax.fori_loop(slot * steps, (slot + 1) * steps, body, 0)

    def position(self, first, size):
        rows = lax.broadcasted_iota(jnp.int32, (size, 1), 0) + first
        return rows.astype(jnp.float32)


    def block(self, j):
        share = self.rows.shape[0]
        return self.normed.at[pl.ds(pl.multiple_of(j * share, share), share)]

    def strip(self, j, t):
        share = self.rows.shape[0]
        size = share // STRIPS
        return self.normed.at[pl.ds(pl.multiple_of(j * share + t * size, size), size)]

    def near_copy_of_rows(self, dx):
        zh, zl, y, x, c = self.at
        j = x * 2 + c
        return remote(
            self.rows,
            self.block(j),
            self.rows_send.at[dx],
            self.rows_arrive.at[j, 0],
            (zh, zl, y, 1 - x if dx else x, zh),
        )

    def far_strip(self, t):
        zh, zl, y, x, c = self.at
        j = x * 2 + c
        size = self.rows.shape[0] // STRIPS
        return remote(
            self.rows.at[pl.ds(pl.multiple_of(t * size, size), size)],
            self.strip(j, t),
            self.rows_send.at[2 + t],
            self.rows_arrive.at[j, t],
            (1 - zh, zl, y, x, zh),
        )

    def onward_strip(self, core, t):
        zh, zl, y, x, c = self.at
        j = x * 2 + core
        return remote(
            self.strip(j, t),
            self.strip(j, t),
            self.rows_send.at[2 + (1 + core) * STRIPS + t],
            self.rows_arrive.at[j, t],
            (zh, zl, y, 1 - x, c),
        )

    def rows_landed(self, part, j, t):
        remote(part, part, self.rows_send.at[0], self.rows_arrive.at[j, t], self.chain(0)).wait_recv()

    def load(self, n):
        source = (self.tokens_in, self.angles_in, self.taps_in)[n]
        target = (self.tokens, self.angles, self.taps)[n]
        return pltpu.make_async_copy(source, target, self.load_sems.at[n])

    def near_rows(self):
        zh, zl, y, x, c = self.at
        j = x * 2 + c
        share = self.rows.shape[0]
        self.load(0).wait()
        tokens = self.tokens[...].astype(jnp.float32)
        scaled = tokens * lax.rsqrt(jnp.mean(tokens * tokens, axis=-1, keepdims=True) + rms_eps)
        self.rows[...] = (scaled * self.norm_gain[...]).astype(self.rows.dtype)

        @pl.when(c == zh)
        def _():
            self.normed[pl.ds(pl.multiple_of(j * share, share), share)] = self.rows[...]

        self.near_copy_of_rows(1).start()
        pl.when(c != zh)(lambda: self.near_copy_of_rows(0).start())

    def tables(self):
        self.load(1).wait()
        self.load(2).wait()
        turn_cosine = self.turns[0, pl.ds(self.link, 1)]
        turn_sine = self.turns[1, pl.ds(self.link, 1)]
        cosine, sine = self.angles[0], self.angles[1]
        self.cosine[...] = cosine * turn_cosine - sine * turn_sine
        self.sine[...] = sine * turn_cosine + cosine * turn_sine

    def relay_rows(self, t):
        zh, zl, y, x, c = self.at

        @pl.when(c != zh)
        def _():
            for core in range(2):
                j = x * 2 + core
                self.rows_landed(self.strip(j, t), j, t)
                self.onward_strip(core, t).start()

    def all_rows(self):
        zh, zl, y, x, c = self.at

        @pl.when(c == zh)
        def _():
            for j in range(4):
                pl.when(x * 2 + c != j)(lambda: self.rows_landed(self.block(j), j, 0))

        @pl.when(c != zh)
        def _():
            for core in range(2):
                for t in range(STRIPS):
                    j = (1 - x) * 2 + core
                    self.rows_landed(self.strip(j, t), j, t)

    def drain_rows(self):
        zh, zl, y, x, c = self.at
        self.near_copy_of_rows(1).wait_send()
        for t in range(STRIPS):
            self.far_strip(t).wait_send()

        @pl.when(c != zh)
        def _():
            self.near_copy_of_rows(0).wait_send()
            for core in range(2):
                for t in range(STRIPS):
                    self.onward_strip(core, t).wait_send()


    def project(self, k, weights, part, parts):
        wide = weights.shape[2] // parts
        columns = pl.ds(part * wide, wide)
        self.products[k, :, columns] = jnp.dot(
            self.normed[...], weights[k, :, columns], preferred_element_type=jnp.float32
        ).astype(self.products.dtype)

    def rotate(self, unit, target, scale, slot, slots):
        wide = KEY // 2

        def rows(first):
            lines = pl.ds(first, 128)
            cosine, sine = self.cosine[lines], self.sine[lines]
            for head in range(self.heads):
                low = pl.ds(head * KEY, wide)
                high = pl.ds(head * KEY + wide, wide)
                front = self.products[unit, lines, low].astype(jnp.float32)
                back = self.products[unit, lines, high].astype(jnp.float32)
                target[lines, low] = ((front * cosine - back * sine) * scale).astype(target.dtype)
                target[lines, high] = ((front * sine + back * cosine) * scale).astype(target.dtype)

        self.by_rows(rows, slot, slots)

    def contribute(self, head):
        columns = pl.ds(head * KEY, KEY)
        left = self.count - 1.0 - self.position(0, self.count)
        trailing = jnp.exp(self.log_decay(head) * left)
        weighted = (self.keys[:, columns].astype(jnp.float32) * trailing).astype(jnp.bfloat16)
        total = lax.dot_general(
            weighted,
            self.products[1 + head],
            (((0,), (0,)), ((), ())),
            preferred_element_type=jnp.float32,
        )
        self.sending[pl.ds(head * KEY, KEY)] = total.astype(self.sending.dtype)

    def slice_copy(self, s):
        size = self.got.shape[1]
        part = self.sending.at[pl.ds(s * size, size)]
        return remote(
            part,
            self.got.at[self.link],
            self.slice_sems.at[0, s],
            self.slice_sems.at[1, self.link],
            self.chain(s),
        )

    def prefix_copy(self, s):
        size = self.got.shape[1]
        lines = pl.ds(pl.multiple_of(self.link * size, size), size)
        return remote(
            self.prefix.at[s],
            self.state.at[lines],
            self.prefix_sems.at[0, s],
            self.prefix_sems.at[1, self.link],
            self.chain(s),
        )

    def others(self, what):
        for s in range(self.links):
            pl.when(self.link != s)(lambda: what(s))

    def send_slices(self):
        self.others(lambda s: self.slice_copy(s).start())
        size = self.got.shape[1]
        lines = pl.ds(pl.multiple_of(self.link * size, size), size)
        self.got[self.link] = self.sending[lines]

    def scan(self):
        size = self.got.shape[1]

        def arrived(s):
            part = self.got.at[s]
            remote(
                part, part, self.slice_sems.at[0, s], self.slice_sems.at[1, s], self.chain(s)
            ).wait_recv()

        self.others(arrived)
        step = jnp.exp(
            jnp.full((1, 1), self.log_decay(self.link * size // KEY) * self.count, jnp.float32)
        )
        state = jnp.zeros(self.got.shape[1:], jnp.float32)
        for s in range(self.links):
            self.prefix[s] = state.astype(self.prefix.dtype)
            state = state * step + self.got[s].astype(jnp.float32)
        self.others(lambda s: self.prefix_copy(s).start())
        lines = pl.ds(pl.multiple_of(self.link * size, size), size)
        self.state[lines] = self.prefix[self.link]

    def state_arrived(self):
        size = self.got.shape[1]

        def arrived(s):
            part = self.state.at[pl.ds(s * size, size)]
            remote(
                part, part, self.prefix_sems.at[0, s], self.prefix_sems.at[1, s], self.chain(s)
            ).wait_recv()

        self.others(arrived)

    def inside(self, head, slot, slots):
        columns = pl.ds(head * KEY, KEY)
        decay = self.log_decay(head)

        def rows(first):
            lines = pl.ds(first, 128)
            scores = contract(self.queries[lines, columns], self.keys[:, columns])
            later = lax.broadcasted_iota(jnp.int32, scores.shape, 0) + first
            ahead = later - lax.broadcasted_iota(jnp.int32, scores.shape, 1)
            weight = jnp.exp(decay * jnp.maximum(ahead, 0).astype(jnp.float32))
            scores = jnp.where(ahead >= 0, scores * weight, 0.0).astype(jnp.bfloat16)
            self.within[head, lines] = jnp.dot(
                scores, self.products[1 + head], preferred_element_type=jnp.float32
            )

        self.by_rows(rows, slot, slots)

    def finish_head(self, head, slot, slots):
        columns = pl.ds(head * KEY, KEY)
        decay = self.log_decay(head)

        def rows(first):
            lines = pl.ds(first, 128)
            cross = jnp.dot(
                self.queries[lines, columns],
                self.state[pl.ds(head * KEY, KEY)],
                preferred_element_type=jnp.float32,
            )
            leading = jnp.exp(decay * (self.position(first, 128) + 1.0))
            raw = self.within[head, lines] + cross * leading
            average = jnp.mean(raw, axis=-1, keepdims=True)
            centred = raw - average
            wide = jnp.mean(jnp.square(centred), axis=-1, keepdims=True)
            switch = self.products[7 + head, lines].astype(jnp.float32)
            result = centred * lax.rsqrt(wide + group_eps) * jax.nn.silu(switch)
            self.hidden[lines, pl.ds(head * VAL, VAL)] = result.astype(self.hidden.dtype)

        self.by_rows(rows, slot, slots)


    def glu(self, slot=0, slots=1):
        lead = self.halo_in.shape[0]

        def rows(first):
            lines = pl.ds(first, 128)
            value = self.products[4, lines].astype(jnp.float32)
            switch = self.products[5, lines].astype(jnp.float32)
            gated = (value * jax.nn.sigmoid(switch)).astype(jnp.bfloat16)
            self.padded[pl.ds(pl.multiple_of(first + lead, 8), 128)] = gated.astype(jnp.float32)

        self.by_rows(rows, slot, slots)
        self.halo_out[...] = self.padded[pl.ds(self.count, lead)].astype(jnp.bfloat16)
        self.padded[pl.ds(self.count + lead, 8)] = jnp.zeros(
            (8, self.padded.shape[1]), jnp.float32
        )
        pl.when(self.link < self.links - 1)(lambda: self.halo_copy().start())

    def halo_copy(self):
        following = jnp.minimum(self.link + 1, self.links - 1)
        return remote(
            self.halo_out,
            self.halo_in,
            self.halo_sems.at[0],
            self.halo_sems.at[1],
            self.chain(following),
        )

    def halo(self):
        lead = self.halo_in.shape[0]
        channels = self.padded.shape[1]

        @pl.when(self.link > 0)
        def _():
            self.halo_copy().wait_recv()
            self.padded[pl.ds(0, lead)] = self.halo_in[...].astype(jnp.float32)

        @pl.when(self.link == 0)
        def _():
            self.padded[pl.ds(0, lead)] = jnp.zeros((lead, channels), jnp.float32)

    def convolve(self, slot, slots):
        lead = self.halo_in.shape[0]
        channels = self.padded.shape[1]
        size = 64
        lanes = 128

        def rows(first):
            for part in range(channels // lanes):
                columns = pl.ds(part * lanes, lanes)
                spot = pl.multiple_of(self.rank * channels + part * lanes, lanes)
                weights = self.taps[:, pl.ds(spot, lanes)]
                source = self.padded[pl.ds(first, size + lead + 8), columns]
                total = None
                for low in range(8):
                    group = None
                    for high in range(lead // 8 + 1):
                        tap = high * 8 + low - (lead - KW + 1)
                        if not 0 <= tap < KW:
                            continue
                        term = source[high * 8 : high * 8 + size + 8] * weights[tap : tap + 1]
                        group = term if group is None else group + term
                    if low:
                        group = pltpu.roll(group, size + 8 - low, 0)
                    total = group[:size] if total is None else total + group[:size]
                self.summed[pl.ds(first, size), columns] = total

        self.by_rows(rows, slot, slots, size)

    def finish_convolution(self, slot, slots):
        channels = self.padded.shape[1]
        spot = pl.ds(pl.multiple_of(self.rank * channels, channels), channels)
        gain, shift = self.gain[:, spot], self.shift[:, spot]

        def rows(first):
            lines = pl.ds(first, 128)
            total = self.summed[lines]
            average = jnp.mean(total, axis=-1, keepdims=True)
            centred = total - average
            wide = jnp.mean(jnp.square(centred), axis=-1, keepdims=True)
            normalized = centred * lax.rsqrt(wide + layer_eps) * gain + shift
            switch = self.products[6, lines].astype(jnp.float32)
            result = jax.nn.silu(normalized) * jax.nn.silu(switch)
            target = pl.ds(self.heads * VAL, channels)
            self.hidden[lines, target] = result.astype(self.hidden.dtype)

        self.by_rows(rows, slot, slots)


    def x_copy(self, n):
        zh, zl, y, x, c = self.at
        return remote(
            self.sent.at[n],
            self.crossed.at[n],
            self.out_sems.at[0, n],
            self.out_sems.at[1, n],
            (zh, zl, y, 1 - x, c),
        )

    def near_copy(self, n):
        zh, zl, y, x, c = self.at
        share = self.out.shape[0]
        part = self.half.at[n, pl.ds(pl.multiple_of((1 - c) * share, share), share)]
        return remote(
            part,
            self.here.at[n],
            self.out_sems.at[2, n],
            self.out_sems.at[3, n],
            (zh, zl, y, x, 1 - c),
        )

    def far_copy(self, n, core):
        zh, zl, y, x, c = self.at
        share = self.out.shape[0]
        return remote(
            self.half.at[n, pl.ds(core * share, share)],
            self.there.at[n],
            self.out_sems.at[2 + 2 * core, n],
            self.out_sems.at[5, n],
            (c, zl, y, x, core),
        )

    def multiply(self, j, q, weights):
        x = self.at[3]
        tile = self.sent.shape[2]
        n = j * 4 + q
        pair = self.sent.shape[1]
        lines = pl.ds(pl.multiple_of(q * tile, tile), tile)
        total = contract(self.hidden[...], weights[j, lines])
        low, high = total[:pair], total[pair:]
        self.kept[n] = jnp.where(x == 0, low, high)
        self.sent[n] = jnp.where(x == 0, high, low).astype(self.sent.dtype)
        self.x_copy(n).start()

    def join(self, n):
        zh, zl, y, x, c = self.at
        self.x_copy(n).wait_recv()
        total = self.kept[n] + self.crossed[n].astype(jnp.float32)
        self.half[n] = total.astype(self.half.dtype)

        @pl.when(c == zh)
        def _():
            self.near_copy(n).start()

        @pl.when(c != zh)
        def _():
            self.far_copy(n, 0).start()
            self.far_copy(n, 1).start()

    def close(self, j, q):
        zh, zl, y, x, c = self.at
        n = j * 4 + q
        share = self.out.shape[0]
        wide = self.sent.shape[2] // 2
        part = self.there.at[n]
        remote(
            part, part, self.out_sems.at[4, n], self.out_sems.at[5, n], (zh, zl, y, 1 - x, c)
        ).wait_recv()
        far_part = self.there[n].astype(jnp.float32)

        def store(near_part):
            total = (near_part.astype(jnp.float32) + far_part).astype(self.out.dtype)
            for k in range(2):
                spot = ((2 * q + k) * 2 + j) * wide
                self.out[:, pl.ds(spot, wide)] = total[:, k * wide : (k + 1) * wide]

        @pl.when(c == zh)
        def _():
            store(self.half[n, pl.ds(pl.multiple_of(c * share, share), share)])

        @pl.when(c != zh)
        def _():
            self.near_copy(n).wait_recv()
            store(self.here[n])

    def drain(self):
        zh, zl, y, x, c = self.at
        self.drain_rows()
        self.others(lambda s: self.slice_copy(s).wait_send())
        self.others(lambda s: self.prefix_copy(s).wait_send())
        pl.when(self.link < self.links - 1)(lambda: self.halo_copy().wait_send())
        for n in range(self.sent.shape[0]):
            self.x_copy(n).wait_send()

            @pl.when(c == zh)
            def _():
                self.near_copy(n).wait_send()

            @pl.when(c != zh)
            def _():
                self.far_copy(n, 0).wait_send()
                self.far_copy(n, 1).wait_send()


def layer_kernel(layout, out_layout, *refs):
    blocks, refs = refs[:9], refs[9:]
    first_gather, refs = refs[-12:-6], refs[:-12] + refs[-6:]
    second_gather, refs = refs[-6:], refs[:-6]
    layer = Layer(refs)
    inward, outward = Gather(*first_gather), Gather(*second_gather)
    units = len(layout)
    total = units + 2

    for n in range(3):
        layer.load(n).start()
    for k, (which, first) in enumerate(layout):
        inward.load(k, blocks[which].at[:, pl.ds(first, inward.source.shape[2])], None)
    for k, parts in enumerate(out_layout):
        for which, row, column in parts:
            ref = blocks[which]
            lines = pl.ds(row, outward.depth)
            outward.load(k, ref.at[lines], pl.ds(column, ref.shape[1]))

    def at_unit(k, what):
        @pl.when(jnp.logical_and(k >= 0, k < units))
        def _():
            what(inward, k)

        @pl.when(jnp.logical_and(k >= units, k < total))
        def _():
            what(outward, k - units)

    def first_sends(own, ahead):
        for k in range(ahead):
            if k < units:
                inward.begin(k, own)
            else:
                outward.begin(k - units, own)

    pl.when(inward.is_own)(lambda: first_sends(True, OWN_AHEAD))
    pl.when(jnp.logical_not(inward.is_own))(lambda: first_sends(False, FAR_AHEAD))
    layer.near_rows()
    layer.far_strip(0).start()

    def next_sends(i):
        @pl.when(inward.is_own)
        def _():
            at_unit(i + OWN_AHEAD, lambda gather, k: gather.begin(k, True))

        @pl.when(jnp.logical_not(inward.is_own))
        def _():
            at_unit(i + FAR_AHEAD, lambda gather, k: gather.begin(k, False))

    inside, finish_head = layer.inside, layer.finish_head
    key_scale = KEY ** (-0.5)
    after = (
        (lambda n: layer.rotate(0, layer.keys, key_scale, n, 2),) * 2,
        (lambda n: layer.contribute(0), None),
        (lambda n: (layer.contribute(1), layer.send_slices()), None),
        (lambda n: layer.rotate(3, layer.queries, 1.0, n, 2),) * 2,
        (lambda n: (layer.scan(), inside(0, 0, 1)), None),
        (lambda n: layer.glu(), lambda n: inside(1, 0, 1)),
        (lambda n: (layer.halo(), layer.convolve(0, 1)), None),
        (lambda n: layer.finish_convolution(0, 1), None),
        (
            lambda n: layer.state_arrived(),
            lambda n: (finish_head(0, 0, 1), finish_head(1, 0, 1)),
        ),
    )

    def compute(k, carry):
        inward.complete_own(k)
        inward.complete_far(k)
        layer.project(k, inward.full, 0, 2)
        layer.project(k, inward.full, 1, 2)
        for unit, events in enumerate(after):

            @pl.when(k == unit)
            def _():
                for n, event in enumerate(events):
                    if event is not None:
                        event(n)

        return carry

    def relay(k, number):
        at_unit(k, lambda gather, k: gather.stage(k, number))

    for number in (0, 1, 4):
        for k in range(LEADS[number]):
            relay(k, number)

    layer.tables()

    def ready(i):
        return jnp.clip(2 * (i - START), 0, jnp.clip(i + 1 - BEHIND, 0, units))

    def step(i, carry):
        relay(i + LEADS[0], 0)
        relay(i + LEADS[1], 1)
        pl.when(jnp.logical_and(i >= 0, i < STRIPS - 1))(lambda: layer.far_strip(i + 1).start())
        next_sends(i)

        @pl.when(jnp.logical_and(i >= ROWS_RELAY, i < ROWS_RELAY + STRIPS))
        def _():
            layer.relay_rows(i - ROWS_RELAY)

        relay(i, 2)
        relay(i + LEADS[4], 4)
        relay(i - 1, 3)
        pl.when(i == START + 1)(layer.all_rows)
        lax.fori_loop(ready(i - 1), ready(i), compute, 0)
        return carry

    lax.fori_loop(0, units + 1, step, 0)
    lax.fori_loop(ready(units), units, compute, 0)

    zh = layer.at[0]

    def tiles(j, half, what):
        for m in range(2):
            what(j, half * 2 + m)

    def multiply(j, q):
        layer.multiply(j, q, outward.full)

    def join(j, q):
        layer.join(j * 4 + q)

    for k in range(units + 1 + LEADS[4], total):
        relay(k, 4)
    outward.complete_own(0)
    tiles(0, zh, multiply)
    relay(units, 3)
    outward.complete_own(1)
    tiles(1, zh, multiply)
    relay(units + 1, 2)
    outward.complete_far(0)
    tiles(0, 1 - zh, multiply)
    tiles(0, zh, join)
    tiles(1, zh, join)
    relay(units + 1, 3)
    outward.complete_far(1)
    tiles(1, 1 - zh, multiply)
    tiles(0, 1 - zh, join)
    tiles(1, 1 - zh, join)
    for j in range(2):
        for q in range(4):
            layer.close(j, q)

    def finish(gather):
        def body(k, carry):
            gather.drain(k)
            return carry

        lax.fori_loop(0, gather.source.shape[0], body, 0)

    finish(inward)
    finish(outward)
    layer.drain()


def whole_layer(tokens, norm_gain, taps, gain, shift, blocks):
    depth, width = blocks[0].shape
    share, model = tokens.shape
    layout = []
    for which, block in enumerate(blocks[:7]):
        layout += [(which, first) for first in range(0, block.shape[1], width)]
    units = len(layout)
    shares, dtype = 8, tokens.dtype
    span = 4 * share
    wide = KEY // 2
    frequency = rope_base ** (-np.arange(wide) / wide)
    angles = [np.arange(span)[:, None] * frequency]
    angles += [span * np.arange(shares)[:, None] * frequency]
    angles, turns = (np.stack([np.cos(a), np.sin(a)]).astype(np.float32) for a in angles)
    inner_width = blocks[7].shape[1] + blocks[8].shape[1]
    half_depth = depth // 2
    out_layout = [
        ((7, j * half_depth, 0), (8, j * half_depth, blocks[7].shape[1])) for j in range(2)
    ]
    heads = width // KEY
    channels = blocks[8].shape[1]
    lead = (KW + 7) // 8 * 8
    tile = 2 * half_depth
    tiles = model // tile
    sem = pltpu.SemaphoreType.DMA
    slice_rows = heads * KEY // shares
    return pl.pallas_call(
        lambda *refs: layer_kernel(layout, out_layout, *refs),
        out_shape=jax.ShapeDtypeStruct((share, model), dtype),
        in_specs=[pl.BlockSpec(memory_space=pl.ANY)] * 11
        + [pl.BlockSpec(memory_space=pltpu.VMEM), pl.BlockSpec(memory_space=pl.ANY)]
        + [pl.BlockSpec(memory_space=pltpu.VMEM)] * 3,
        out_specs=pl.BlockSpec(memory_space=pltpu.VMEM),
        scratch_shapes=[
            pltpu.VMEM((share, model), dtype),
            pltpu.VMEM(angles.shape, jnp.float32),
            pltpu.VMEM(taps.shape, jnp.float32),
            pltpu.VMEM((share, model), dtype),
            pltpu.VMEM((span, wide), jnp.float32),
            pltpu.VMEM((span, wide), jnp.float32),
            pltpu.VMEM((span, model), dtype),
            pltpu.VMEM((units, span, width), dtype),
            pltpu.VMEM((span, width), dtype),
            pltpu.VMEM((span, width), dtype),
            pltpu.VMEM((heads, span, VAL), jnp.float32),
            pltpu.VMEM((heads * KEY, VAL), dtype),
            pltpu.VMEM((shares, slice_rows, VAL), dtype),
            pltpu.VMEM((shares, slice_rows, VAL), dtype),
            pltpu.VMEM((heads * KEY, VAL), dtype),
            pltpu.VMEM((span + lead + 8, channels), jnp.float32),
            pltpu.VMEM((lead, channels), dtype),
            pltpu.VMEM((lead, channels), dtype),
            pltpu.VMEM((span, channels), jnp.float32),
            pltpu.VMEM((span, inner_width), dtype),
            pltpu.VMEM((tiles, 2 * share, tile), jnp.float32),
            pltpu.VMEM((tiles, 2 * share, tile), dtype),
            pltpu.VMEM((tiles, 2 * share, tile), dtype),
            pltpu.VMEM((tiles, 2 * share, tile), dtype),
            pltpu.VMEM((tiles, share, tile), dtype),
            pltpu.VMEM((tiles, share, tile), dtype),
            sem((2 + 3 * STRIPS,)),
            sem((4, STRIPS)),
            sem((2, shares)),
            sem((2, shares)),
            sem((2,)),
            sem((6, tiles)),
            sem((3,)),
        ]
        + gather_scratch(units, depth, width, shares, dtype)
        + gather_scratch(2, half_depth, inner_width, shares, dtype),
        compiler_params=pltpu.CompilerParams(has_side_effects=True, vmem_limit_bytes=60 << 20),
        name="layer",
    )(*blocks, tokens, angles, turns, taps, norm_gain, gain, shift)


def local_squares(
    tokens,
    norm_gain,
    query_weight,
    key_weight,
    value_weight,
    retain_gate,
    unit_value,
    unit_gate,
    convolve_gate,
    filter_taps,
    layer_gain,
    layer_shift,
    retain_output,
    convolve_output,
):
    blocks = (key_weight, value_weight, query_weight, unit_value, unit_gate, convolve_gate)
    blocks += (retain_gate, retain_output, convolve_output)
    return whole_layer(
        tokens,
        norm_gain[None],
        filter_taps,
        layer_gain[None],
        layer_shift[None],
        blocks,
    )


def squares(mesh):
    boxes = Mesh(mesh.devices.reshape(2, 2, 2, 2, 2), SQUARE)
    rows, blocks = P(SQUARE, None), P(("zh", "zl", "y"), ("x", "c"))
    return jax.shard_map(
        local_squares,
        mesh=boxes,
        in_specs=(rows, P()) + (blocks,) * 7 + (P(),) * 3 + (blocks,) * 2,
        out_specs=rows,
        check_vma=False,
    )


def solution(mesh):
    sp, tp = mesh.shape["sp"], mesh.shape["tp"]
    if (sp, tp) == (8, 4):
        return squares(mesh)
    planes = Mesh(mesh.devices.reshape(tp, sp // tp, tp), ("hi", "lo", "tp"))
    return jax.shard_map(
        local,
        mesh=planes,
        in_specs=(
            P(("hi", "lo", "tp"), None),
            P(),
            P(("hi", "lo"), "tp"),
            P(("hi", "lo"), "tp"),
            P(("hi", "lo"), "tp"),
            P(("hi", "lo"), "tp"),
            P(("hi", "lo"), "tp"),
            P(("hi", "lo"), "tp"),
            P(("hi", "lo"), "tp"),
            P(),
            P(),
            P(),
            P(("hi", "lo"), "tp"),
            P(("hi", "lo"), "tp"),
        ),
        out_specs=P(("hi", "lo", "tp"), None),
        check_vma=False,
    )
```

```python
import math

import jax
import jax.numpy as jnp
import numpy as np
from jax import lax
from jax.experimental import pallas as pl
from jax.experimental.pallas import tpu as pltpu
from jax.sharding import Mesh
from jax.sharding import PartitionSpec as P

KEY = 256
VAL = 512
GROUP = 512
KW = 31


rms_eps = 1e-06
group_eps = 1.0
layer_eps = 0.001
rope_base = 10000.0


SPANS = ("tp", "lo")


def swap_planes(x):
    size = lax.axis_size("tp")
    pairs = [(h * size + t, t * size + h) for h in range(size) for t in range(size)]
    return lax.ppermute(x, ("hi", "tp"), pairs)


def from_behind(x, by):
    outer, inner = lax.axis_size("tp"), lax.axis_size("lo")
    spot = [(i % inner) * outer + i // inner for i in range(outer * inner)]
    return lax.ppermute(x, ("lo", "tp"), list(zip(spot[:-by], spot[by:])))


def carried_in(contribution, log_span_decay):
    length = lax.axis_size(SPANS)
    state = from_behind(contribution.astype(jnp.bfloat16), 1).astype(jnp.float32)
    by = 1
    while by < length:
        earlier = from_behind(state.astype(jnp.bfloat16), by).astype(jnp.float32)
        state = state + jnp.exp(log_span_decay * by)[:, None, None] * earlier
        by *= 2
    return state


def rms_normalize(tokens, norm_gain):
    widened = tokens.astype(jnp.float32)
    scaled = widened * lax.rsqrt(jnp.mean(widened * widened, axis=-1, keepdims=True) + rms_eps)
    return (scaled * norm_gain).astype(jnp.bfloat16)


def rotate(vectors, positions):
    half_width = vectors.shape[-1] // 2
    frequency = rope_base ** (-jnp.arange(half_width, dtype=jnp.float32) / half_width)
    angles = positions.astype(jnp.float32)[:, None] * frequency
    cosine = jnp.cos(angles)[:, None, :]
    sine_part = jnp.sin(angles)[:, None, :]
    front_half = vectors[..., :half_width]
    back_half = vectors[..., half_width:]
    return jnp.concatenate(
        [front_half * cosine - back_half * sine_part, front_half * sine_part + back_half * cosine],
        axis=-1,
    )


def prepare(queries, key_rows, values, positions):
    row_count = queries.shape[0]
    rotated_query = rotate(
        queries.astype(jnp.float32).reshape(row_count, -1, KEY), positions
    ).astype(jnp.bfloat16)
    rotated_keys = (
        rotate(key_rows.astype(jnp.float32).reshape(row_count, -1, KEY), positions) * KEY ** (-0.5)
    ).astype(jnp.bfloat16)
    value_heads = values.reshape(row_count, -1, VAL)
    return (rotated_query, rotated_keys, value_heads)


def decay_logs(first_head, head_total, all_heads, seq_length):
    ratio = (first_head + jnp.arange(head_total)).astype(jnp.float32) / (all_heads - 1)
    return (jnp.log(0.05) + ratio * jnp.log(18.0)) / seq_length


def local_parts(queries, key_rows, values, log_decay):
    row_count = queries.shape[0]
    indices = jnp.arange(row_count, dtype=jnp.float32)
    offsets = indices[:, None] - indices[None, :]
    causal = offsets >= 0
    weight = jnp.where(
        causal[None], jnp.exp(log_decay[:, None, None] * jnp.where(causal, offsets, 0.0)[None]), 0.0
    )
    scores = (
        jnp.einsum("ihd,jhd->hij", queries, key_rows, preferred_element_type=jnp.float32) * weight
    ).astype(jnp.bfloat16)
    within = jnp.einsum("hij,jhe->ihe", scores, values, preferred_element_type=jnp.float32)
    trailing = jnp.exp(log_decay[None, :] * (row_count - 1.0 - indices)[:, None])
    weighted = (key_rows.astype(jnp.float32) * trailing[:, :, None]).astype(jnp.bfloat16)
    contribution = jnp.einsum("jhd,jhe->hde", weighted, values, preferred_element_type=jnp.float32)
    return (within, contribution)


def cross_part(queries, carry_state, log_decay):
    row_count = queries.shape[0]
    indices = jnp.arange(row_count, dtype=jnp.float32)
    leading = jnp.exp(log_decay[None, :] * (indices + 1.0)[:, None])
    return (
        jnp.einsum(
            "ihd,hde->ihe",
            queries,
            carry_state.astype(jnp.bfloat16),
            preferred_element_type=jnp.float32,
        )
        * leading[:, :, None]
    )


def retain_finish(raw, switch):
    average = jnp.mean(raw, axis=-1, keepdims=True)
    spread = jnp.mean(jnp.square(raw - average), axis=-1, keepdims=True)
    normalized = ((raw - average) * lax.rsqrt(spread + group_eps)).reshape(raw.shape[0], -1)
    return (normalized * jax.nn.silu(switch.astype(jnp.float32))).astype(jnp.bfloat16)


def convolve_branch(gated_input, before, tap_slice, gain_slice, shift_slice, switch):
    padded = jnp.concatenate([before, gated_input], axis=0)
    row_count = gated_input.shape[0]
    summed = jnp.zeros(gated_input.shape, jnp.float32)
    for tap_index in range(tap_slice.shape[0]):
        summed = (
            summed
            + padded[tap_index : tap_index + row_count].astype(jnp.float32) * tap_slice[tap_index]
        )
    grouped = summed.reshape(row_count, -1, GROUP)
    average = jnp.mean(grouped, axis=-1, keepdims=True)
    spread = jnp.mean(jnp.square(grouped - average), axis=-1, keepdims=True)
    normalized = ((grouped - average) * lax.rsqrt(spread + layer_eps)).reshape(row_count, -1)
    normalized = normalized * gain_slice + shift_slice
    return (jax.nn.silu(normalized) * jax.nn.silu(switch.astype(jnp.float32))).astype(jnp.bfloat16)


def contract(hidden, matrix):
    return lax.dot_general(
        hidden, matrix, (((1,), (1,)), ((), ())), preferred_element_type=jnp.float32
    )


def local(
    tokens,
    norm_gain,
    query_weight,
    key_weight,
    value_weight,
    retain_gate,
    unit_value,
    unit_gate,
    convolve_gate,
    filter_taps,
    layer_gain,
    layer_shift,
    retain_output,
    convolve_output,
):
    head_groups = lax.axis_size("hi")
    chain_length = lax.axis_size(SPANS)
    head_rank = lax.axis_index("hi")
    chain_rank = lax.axis_index(SPANS)
    def project(rows, merged, *matrices):
        product = jnp.dot(rows, merged, preferred_element_type=jnp.float32).astype(jnp.bfloat16)
        ends = [sum(m.shape[1] for m in matrices[: k + 1]) for k in range(len(matrices) - 1)]
        return jnp.split(product, ends, axis=1)

    first = (key_weight, value_weight, query_weight)
    second = (unit_value, unit_gate, convolve_gate, retain_gate)
    third = (retain_output, convolve_output)
    groups = (first, second, third)
    merged = [jnp.concatenate(group, axis=1) for group in groups]
    normed = rms_normalize(tokens, norm_gain)
    normed = lax.all_gather(swap_planes(normed), "hi", axis=0, tiled=True)
    merged = [lax.all_gather(swap_planes(m), SPANS, axis=0, tiled=True) for m in merged]
    key_rows, values, queries = project(normed, merged[0], *first)
    glu_value, glu_switch, convolve_switch, retain_switch = project(normed, merged[1], *second)
    out_full = merged[2]
    row_count = normed.shape[0]
    local_heads = queries.shape[1] // KEY
    positions = chain_rank * row_count + jnp.arange(row_count, dtype=jnp.int32)
    rotated_query, rotated_keys, value_heads = prepare(queries, key_rows, values, positions)
    log_decay = decay_logs(
        head_rank * local_heads, local_heads, local_heads * head_groups, row_count * chain_length
    )
    within, contribution = local_parts(rotated_query, rotated_keys, value_heads, log_decay)
    gated_input = (
        glu_value.astype(jnp.float32) * jax.nn.sigmoid(glu_switch.astype(jnp.float32))
    ).astype(jnp.bfloat16)
    channels = gated_input.shape[1]
    before = from_behind(gated_input[row_count - (KW - 1) :], 1)
    incoming = carried_in(contribution, log_decay * row_count)
    raw = within + cross_part(rotated_query, incoming, log_decay)
    retain_hidden = retain_finish(raw, retain_switch)
    tap_slice = lax.dynamic_slice_in_dim(filter_taps, head_rank * channels, channels, 1)
    gain_slice = lax.dynamic_slice_in_dim(layer_gain, head_rank * channels, channels, 0)
    shift_slice = lax.dynamic_slice_in_dim(layer_shift, head_rank * channels, channels, 0)
    convolve_hidden = convolve_branch(
        gated_input, before, tap_slice, gain_slice, shift_slice, convolve_switch
    )
    hidden = jnp.concatenate([retain_hidden, convolve_hidden], axis=1)
    mixed = contract(hidden, out_full).astype(jnp.bfloat16)
    return swap_planes(lax.psum_scatter(mixed, "hi", scatter_dimension=0, tiled=True))


OWN_AHEAD = 4
FAR_AHEAD = 2
LEADS = (1, 1, 0, -1, 0)
STRIPS = 4
ROWS_RELAY = 1
START = 4
BEHIND = 1
MESH = pl.DeviceIdType.MESH
SQUARE = ("zh", "zl", "y", "x", "c")
CHAIN = ("c", "zl", "y")


def remote(source, target, out_sem, in_sem, device):
    return pltpu.make_async_remote_copy(
        src_ref=source,
        dst_ref=target,
        send_sem=out_sem,
        recv_sem=in_sem,
        device_id=device,
        device_id_type=MESH,
    )


def place():
    return tuple(lax.axis_index(name) for name in SQUARE)


def meet():
    zh, zl, y, x, c = place()
    barrier = pltpu.get_barrier_semaphore()
    peers = []
    for n in range(1, 16):
        flips = [(n >> bit) & 1 for bit in range(4)]
        a, b, d, e = (1 - v if flip else v for v, flip in zip((zh, zl, y, c), flips))
        peers.append((a, b, d, x, e))
    peers += [(zh, zl, y, 1 - x, c), (zh, zl, y, 1 - x, 1 - c)]
    for peer in peers:
        pl.semaphore_signal(barrier, inc=1, device_id=peer, device_id_type=MESH)
    pl.semaphore_wait(barrier, len(peers))


class Gather:
    def __init__(self, source, full, near, send, arrive, beside):
        self.source, self.full, self.near = source, full, near
        self.send, self.arrive, self.beside = send, arrive, beside
        zh, zl, y, x, c = self.at = place()
        self.depth = source.shape[1]
        self.half = self.depth // 2
        self.outer = zl * zh + (1 - zl) * (1 - zh)
        self.mine = self.index(zh, self.outer, y)
        self.is_own = c == zh

    def index(self, zh, outer, y):
        zl = outer * zh + (1 - outer) * (1 - zh)
        return (zh * 2 + zl) * 2 + y

    def own(self, outer, flip):
        return self.index(self.at[0], outer, self.at[2] if not flip else 1 - self.at[2])

    def far(self, outer, flip):
        return self.index(1 - self.at[0], outer, self.at[2] if not flip else 1 - self.at[2])

    def rows(self, k, s, half):
        start = pl.multiple_of(s * self.depth + half * self.half, self.half)
        return self.full.at[k, pl.ds(start, self.half)]

    def whole(self, k, s):
        return self.full.at[k, pl.ds(pl.multiple_of(s * self.depth, self.depth), self.depth)]

    def z_mate(self, core):
        zh, zl, y, x, c = self.at
        return (zh, 1 - zl, y, x, core)

    def y_mate(self, core):
        zh, zl, y, x, c = self.at
        return (zh, zl, 1 - y, x, core)

    def sibling(self):
        zh, zl, y, x, c = self.at
        return (zh, zl, y, x, 1 - c)

    def load(self, k, part, columns):
        columns = pl.ds(0, self.source.shape[2]) if columns is None else columns

        @pl.when(self.is_own)
        def _():
            target = self.whole(k, self.mine).at[:, columns]
            pltpu.make_async_copy(part, target, self.near.at[k]).start()

        @pl.when(jnp.logical_not(self.is_own))
        def _():
            target = self.source.at[k].at[:, columns]
            pltpu.make_async_copy(part, target, self.near.at[k]).start()

    def own_sends(self, k):
        zh, zl, y, x, c = self.at
        part = self.whole(k, self.mine)
        copies = [remote(part, part, self.send.at[k, 16], self.beside.at[k], self.sibling())]
        for r in range(2):
            piece = self.rows(k, self.mine, r)
            arrive = self.arrive.at[k, self.mine, r]
            copies.append(remote(piece, piece, self.send.at[k, 12 + r], arrive, self.z_mate(r)))
            copies.append(remote(piece, piece, self.send.at[k, 14 + r], arrive, self.y_mate(r)))
        return copies

    def far_sends(self, k):
        zh, zl, y, x, c = self.at
        copies = []
        for r in range(2):
            piece = self.source.at[k, pl.ds(r * self.half, self.half)]
            copies.append(
                remote(
                    piece,
                    self.rows(k, self.mine, r),
                    self.send.at[k, 12 + r],
                    self.arrive.at[k, self.mine, r],
                    (c, 1 - c, y, x, r),
                )
            )
        return copies

    def begin(self, k, own):
        pltpu.make_async_copy(self.source.at[k], self.source.at[k], self.near.at[k]).wait()
        for copy in self.own_sends(k) if own else self.far_sends(k):
            copy.start()

    def onward(self, k, s, device, slot):
        piece = self.rows(k, s, self.at[4])
        return remote(piece, piece, self.send.at[k, slot], self.arrive.at[k, s, self.at[4]], device)

    def landed(self, k, s, half):
        piece = self.rows(k, s, half)
        remote(
            piece, piece, self.send.at[k, 0], self.arrive.at[k, s, half], self.sibling()
        ).wait_recv()

    def table(self):
        c = self.at[4]
        z_mate, y_mate, sibling = self.z_mate(c), self.y_mate(c), self.sibling()
        inner = (
            (
                (self.far(0, 0), ((z_mate, 0, None), (y_mate, 1, None), (sibling, 2, None))),
                (self.far(1, 0), ((z_mate, 3, None), (y_mate, 4, None), (sibling, 5, None))),
            ),
            (
                (self.own(0, 1), ((z_mate, 8, 0), (sibling, 7, None))),
                (self.own(1, 0), ((sibling, 6, None),)),
            ),
            (
                (self.far(0, 1), ((sibling, 9, None),)),
                (self.far(1, 1), ((sibling, 10, None),)),
            ),
            (),
            ((self.own(1, 1), ((sibling, 11, None),)),),
        )
        outer = (
            (),
            (
                (self.own(1, 1), ((z_mate, 2, None), (sibling, 3, None))),
                (self.own(0, 0), ((y_mate, 1, 1), (sibling, 0, None))),
            ),
            (
                (self.far(0, 0), ((y_mate, 4, None), (sibling, 5, None))),
                (self.far(1, 0), ((y_mate, 6, None), (sibling, 7, None))),
            ),
            (
                (self.far(0, 1), ((sibling, 8, None),)),
                (self.far(1, 1), ((sibling, 9, None),)),
            ),
            ((self.own(0, 1), ((sibling, 10, None),)),),
        )
        return inner, outer

    def stage(self, k, number):
        for role, moves in enumerate(self.table()):
            if not moves[number]:
                continue

            @pl.when(self.outer == role)
            def _():
                for s, targets in moves[number]:
                    self.landed(k, s, self.at[4])
                    for device, slot, lane in targets:
                        copy = self.onward(k, s, device, slot)
                        if lane is None:
                            copy.start()
                        else:
                            pl.when(self.at[4] == lane)(copy.start)

    def complete_own(self, k):
        other = 1 - self.at[4]
        for outer, flip in ((1 - self.outer, 0), (self.outer, 1), (1 - self.outer, 1)):
            self.landed(k, self.own(outer, flip), other)

        @pl.when(jnp.logical_not(self.is_own))
        def _():
            part = self.whole(k, self.mine)
            remote(
                part, part, self.send.at[k, 0], self.beside.at[k], self.sibling()
            ).wait_recv()

    def complete_far(self, k):
        other = 1 - self.at[4]
        for outer, flip in ((0, 0), (1, 0), (0, 1), (1, 1)):
            self.landed(k, self.far(outer, flip), other)

    def drain(self, k):
        @pl.when(self.is_own)
        def _():
            for copy in self.own_sends(k):
                copy.wait_send()

        @pl.when(jnp.logical_not(self.is_own))
        def _():
            for copy in self.far_sends(k):
                copy.wait_send()

        for role, moves in enumerate(self.table()):

            @pl.when(self.outer == role)
            def _():
                for number in range(len(moves)):
                    for s, targets in moves[number]:
                        for device, slot, lane in targets:
                            copy = self.onward(k, s, device, slot)
                            if lane is None:
                                copy.wait_send()
                            else:
                                pl.when(self.at[4] == lane)(copy.wait_send)


def gather_scratch(units, depth, width, shares, dtype):
    return [
        pltpu.VMEM((units, depth, width), dtype),
        pltpu.VMEM((units, shares * depth, width), dtype),
        pltpu.SemaphoreType.DMA((units,)),
        pltpu.SemaphoreType.DMA((units, 17)),
        pltpu.SemaphoreType.DMA((units, shares, 2)),
        pltpu.SemaphoreType.DMA((units,)),
    ]


class Layer:
    def __init__(self, refs):
        names = (
            "tokens_in",
            "angles_in",
            "turns",
            "taps_in",
            "norm_gain",
            "gain",
            "shift",
            "out",
            "tokens",
            "angles",
            "taps",
            "rows",
            "cosine",
            "sine",
            "normed",
            "products",
            "keys",
            "queries",
            "within",
            "sending",
            "got",
            "prefix",
            "state",
            "padded",
            "halo_out",
            "halo_in",
            "summed",
            "hidden",
            "kept",
            "sent",
            "crossed",
            "half",
            "here",
            "there",
        )
        for name, ref in zip(names, refs):
            setattr(self, name, ref)
        sems = refs[len(names) :]
        (
            self.rows_send,
            self.rows_arrive,
            self.slice_sems,
            self.prefix_sems,
            self.halo_sems,
            self.out_sems,
            self.load_sems,
        ) = sems
        zh, zl, y, x, c = self.at = place()
        self.count = self.normed.shape[0]
        self.heads = self.keys.shape[1] // KEY
        self.rank = x * 2 + zh
        self.link = (c * 2 + zl) * 2 + y
        self.links = 8
        self.groups = 4

    def chain(self, s):
        zh, zl, y, x, c = self.at
        return (zh, (s // 2) % 2, s % 2, x, s // 4)

    def log_decay(self, head):
        ratio = (self.rank * self.heads + head).astype(jnp.float32) / (
            self.heads * self.groups - 1
        )
        return (math.log(0.05) + ratio * math.log(18.0)) / (self.count * self.links)

    def by_rows(self, what, slot=0, slots=1, size=128):
        steps = self.count // size // slots

        def body(n, carry):
            what(pl.multiple_of(n * size, size))
            return carry

        lax.fori_loop(slot * steps, (slot + 1) * steps, body, 0)

    def position(self, first, size):
        rows = lax.broadcasted_iota(jnp.int32, (size, 1), 0) + first
        return rows.astype(jnp.float32)


    def block(self, j):
        share = self.rows.shape[0]
        return self.normed.at[pl.ds(pl.multiple_of(j * share, share), share)]

    def strip(self, j, t):
        share = self.rows.shape[0]
        size = share // STRIPS
        return self.normed.at[pl.ds(pl.multiple_of(j * share + t * size, size), size)]

    def near_copy_of_rows(self, dx):
        zh, zl, y, x, c = self.at
        j = x * 2 + c
        return remote(
            self.rows,
            self.block(j),
            self.rows_send.at[dx],
            self.rows_arrive.at[j, 0],
            (zh, zl, y, 1 - x if dx else x, zh),
        )

    def far_strip(self, t):
        zh, zl, y, x, c = self.at
        j = x * 2 + c
        size = self.rows.shape[0] // STRIPS
        return remote(
            self.rows.at[pl.ds(pl.multiple_of(t * size, size), size)],
            self.strip(j, t),
            self.rows_send.at[2 + t],
            self.rows_arrive.at[j, t],
            (1 - zh, zl, y, x, zh),
        )

    def onward_strip(self, core, t):
        zh, zl, y, x, c = self.at
        j = x * 2 + core
        return remote(
            self.strip(j, t),
            self.strip(j, t),
            self.rows_send.at[2 + (1 + core) * STRIPS + t],
            self.rows_arrive.at[j, t],
            (zh, zl, y, 1 - x, c),
        )

    def rows_landed(self, part, j, t):
        remote(part, part, self.rows_send.at[0], self.rows_arrive.at[j, t], self.chain(0)).wait_recv()

    def load(self, n):
        source = (self.tokens_in, self.angles_in, self.taps_in)[n]
        target = (self.tokens, self.angles, self.taps)[n]
        return pltpu.make_async_copy(source, target, self.load_sems.at[n])

    def near_rows(self):
        zh, zl, y, x, c = self.at
        j = x * 2 + c
        share = self.rows.shape[0]
        self.load(0).wait()
        tokens = self.tokens[...].astype(jnp.float32)
        scaled = tokens * lax.rsqrt(jnp.mean(tokens * tokens, axis=-1, keepdims=True) + rms_eps)
        self.rows[...] = (scaled * self.norm_gain[...]).astype(self.rows.dtype)

        @pl.when(c == zh)
        def _():
            self.normed[pl.ds(pl.multiple_of(j * share, share), share)] = self.rows[...]

        self.near_copy_of_rows(1).start()
        pl.when(c != zh)(lambda: self.near_copy_of_rows(0).start())

    def tables(self):
        self.load(1).wait()
        self.load(2).wait()
        turn_cosine = self.turns[0, pl.ds(self.link, 1)]
        turn_sine = self.turns[1, pl.ds(self.link, 1)]
        cosine, sine = self.angles[0], self.angles[1]
        self.cosine[...] = cosine * turn_cosine - sine * turn_sine
        self.sine[...] = sine * turn_cosine + cosine * turn_sine

    def relay_rows(self, t):
        zh, zl, y, x, c = self.at

        @pl.when(c != zh)
        def _():
            for core in range(2):
                j = x * 2 + core
                self.rows_landed(self.strip(j, t), j, t)
                self.onward_strip(core, t).start()

    def all_rows(self):
        zh, zl, y, x, c = self.at

        @pl.when(c == zh)
        def _():
            for j in range(4):
                pl.when(x * 2 + c != j)(lambda: self.rows_landed(self.block(j), j, 0))

        @pl.when(c != zh)
        def _():
            for core in range(2):
                for t in range(STRIPS):
                    j = (1 - x) * 2 + core
                    self.rows_landed(self.strip(j, t), j, t)

    def drain_rows(self):
        zh, zl, y, x, c = self.at
        self.near_copy_of_rows(1).wait_send()
        for t in range(STRIPS):
            self.far_strip(t).wait_send()

        @pl.when(c != zh)
        def _():
            self.near_copy_of_rows(0).wait_send()
            for core in range(2):
                for t in range(STRIPS):
                    self.onward_strip(core, t).wait_send()


    def project(self, k, weights, part, parts):
        wide = weights.shape[2] // parts
        columns = pl.ds(part * wide, wide)
        self.products[k, :, columns] = jnp.dot(
            self.normed[...], weights[k, :, columns], preferred_element_type=jnp.float32
        ).astype(self.products.dtype)

    def rotate(self, unit, target, scale, slot, slots):
        wide = KEY // 2

        def rows(first):
            lines = pl.ds(first, 128)
            cosine, sine = self.cosine[lines], self.sine[lines]
            for head in range(self.heads):
                low = pl.ds(head * KEY, wide)
                high = pl.ds(head * KEY + wide, wide)
                front = self.products[unit, lines, low].astype(jnp.float32)
                back = self.products[unit, lines, high].astype(jnp.float32)
                target[lines, low] = ((front * cosine - back * sine) * scale).astype(target.dtype)
                target[lines, high] = ((front * sine + back * cosine) * scale).astype(target.dtype)

        self.by_rows(rows, slot, slots)

    def contribute(self, head):
        columns = pl.ds(head * KEY, KEY)
        left = self.count - 1.0 - self.position(0, self.count)
        trailing = jnp.exp(self.log_decay(head) * left)
        weighted = (self.keys[:, columns].astype(jnp.float32) * trailing).astype(jnp.bfloat16)
        total = lax.dot_general(
            weighted,
            self.products[1 + head],
            (((0,), (0,)), ((), ())),
            preferred_element_type=jnp.float32,
        )
        self.sending[pl.ds(head * KEY, KEY)] = total.astype(self.sending.dtype)

    def slice_copy(self, s):
        size = self.got.shape[1]
        part = self.sending.at[pl.ds(s * size, size)]
        return remote(
            part,
            self.got.at[self.link],
            self.slice_sems.at[0, s],
            self.slice_sems.at[1, self.link],
            self.chain(s),
        )

    def prefix_copy(self, s):
        size = self.got.shape[1]
        lines = pl.ds(pl.multiple_of(self.link * size, size), size)
        return remote(
            self.prefix.at[s],
            self.state.at[lines],
            self.prefix_sems.at[0, s],
            self.prefix_sems.at[1, self.link],
            self.chain(s),
        )

    def others(self, what):
        for s in range(self.links):
            pl.when(self.link != s)(lambda: what(s))

    def send_slices(self):
        self.others(lambda s: self.slice_copy(s).start())
        size = self.got.shape[1]
        lines = pl.ds(pl.multiple_of(self.link * size, size), size)
        self.got[self.link] = self.sending[lines]

    def scan(self):
        size = self.got.shape[1]

        def arrived(s):
            part = self.got.at[s]
            remote(
                part, part, self.slice_sems.at[0, s], self.slice_sems.at[1, s], self.chain(s)
            ).wait_recv()

        self.others(arrived)
        step = jnp.exp(
            jnp.full((1, 1), self.log_decay(self.link * size // KEY) * self.count, jnp.float32)
        )
        state = jnp.zeros(self.got.shape[1:], jnp.float32)
        for s in range(self.links):
            self.prefix[s] = state.astype(self.prefix.dtype)
            state = state * step + self.got[s].astype(jnp.float32)
        self.others(lambda s: self.prefix_copy(s).start())
        lines = pl.ds(pl.multiple_of(self.link * size, size), size)
        self.state[lines] = self.prefix[self.link]

    def state_arrived(self):
        size = self.got.shape[1]

        def arrived(s):
            part = self.state.at[pl.ds(s * size, size)]
            remote(
                part, part, self.prefix_sems.at[0, s], self.prefix_sems.at[1, s], self.chain(s)
            ).wait_recv()

        self.others(arrived)

    def inside(self, head, slot, slots):
        columns = pl.ds(head * KEY, KEY)
        decay = self.log_decay(head)

        def rows(first):
            lines = pl.ds(first, 128)
            scores = contract(self.queries[lines, columns], self.keys[:, columns])
            later = lax.broadcasted_iota(jnp.int32, scores.shape, 0) + first
            ahead = later - lax.broadcasted_iota(jnp.int32, scores.shape, 1)
            weight = jnp.exp(decay * jnp.maximum(ahead, 0).astype(jnp.float32))
            scores = jnp.where(ahead >= 0, scores * weight, 0.0).astype(jnp.bfloat16)
            self.within[head, lines] = jnp.dot(
                scores, self.products[1 + head], preferred_element_type=jnp.float32
            )

        self.by_rows(rows, slot, slots)

    def finish_head(self, head, slot, slots):
        columns = pl.ds(head * KEY, KEY)
        decay = self.log_decay(head)

        def rows(first):
            lines = pl.ds(first, 128)
            cross = jnp.dot(
                self.queries[lines, columns],
                self.state[pl.ds(head * KEY, KEY)],
                preferred_element_type=jnp.float32,
            )
            leading = jnp.exp(decay * (self.position(first, 128) + 1.0))
            raw = self.within[head, lines] + cross * leading
            average = jnp.mean(raw, axis=-1, keepdims=True)
            centred = raw - average
            wide = jnp.mean(jnp.square(centred), axis=-1, keepdims=True)
            switch = self.products[7 + head, lines].astype(jnp.float32)
            result = centred * lax.rsqrt(wide + group_eps) * jax.nn.silu(switch)
            self.hidden[lines, pl.ds(head * VAL, VAL)] = result.astype(self.hidden.dtype)

        self.by_rows(rows, slot, slots)


    def glu(self, slot=0, slots=1):
        lead = self.halo_in.shape[0]

        def rows(first):
            lines = pl.ds(first, 128)
            value = self.products[4, lines].astype(jnp.float32)
            switch = self.products[5, lines].astype(jnp.float32)
            gated = (value * jax.nn.sigmoid(switch)).astype(jnp.bfloat16)
            self.padded[pl.ds(pl.multiple_of(first + lead, 8), 128)] = gated.astype(jnp.float32)

        self.by_rows(rows, slot, slots)
        self.halo_out[...] = self.padded[pl.ds(self.count, lead)].astype(jnp.bfloat16)
        self.padded[pl.ds(self.count + lead, 8)] = jnp.zeros(
            (8, self.padded.shape[1]), jnp.float32
        )
        pl.when(self.link < self.links - 1)(lambda: self.halo_copy().start())

    def halo_copy(self):
        following = jnp.minimum(self.link + 1, self.links - 1)
        return remote(
            self.halo_out,
            self.halo_in,
            self.halo_sems.at[0],
            self.halo_sems.at[1],
            self.chain(following),
        )

    def halo(self):
        lead = self.halo_in.shape[0]
        channels = self.padded.shape[1]

        @pl.when(self.link > 0)
        def _():
            self.halo_copy().wait_recv()
            self.padded[pl.ds(0, lead)] = self.halo_in[...].astype(jnp.float32)

        @pl.when(self.link == 0)
        def _():
            self.padded[pl.ds(0, lead)] = jnp.zeros((lead, channels), jnp.float32)

    def convolve(self, slot, slots):
        lead = self.halo_in.shape[0]
        channels = self.padded.shape[1]
        size = 64
        lanes = 128

        def rows(first):
            for part in range(channels // lanes):
                columns = pl.ds(part * lanes, lanes)
                spot = pl.multiple_of(self.rank * channels + part * lanes, lanes)
                weights = self.taps[:, pl.ds(spot, lanes)]
                source = self.padded[pl.ds(first, size + lead + 8), columns]
                total = None
                for low in range(8):
                    group = None
                    for high in range(lead // 8 + 1):
                        tap = high * 8 + low - (lead - KW + 1)
                        if not 0 <= tap < KW:
                            continue
                        term = source[high * 8 : high * 8 + size + 8] * weights[tap : tap + 1]
                        group = term if group is None else group + term
                    if low:
                        group = pltpu.roll(group, size + 8 - low, 0)
                    total = group[:size] if total is None else total + group[:size]
                self.summed[pl.ds(first, size), columns] = total

        self.by_rows(rows, slot, slots, size)

    def finish_convolution(self, slot, slots):
        channels = self.padded.shape[1]
        spot = pl.ds(pl.multiple_of(self.rank * channels, channels), channels)
        gain, shift = self.gain[:, spot], self.shift[:, spot]

        def rows(first):
            lines = pl.ds(first, 128)
            total = self.summed[lines]
            average = jnp.mean(total, axis=-1, keepdims=True)
            centred = total - average
            wide = jnp.mean(jnp.square(centred), axis=-1, keepdims=True)
            normalized = centred * lax.rsqrt(wide + layer_eps) * gain + shift
            switch = self.products[6, lines].astype(jnp.float32)
            result = jax.nn.silu(normalized) * jax.nn.silu(switch)
            target = pl.ds(self.heads * VAL, channels)
            self.hidden[lines, target] = result.astype(self.hidden.dtype)

        self.by_rows(rows, slot, slots)


    def x_copy(self, n):
        zh, zl, y, x, c = self.at
        return remote(
            self.sent.at[n],
            self.crossed.at[n],
            self.out_sems.at[0, n],
            self.out_sems.at[1, n],
            (zh, zl, y, 1 - x, c),
        )

    def near_copy(self, n):
        zh, zl, y, x, c = self.at
        share = self.out.shape[0]
        part = self.half.at[n, pl.ds(pl.multiple_of((1 - c) * share, share), share)]
        return remote(
            part,
            self.here.at[n],
            self.out_sems.at[2, n],
            self.out_sems.at[3, n],
            (zh, zl, y, x, 1 - c),
        )

    def far_copy(self, n, core):
        zh, zl, y, x, c = self.at
        share = self.out.shape[0]
        return remote(
            self.half.at[n, pl.ds(core * share, share)],
            self.there.at[n],
            self.out_sems.at[2 + 2 * core, n],
            self.out_sems.at[5, n],
            (c, zl, y, x, core),
        )

    def multiply(self, j, q, weights):
        x = self.at[3]
        tile = self.sent.shape[2]
        n = j * 4 + q
        pair = self.sent.shape[1]
        lines = pl.ds(pl.multiple_of(q * tile, tile), tile)
        total = contract(self.hidden[...], weights[j, lines])
        low, high = total[:pair], total[pair:]
        self.kept[n] = jnp.where(x == 0, low, high)
        self.sent[n] = jnp.where(x == 0, high, low).astype(self.sent.dtype)
        self.x_copy(n).start()

    def join(self, n):
        zh, zl, y, x, c = self.at
        self.x_copy(n).wait_recv()
        total = self.kept[n] + self.crossed[n].astype(jnp.float32)
        self.half[n] = total.astype(self.half.dtype)

        @pl.when(c == zh)
        def _():
            self.near_copy(n).start()

        @pl.when(c != zh)
        def _():
            self.far_copy(n, 0).start()
            self.far_copy(n, 1).start()

    def close(self, j, q):
        zh, zl, y, x, c = self.at
        n = j * 4 + q
        share = self.out.shape[0]
        wide = self.sent.shape[2] // 2
        part = self.there.at[n]
        remote(
            part, part, self.out_sems.at[4, n], self.out_sems.at[5, n], (zh, zl, y, 1 - x, c)
        ).wait_recv()
        far_part = self.there[n].astype(jnp.float32)

        def store(near_part):
            total = (near_part.astype(jnp.float32) + far_part).astype(self.out.dtype)
            for k in range(2):
                spot = ((2 * q + k) * 2 + j) * wide
                self.out[:, pl.ds(spot, wide)] = total[:, k * wide : (k + 1) * wide]

        @pl.when(c == zh)
        def _():
            store(self.half[n, pl.ds(pl.multiple_of(c * share, share), share)])

        @pl.when(c != zh)
        def _():
            self.near_copy(n).wait_recv()
            store(self.here[n])

    def drain(self):
        zh, zl, y, x, c = self.at
        self.drain_rows()
        self.others(lambda s: self.slice_copy(s).wait_send())
        self.others(lambda s: self.prefix_copy(s).wait_send())
        pl.when(self.link < self.links - 1)(lambda: self.halo_copy().wait_send())
        for n in range(self.sent.shape[0]):
            self.x_copy(n).wait_send()

            @pl.when(c == zh)
            def _():
                self.near_copy(n).wait_send()

            @pl.when(c != zh)
            def _():
                self.far_copy(n, 0).wait_send()
                self.far_copy(n, 1).wait_send()


def layer_kernel(layout, out_layout, *refs):
    blocks, refs = refs[:9], refs[9:]
    first_gather, refs = refs[-12:-6], refs[:-12] + refs[-6:]
    second_gather, refs = refs[-6:], refs[:-6]
    layer = Layer(refs)
    inward, outward = Gather(*first_gather), Gather(*second_gather)
    units = len(layout)
    total = units + 2

    for n in range(3):
        layer.load(n).start()
    for k, (which, first) in enumerate(layout):
        inward.load(k, blocks[which].at[:, pl.ds(first, inward.source.shape[2])], None)
    for k, parts in enumerate(out_layout):
        for which, row, column in parts:
            ref = blocks[which]
            lines = pl.ds(row, outward.depth)
            outward.load(k, ref.at[lines], pl.ds(column, ref.shape[1]))

    def at_unit(k, what):
        @pl.when(jnp.logical_and(k >= 0, k < units))
        def _():
            what(inward, k)

        @pl.when(jnp.logical_and(k >= units, k < total))
        def _():
            what(outward, k - units)

    meet()

    def first_sends(own, ahead):
        for k in range(ahead):
            if k < units:
                inward.begin(k, own)
            else:
                outward.begin(k - units, own)

    pl.when(inward.is_own)(lambda: first_sends(True, OWN_AHEAD))
    pl.when(jnp.logical_not(inward.is_own))(lambda: first_sends(False, FAR_AHEAD))
    layer.near_rows()
    layer.far_strip(0).start()

    def next_sends(i):
        @pl.when(inward.is_own)
        def _():
            at_unit(i + OWN_AHEAD, lambda gather, k: gather.begin(k, True))

        @pl.when(jnp.logical_not(inward.is_own))
        def _():
            at_unit(i + FAR_AHEAD, lambda gather, k: gather.begin(k, False))

    inside, finish_head = layer.inside, layer.finish_head
    key_scale = KEY ** (-0.5)
    after = (
        (lambda n: layer.rotate(0, layer.keys, key_scale, n, 2),) * 2,
        (lambda n: layer.contribute(0), None),
        (lambda n: (layer.contribute(1), layer.send_slices()), None),
        (lambda n: layer.rotate(3, layer.queries, 1.0, n, 2),) * 2,
        (lambda n: inside(0, 0, 1), None),
        (lambda n: layer.glu(), lambda n: inside(1, 0, 1)),
        (lambda n: layer.scan(), lambda n: (layer.halo(), layer.convolve(0, 1))),
        (lambda n: layer.finish_convolution(0, 1), None),
        (
            lambda n: layer.state_arrived(),
            lambda n: (finish_head(0, 0, 1), finish_head(1, 0, 1)),
        ),
    )

    def compute(k, carry):
        inward.complete_own(k)
        inward.complete_far(k)
        layer.project(k, inward.full, 0, 2)
        layer.project(k, inward.full, 1, 2)
        for unit, events in enumerate(after):

            @pl.when(k == unit)
            def _():
                for n, event in enumerate(events):
                    if event is not None:
                        event(n)

        return carry

    def relay(k, number):
        at_unit(k, lambda gather, k: gather.stage(k, number))

    for number in (0, 1, 4):
        for k in range(LEADS[number]):
            relay(k, number)

    layer.tables()

    def ready(i):
        return jnp.clip(2 * (i - START), 0, jnp.clip(i + 1 - BEHIND, 0, units))

    def step(i, carry):
        relay(i + LEADS[0], 0)
        relay(i + LEADS[1], 1)
        pl.when(jnp.logical_and(i >= 0, i < STRIPS - 1))(lambda: layer.far_strip(i + 1).start())
        next_sends(i)

        @pl.when(jnp.logical_and(i >= ROWS_RELAY, i < ROWS_RELAY + STRIPS))
        def _():
            layer.relay_rows(i - ROWS_RELAY)

        relay(i, 2)
        relay(i + LEADS[4], 4)
        relay(i - 1, 3)
        pl.when(i == START + 1)(layer.all_rows)
        lax.fori_loop(ready(i - 1), ready(i), compute, 0)
        return carry

    lax.fori_loop(0, units + 1, step, 0)
    lax.fori_loop(ready(units), units, compute, 0)

    zh = layer.at[0]

    def tiles(j, half, what):
        for m in range(2):
            what(j, half * 2 + m)

    def multiply(j, q):
        layer.multiply(j, q, outward.full)

    def join(j, q):
        layer.join(j * 4 + q)

    for k in range(units + 1 + LEADS[4], total):
        relay(k, 4)
    outward.complete_own(0)
    tiles(0, zh, multiply)
    relay(units, 3)
    outward.complete_own(1)
    tiles(1, zh, multiply)
    relay(units + 1, 2)
    outward.complete_far(0)
    tiles(0, 1 - zh, multiply)
    tiles(0, zh, join)
    tiles(1, zh, join)
    relay(units + 1, 3)
    outward.complete_far(1)
    tiles(1, 1 - zh, multiply)
    tiles(0, 1 - zh, join)
    tiles(1, 1 - zh, join)
    for j in range(2):
        for q in range(4):
            layer.close(j, q)

    def finish(gather):
        def body(k, carry):
            gather.drain(k)
            return carry

        lax.fori_loop(0, gather.source.shape[0], body, 0)

    finish(inward)
    finish(outward)
    layer.drain()


def whole_layer(tokens, norm_gain, taps, gain, shift, blocks):
    depth, width = blocks[0].shape
    share, model = tokens.shape
    layout = []
    for which, block in enumerate(blocks[:7]):
        layout += [(which, first) for first in range(0, block.shape[1], width)]
    units = len(layout)
    shares, dtype = 8, tokens.dtype
    span = 4 * share
    wide = KEY // 2
    frequency = rope_base ** (-np.arange(wide) / wide)
    angles = [np.arange(span)[:, None] * frequency]
    angles += [span * np.arange(shares)[:, None] * frequency]
    angles, turns = (np.stack([np.cos(a), np.sin(a)]).astype(np.float32) for a in angles)
    inner_width = blocks[7].shape[1] + blocks[8].shape[1]
    half_depth = depth // 2
    out_layout = [
        ((7, j * half_depth, 0), (8, j * half_depth, blocks[7].shape[1])) for j in range(2)
    ]
    heads = width // KEY
    channels = blocks[8].shape[1]
    lead = (KW + 7) // 8 * 8
    tile = 2 * half_depth
    tiles = model // tile
    sem = pltpu.SemaphoreType.DMA
    slice_rows = heads * KEY // shares
    return pl.pallas_call(
        lambda *refs: layer_kernel(layout, out_layout, *refs),
        out_shape=jax.ShapeDtypeStruct((share, model), dtype),
        in_specs=[pl.BlockSpec(memory_space=pl.ANY)] * 11
        + [pl.BlockSpec(memory_space=pltpu.VMEM), pl.BlockSpec(memory_space=pl.ANY)]
        + [pl.BlockSpec(memory_space=pltpu.VMEM)] * 3,
        out_specs=pl.BlockSpec(memory_space=pltpu.VMEM),
        scratch_shapes=[
            pltpu.VMEM((share, model), dtype),
            pltpu.VMEM(angles.shape, jnp.float32),
            pltpu.VMEM(taps.shape, jnp.float32),
            pltpu.VMEM((share, model), dtype),
            pltpu.VMEM((span, wide), jnp.float32),
            pltpu.VMEM((span, wide), jnp.float32),
            pltpu.VMEM((span, model), dtype),
            pltpu.VMEM((units, span, width), dtype),
            pltpu.VMEM((span, width), dtype),
            pltpu.VMEM((span, width), dtype),
            pltpu.VMEM((heads, span, VAL), jnp.float32),
            pltpu.VMEM((heads * KEY, VAL), dtype),
            pltpu.VMEM((shares, slice_rows, VAL), dtype),
            pltpu.VMEM((shares, slice_rows, VAL), dtype),
            pltpu.VMEM((heads * KEY, VAL), dtype),
            pltpu.VMEM((span + lead + 8, channels), jnp.float32),
            pltpu.VMEM((lead, channels), dtype),
            pltpu.VMEM((lead, channels), dtype),
            pltpu.VMEM((span, channels), jnp.float32),
            pltpu.VMEM((span, inner_width), dtype),
            pltpu.VMEM((tiles, 2 * share, tile), jnp.float32),
            pltpu.VMEM((tiles, 2 * share, tile), dtype),
            pltpu.VMEM((tiles, 2 * share, tile), dtype),
            pltpu.VMEM((tiles, 2 * share, tile), dtype),
            pltpu.VMEM((tiles, share, tile), dtype),
            pltpu.VMEM((tiles, share, tile), dtype),
            sem((2 + 3 * STRIPS,)),
            sem((4, STRIPS)),
            sem((2, shares)),
            sem((2, shares)),
            sem((2,)),
            sem((6, tiles)),
            sem((3,)),
        ]
        + gather_scratch(units, depth, width, shares, dtype)
        + gather_scratch(2, half_depth, inner_width, shares, dtype),
        compiler_params=pltpu.CompilerParams(
            has_side_effects=True, collective_id=0, vmem_limit_bytes=60 << 20
        ),
        name="layer",
    )(*blocks, tokens, angles, turns, taps, norm_gain, gain, shift)


def local_squares(
    tokens,
    norm_gain,
    query_weight,
    key_weight,
    value_weight,
    retain_gate,
    unit_value,
    unit_gate,
    convolve_gate,
    filter_taps,
    layer_gain,
    layer_shift,
    retain_output,
    convolve_output,
):
    blocks = (key_weight, value_weight, query_weight, unit_value, unit_gate, convolve_gate)
    blocks += (retain_gate, retain_output, convolve_output)
    return whole_layer(
        tokens,
        norm_gain[None],
        filter_taps,
        layer_gain[None],
        layer_shift[None],
        blocks,
    )


def squares(mesh):
    boxes = Mesh(mesh.devices.reshape(2, 2, 2, 2, 2), SQUARE)
    rows, blocks = P(SQUARE, None), P(("zh", "zl", "y"), ("x", "c"))
    return jax.shard_map(
        local_squares,
        mesh=boxes,
        in_specs=(rows, P()) + (blocks,) * 7 + (P(),) * 3 + (blocks,) * 2,
        out_specs=rows,
        check_vma=False,
    )


def solution(mesh):
    sp, tp = mesh.shape["sp"], mesh.shape["tp"]
    if (sp, tp) == (8, 4):
        return squares(mesh)
    planes = Mesh(mesh.devices.reshape(tp, sp // tp, tp), ("hi", "lo", "tp"))
    return jax.shard_map(
        local,
        mesh=planes,
        in_specs=(
            P(("hi", "lo", "tp"), None),
            P(),
            P(("hi", "lo"), "tp"),
            P(("hi", "lo"), "tp"),
            P(("hi", "lo"), "tp"),
            P(("hi", "lo"), "tp"),
            P(("hi", "lo"), "tp"),
            P(("hi", "lo"), "tp"),
            P(("hi", "lo"), "tp"),
            P(),
            P(),
            P(),
            P(("hi", "lo"), "tp"),
            P(("hi", "lo"), "tp"),
        ),
        out_specs=P(("hi", "lo", "tp"), None),
        check_vma=False,
    )
```

```python
import math

import jax
import jax.numpy as jnp
import numpy as np
from jax import lax
from jax.experimental import pallas as pl
from jax.experimental.pallas import tpu as pltpu
from jax.sharding import Mesh
from jax.sharding import PartitionSpec as P

KEY = 256
VAL = 512
GROUP = 512
KW = 31


rms_eps = 1e-06
group_eps = 1.0
layer_eps = 0.001
rope_base = 10000.0


SPANS = ("tp", "lo")


def swap_planes(x):
    size = lax.axis_size("tp")
    pairs = [(h * size + t, t * size + h) for h in range(size) for t in range(size)]
    return lax.ppermute(x, ("hi", "tp"), pairs)


def from_behind(x, by):
    outer, inner = lax.axis_size("tp"), lax.axis_size("lo")
    spot = [(i % inner) * outer + i // inner for i in range(outer * inner)]
    return lax.ppermute(x, ("lo", "tp"), list(zip(spot[:-by], spot[by:])))


def carried_in(contribution, log_span_decay):
    length = lax.axis_size(SPANS)
    state = from_behind(contribution.astype(jnp.bfloat16), 1).astype(jnp.float32)
    by = 1
    while by < length:
        earlier = from_behind(state.astype(jnp.bfloat16), by).astype(jnp.float32)
        state = state + jnp.exp(log_span_decay * by)[:, None, None] * earlier
        by *= 2
    return state


def rms_normalize(tokens, norm_gain):
    widened = tokens.astype(jnp.float32)
    scaled = widened * lax.rsqrt(jnp.mean(widened * widened, axis=-1, keepdims=True) + rms_eps)
    return (scaled * norm_gain).astype(jnp.bfloat16)


def rotate(vectors, positions):
    half_width = vectors.shape[-1] // 2
    frequency = rope_base ** (-jnp.arange(half_width, dtype=jnp.float32) / half_width)
    angles = positions.astype(jnp.float32)[:, None] * frequency
    cosine = jnp.cos(angles)[:, None, :]
    sine_part = jnp.sin(angles)[:, None, :]
    front_half = vectors[..., :half_width]
    back_half = vectors[..., half_width:]
    return jnp.concatenate(
        [front_half * cosine - back_half * sine_part, front_half * sine_part + back_half * cosine],
        axis=-1,
    )


def prepare(queries, key_rows, values, positions):
    row_count = queries.shape[0]
    rotated_query = rotate(
        queries.astype(jnp.float32).reshape(row_count, -1, KEY), positions
    ).astype(jnp.bfloat16)
    rotated_keys = (
        rotate(key_rows.astype(jnp.float32).reshape(row_count, -1, KEY), positions) * KEY ** (-0.5)
    ).astype(jnp.bfloat16)
    value_heads = values.reshape(row_count, -1, VAL)
    return (rotated_query, rotated_keys, value_heads)


def decay_logs(first_head, head_total, all_heads, seq_length):
    ratio = (first_head + jnp.arange(head_total)).astype(jnp.float32) / (all_heads - 1)
    return (jnp.log(0.05) + ratio * jnp.log(18.0)) / seq_length


def local_parts(queries, key_rows, values, log_decay):
    row_count = queries.shape[0]
    indices = jnp.arange(row_count, dtype=jnp.float32)
    offsets = indices[:, None] - indices[None, :]
    causal = offsets >= 0
    weight = jnp.where(
        causal[None], jnp.exp(log_decay[:, None, None] * jnp.where(causal, offsets, 0.0)[None]), 0.0
    )
    scores = (
        jnp.einsum("ihd,jhd->hij", queries, key_rows, preferred_element_type=jnp.float32) * weight
    ).astype(jnp.bfloat16)
    within = jnp.einsum("hij,jhe->ihe", scores, values, preferred_element_type=jnp.float32)
    trailing = jnp.exp(log_decay[None, :] * (row_count - 1.0 - indices)[:, None])
    weighted = (key_rows.astype(jnp.float32) * trailing[:, :, None]).astype(jnp.bfloat16)
    contribution = jnp.einsum("jhd,jhe->hde", weighted, values, preferred_element_type=jnp.float32)
    return (within, contribution)


def cross_part(queries, carry_state, log_decay):
    row_count = queries.shape[0]
    indices = jnp.arange(row_count, dtype=jnp.float32)
    leading = jnp.exp(log_decay[None, :] * (indices + 1.0)[:, None])
    return (
        jnp.einsum(
            "ihd,hde->ihe",
            queries,
            carry_state.astype(jnp.bfloat16),
            preferred_element_type=jnp.float32,
        )
        * leading[:, :, None]
    )


def retain_finish(raw, switch):
    average = jnp.mean(raw, axis=-1, keepdims=True)
    spread = jnp.mean(jnp.square(raw - average), axis=-1, keepdims=True)
    normalized = ((raw - average) * lax.rsqrt(spread + group_eps)).reshape(raw.shape[0], -1)
    return (normalized * jax.nn.silu(switch.astype(jnp.float32))).astype(jnp.bfloat16)


def convolve_branch(gated_input, before, tap_slice, gain_slice, shift_slice, switch):
    padded = jnp.concatenate([before, gated_input], axis=0)
    row_count = gated_input.shape[0]
    summed = jnp.zeros(gated_input.shape, jnp.float32)
    for tap_index in range(tap_slice.shape[0]):
        summed = (
            summed
            + padded[tap_index : tap_index + row_count].astype(jnp.float32) * tap_slice[tap_index]
        )
    grouped = summed.reshape(row_count, -1, GROUP)
    average = jnp.mean(grouped, axis=-1, keepdims=True)
    spread = jnp.mean(jnp.square(grouped - average), axis=-1, keepdims=True)
    normalized = ((grouped - average) * lax.rsqrt(spread + layer_eps)).reshape(row_count, -1)
    normalized = normalized * gain_slice + shift_slice
    return (jax.nn.silu(normalized) * jax.nn.silu(switch.astype(jnp.float32))).astype(jnp.bfloat16)


def contract(hidden, matrix):
    return lax.dot_general(
        hidden, matrix, (((1,), (1,)), ((), ())), preferred_element_type=jnp.float32
    )


def local(
    tokens,
    norm_gain,
    query_weight,
    key_weight,
    value_weight,
    retain_gate,
    unit_value,
    unit_gate,
    convolve_gate,
    filter_taps,
    layer_gain,
    layer_shift,
    retain_output,
    convolve_output,
):
    head_groups = lax.axis_size("hi")
    chain_length = lax.axis_size(SPANS)
    head_rank = lax.axis_index("hi")
    chain_rank = lax.axis_index(SPANS)
    def project(rows, merged, *matrices):
        product = jnp.dot(rows, merged, preferred_element_type=jnp.float32).astype(jnp.bfloat16)
        ends = [sum(m.shape[1] for m in matrices[: k + 1]) for k in range(len(matrices) - 1)]
        return jnp.split(product, ends, axis=1)

    first = (key_weight, value_weight, query_weight)
    second = (unit_value, unit_gate, convolve_gate, retain_gate)
    third = (retain_output, convolve_output)
    groups = (first, second, third)
    merged = [jnp.concatenate(group, axis=1) for group in groups]
    normed = rms_normalize(tokens, norm_gain)
    normed = lax.all_gather(swap_planes(normed), "hi", axis=0, tiled=True)
    merged = [lax.all_gather(swap_planes(m), SPANS, axis=0, tiled=True) for m in merged]
    key_rows, values, queries = project(normed, merged[0], *first)
    glu_value, glu_switch, convolve_switch, retain_switch = project(normed, merged[1], *second)
    out_full = merged[2]
    row_count = normed.shape[0]
    local_heads = queries.shape[1] // KEY
    positions = chain_rank * row_count + jnp.arange(row_count, dtype=jnp.int32)
    rotated_query, rotated_keys, value_heads = prepare(queries, key_rows, values, positions)
    log_decay = decay_logs(
        head_rank * local_heads, local_heads, local_heads * head_groups, row_count * chain_length
    )
    within, contribution = local_parts(rotated_query, rotated_keys, value_heads, log_decay)
    gated_input = (
        glu_value.astype(jnp.float32) * jax.nn.sigmoid(glu_switch.astype(jnp.float32))
    ).astype(jnp.bfloat16)
    channels = gated_input.shape[1]
    before = from_behind(gated_input[row_count - (KW - 1) :], 1)
    incoming = carried_in(contribution, log_decay * row_count)
    raw = within + cross_part(rotated_query, incoming, log_decay)
    retain_hidden = retain_finish(raw, retain_switch)
    tap_slice = lax.dynamic_slice_in_dim(filter_taps, head_rank * channels, channels, 1)
    gain_slice = lax.dynamic_slice_in_dim(layer_gain, head_rank * channels, channels, 0)
    shift_slice = lax.dynamic_slice_in_dim(layer_shift, head_rank * channels, channels, 0)
    convolve_hidden = convolve_branch(
        gated_input, before, tap_slice, gain_slice, shift_slice, convolve_switch
    )
    hidden = jnp.concatenate([retain_hidden, convolve_hidden], axis=1)
    mixed = contract(hidden, out_full).astype(jnp.bfloat16)
    return swap_planes(lax.psum_scatter(mixed, "hi", scatter_dimension=0, tiled=True))


OWN_AHEAD = 4
FAR_AHEAD = 2
LEADS = (1, 1, 0, -1, 0)
STRIPS = 4
ROWS_RELAY = 1
START = 4
BEHIND = 1
MESH = pl.DeviceIdType.MESH
SQUARE = ("zh", "zl", "y", "x", "c")
CHAIN = ("c", "zl", "y")


def remote(source, target, out_sem, in_sem, device):
    return pltpu.make_async_remote_copy(
        src_ref=source,
        dst_ref=target,
        send_sem=out_sem,
        recv_sem=in_sem,
        device_id=device,
        device_id_type=MESH,
    )


def place():
    return tuple(lax.axis_index(name) for name in SQUARE)


def meet():
    zh, zl, y, x, c = place()
    barrier = pltpu.get_barrier_semaphore()
    peers = []
    for n in range(1, 16):
        flips = [(n >> bit) & 1 for bit in range(4)]
        a, b, d, e = (1 - v if flip else v for v, flip in zip((zh, zl, y, c), flips))
        peers.append((a, b, d, x, e))
    peers += [(zh, zl, y, 1 - x, c), (zh, zl, y, 1 - x, 1 - c)]
    for peer in peers:
        pl.semaphore_signal(barrier, inc=1, device_id=peer, device_id_type=MESH)
    return lambda: pl.semaphore_wait(barrier, len(peers))


class Gather:
    def __init__(self, source, full, near, send, arrive, beside):
        self.source, self.full, self.near = source, full, near
        self.send, self.arrive, self.beside = send, arrive, beside
        zh, zl, y, x, c = self.at = place()
        self.depth = source.shape[1]
        self.half = self.depth // 2
        self.outer = zl * zh + (1 - zl) * (1 - zh)
        self.mine = self.index(zh, self.outer, y)
        self.is_own = c == zh

    def index(self, zh, outer, y):
        zl = outer * zh + (1 - outer) * (1 - zh)
        return (zh * 2 + zl) * 2 + y

    def own(self, outer, flip):
        return self.index(self.at[0], outer, self.at[2] if not flip else 1 - self.at[2])

    def far(self, outer, flip):
        return self.index(1 - self.at[0], outer, self.at[2] if not flip else 1 - self.at[2])

    def rows(self, k, s, half):
        start = pl.multiple_of(s * self.depth + half * self.half, self.half)
        return self.full.at[k, pl.ds(start, self.half)]

    def whole(self, k, s):
        return self.full.at[k, pl.ds(pl.multiple_of(s * self.depth, self.depth), self.depth)]

    def z_mate(self, core):
        zh, zl, y, x, c = self.at
        return (zh, 1 - zl, y, x, core)

    def y_mate(self, core):
        zh, zl, y, x, c = self.at
        return (zh, zl, 1 - y, x, core)

    def sibling(self):
        zh, zl, y, x, c = self.at
        return (zh, zl, y, x, 1 - c)

    def load(self, k, part, columns):
        columns = pl.ds(0, self.source.shape[2]) if columns is None else columns

        @pl.when(self.is_own)
        def _():
            target = self.whole(k, self.mine).at[:, columns]
            pltpu.make_async_copy(part, target, self.near.at[k]).start()

        @pl.when(jnp.logical_not(self.is_own))
        def _():
            target = self.source.at[k].at[:, columns]
            pltpu.make_async_copy(part, target, self.near.at[k]).start()

    def own_sends(self, k):
        zh, zl, y, x, c = self.at
        part = self.whole(k, self.mine)
        copies = [remote(part, part, self.send.at[k, 16], self.beside.at[k], self.sibling())]
        for r in range(2):
            piece = self.rows(k, self.mine, r)
            arrive = self.arrive.at[k, self.mine, r]
            copies.append(remote(piece, piece, self.send.at[k, 12 + r], arrive, self.z_mate(r)))
            copies.append(remote(piece, piece, self.send.at[k, 14 + r], arrive, self.y_mate(r)))
        return copies

    def far_sends(self, k):
        zh, zl, y, x, c = self.at
        copies = []
        for r in range(2):
            piece = self.source.at[k, pl.ds(r * self.half, self.half)]
            copies.append(
                remote(
                    piece,
                    self.rows(k, self.mine, r),
                    self.send.at[k, 12 + r],
                    self.arrive.at[k, self.mine, r],
                    (c, 1 - c, y, x, r),
                )
            )
        return copies

    def begin(self, k, own):
        pltpu.make_async_copy(self.source.at[k], self.source.at[k], self.near.at[k]).wait()
        for copy in self.own_sends(k) if own else self.far_sends(k):
            copy.start()

    def onward(self, k, s, device, slot):
        piece = self.rows(k, s, self.at[4])
        return remote(piece, piece, self.send.at[k, slot], self.arrive.at[k, s, self.at[4]], device)

    def landed(self, k, s, half):
        piece = self.rows(k, s, half)
        remote(
            piece, piece, self.send.at[k, 0], self.arrive.at[k, s, half], self.sibling()
        ).wait_recv()

    def table(self):
        c = self.at[4]
        z_mate, y_mate, sibling = self.z_mate(c), self.y_mate(c), self.sibling()
        inner = (
            (
                (self.far(0, 0), ((z_mate, 0, None), (y_mate, 1, None), (sibling, 2, None))),
                (self.far(1, 0), ((z_mate, 3, None), (y_mate, 4, None), (sibling, 5, None))),
            ),
            (
                (self.own(0, 1), ((z_mate, 8, 0), (sibling, 7, None))),
                (self.own(1, 0), ((sibling, 6, None),)),
            ),
            (
                (self.far(0, 1), ((sibling, 9, None),)),
                (self.far(1, 1), ((sibling, 10, None),)),
            ),
            (),
            ((self.own(1, 1), ((sibling, 11, None),)),),
        )
        outer = (
            (),
            (
                (self.own(1, 1), ((z_mate, 2, None), (sibling, 3, None))),
                (self.own(0, 0), ((y_mate, 1, 1), (sibling, 0, None))),
            ),
            (
                (self.far(0, 0), ((y_mate, 4, None), (sibling, 5, None))),
                (self.far(1, 0), ((y_mate, 6, None), (sibling, 7, None))),
            ),
            (
                (self.far(0, 1), ((sibling, 8, None),)),
                (self.far(1, 1), ((sibling, 9, None),)),
            ),
            ((self.own(0, 1), ((sibling, 10, None),)),),
        )
        return inner, outer

    def stage(self, k, number):
        for role, moves in enumerate(self.table()):
            if not moves[number]:
                continue

            @pl.when(self.outer == role)
            def _():
                for s, targets in moves[number]:
                    self.landed(k, s, self.at[4])
                    for device, slot, lane in targets:
                        copy = self.onward(k, s, device, slot)
                        if lane is None:
                            copy.start()
                        else:
                            pl.when(self.at[4] == lane)(copy.start)

    def complete_own(self, k):
        other = 1 - self.at[4]
        for outer, flip in ((1 - self.outer, 0), (self.outer, 1), (1 - self.outer, 1)):
            self.landed(k, self.own(outer, flip), other)

        @pl.when(jnp.logical_not(self.is_own))
        def _():
            part = self.whole(k, self.mine)
            remote(
                part, part, self.send.at[k, 0], self.beside.at[k], self.sibling()
            ).wait_recv()

    def complete_far(self, k):
        other = 1 - self.at[4]
        for outer, flip in ((0, 0), (1, 0), (0, 1), (1, 1)):
            self.landed(k, self.far(outer, flip), other)

    def drain(self, k):
        @pl.when(self.is_own)
        def _():
            for copy in self.own_sends(k):
                copy.wait_send()

        @pl.when(jnp.logical_not(self.is_own))
        def _():
            for copy in self.far_sends(k):
                copy.wait_send()

        for role, moves in enumerate(self.table()):

            @pl.when(self.outer == role)
            def _():
                for number in range(len(moves)):
                    for s, targets in moves[number]:
                        for device, slot, lane in targets:
                            copy = self.onward(k, s, device, slot)
                            if lane is None:
                                copy.wait_send()
                            else:
                                pl.when(self.at[4] == lane)(copy.wait_send)


def gather_scratch(units, depth, width, shares, dtype):
    return [
        pltpu.VMEM((units, depth, width), dtype),
        pltpu.VMEM((units, shares * depth, width), dtype),
        pltpu.SemaphoreType.DMA((units,)),
        pltpu.SemaphoreType.DMA((units, 17)),
        pltpu.SemaphoreType.DMA((units, shares, 2)),
        pltpu.SemaphoreType.DMA((units,)),
    ]


class Layer:
    def __init__(self, refs):
        names = (
            "tokens_in",
            "angles_in",
            "turns",
            "taps_in",
            "norm_gain",
            "gain",
            "shift",
            "out",
            "tokens",
            "angles",
            "taps",
            "rows",
            "cosine",
            "sine",
            "normed",
            "products",
            "keys",
            "queries",
            "within",
            "sending",
            "got",
            "prefix",
            "state",
            "padded",
            "halo_out",
            "halo_in",
            "summed",
            "hidden",
            "kept",
            "sent",
            "crossed",
            "half",
            "here",
            "there",
        )
        for name, ref in zip(names, refs):
            setattr(self, name, ref)
        sems = refs[len(names) :]
        (
            self.rows_send,
            self.rows_arrive,
            self.slice_sems,
            self.prefix_sems,
            self.halo_sems,
            self.out_sems,
            self.load_sems,
        ) = sems
        zh, zl, y, x, c = self.at = place()
        self.count = self.normed.shape[0]
        self.heads = self.keys.shape[1] // KEY
        self.rank = x * 2 + zh
        self.link = (c * 2 + zl) * 2 + y
        self.links = 8
        self.groups = 4

    def chain(self, s):
        zh, zl, y, x, c = self.at
        return (zh, (s // 2) % 2, s % 2, x, s // 4)

    def log_decay(self, head):
        ratio = (self.rank * self.heads + head).astype(jnp.float32) / (
            self.heads * self.groups - 1
        )
        return (math.log(0.05) + ratio * math.log(18.0)) / (self.count * self.links)

    def by_rows(self, what, slot=0, slots=1, size=128):
        steps = self.count // size // slots

        def body(n, carry):
            what(pl.multiple_of(n * size, size))
            return carry

        lax.fori_loop(slot * steps, (slot + 1) * steps, body, 0)

    def position(self, first, size):
        rows = lax.broadcasted_iota(jnp.int32, (size, 1), 0) + first
        return rows.astype(jnp.float32)


    def block(self, j):
        share = self.rows.shape[0]
        return self.normed.at[pl.ds(pl.multiple_of(j * share, share), share)]

    def strip(self, j, t):
        share = self.rows.shape[0]
        size = share // STRIPS
        return self.normed.at[pl.ds(pl.multiple_of(j * share + t * size, size), size)]

    def near_copy_of_rows(self, dx):
        zh, zl, y, x, c = self.at
        j = x * 2 + c
        return remote(
            self.rows,
            self.block(j),
            self.rows_send.at[dx],
            self.rows_arrive.at[j, 0],
            (zh, zl, y, 1 - x if dx else x, zh),
        )

    def far_strip(self, t):
        zh, zl, y, x, c = self.at
        j = x * 2 + c
        size = self.rows.shape[0] // STRIPS
        return remote(
            self.rows.at[pl.ds(pl.multiple_of(t * size, size), size)],
            self.strip(j, t),
            self.rows_send.at[2 + t],
            self.rows_arrive.at[j, t],
            (1 - zh, zl, y, x, zh),
        )

    def onward_strip(self, core, t):
        zh, zl, y, x, c = self.at
        j = x * 2 + core
        return remote(
            self.strip(j, t),
            self.strip(j, t),
            self.rows_send.at[2 + (1 + core) * STRIPS + t],
            self.rows_arrive.at[j, t],
            (zh, zl, y, 1 - x, c),
        )

    def rows_landed(self, part, j, t):
        remote(part, part, self.rows_send.at[0], self.rows_arrive.at[j, t], self.chain(0)).wait_recv()

    def load(self, n):
        source = (self.tokens_in, self.angles_in, self.taps_in)[n]
        target = (self.tokens, self.angles, self.taps)[n]
        return pltpu.make_async_copy(source, target, self.load_sems.at[n])

    def near_rows(self):
        zh, zl, y, x, c = self.at
        j = x * 2 + c
        share = self.rows.shape[0]
        self.load(0).wait()
        tokens = self.tokens[...].astype(jnp.float32)
        scaled = tokens * lax.rsqrt(jnp.mean(tokens * tokens, axis=-1, keepdims=True) + rms_eps)
        self.rows[...] = (scaled * self.norm_gain[...]).astype(self.rows.dtype)

        @pl.when(c == zh)
        def _():
            self.normed[pl.ds(pl.multiple_of(j * share, share), share)] = self.rows[...]

        self.near_copy_of_rows(1).start()
        pl.when(c != zh)(lambda: self.near_copy_of_rows(0).start())

    def tables(self):
        self.load(1).wait()
        self.load(2).wait()
        turn_cosine = self.turns[0, pl.ds(self.link, 1)]
        turn_sine = self.turns[1, pl.ds(self.link, 1)]
        cosine, sine = self.angles[0], self.angles[1]
        self.cosine[...] = cosine * turn_cosine - sine * turn_sine
        self.sine[...] = sine * turn_cosine + cosine * turn_sine

    def relay_rows(self, t):
        zh, zl, y, x, c = self.at

        @pl.when(c != zh)
        def _():
            for core in range(2):
                j = x * 2 + core
                self.rows_landed(self.strip(j, t), j, t)
                self.onward_strip(core, t).start()

    def all_rows(self):
        zh, zl, y, x, c = self.at

        @pl.when(c == zh)
        def _():
            for j in range(4):
                pl.when(x * 2 + c != j)(lambda: self.rows_landed(self.block(j), j, 0))

        @pl.when(c != zh)
        def _():
            for core in range(2):
                for t in range(STRIPS):
                    j = (1 - x) * 2 + core
                    self.rows_landed(self.strip(j, t), j, t)

    def drain_rows(self):
        zh, zl, y, x, c = self.at
        self.near_copy_of_rows(1).wait_send()
        for t in range(STRIPS):
            self.far_strip(t).wait_send()

        @pl.when(c != zh)
        def _():
            self.near_copy_of_rows(0).wait_send()
            for core in range(2):
                for t in range(STRIPS):
                    self.onward_strip(core, t).wait_send()


    def project(self, k, weights, part, parts):
        wide = weights.shape[2] // parts
        columns = pl.ds(part * wide, wide)
        self.products[k, :, columns] = jnp.dot(
            self.normed[...], weights[k, :, columns], preferred_element_type=jnp.float32
        ).astype(self.products.dtype)

    def rotate(self, unit, target, scale, slot, slots):
        wide = KEY // 2

        def rows(first):
            lines = pl.ds(first, 128)
            cosine, sine = self.cosine[lines], self.sine[lines]
            for head in range(self.heads):
                low = pl.ds(head * KEY, wide)
                high = pl.ds(head * KEY + wide, wide)
                front = self.products[unit, lines, low].astype(jnp.float32)
                back = self.products[unit, lines, high].astype(jnp.float32)
                target[lines, low] = ((front * cosine - back * sine) * scale).astype(target.dtype)
                target[lines, high] = ((front * sine + back * cosine) * scale).astype(target.dtype)

        self.by_rows(rows, slot, slots)

    def contribute(self, head):
        columns = pl.ds(head * KEY, KEY)
        left = self.count - 1.0 - self.position(0, self.count)
        trailing = jnp.exp(self.log_decay(head) * left)
        weighted = (self.keys[:, columns].astype(jnp.float32) * trailing).astype(jnp.bfloat16)
        total = lax.dot_general(
            weighted,
            self.products[1 + head],
            (((0,), (0,)), ((), ())),
            preferred_element_type=jnp.float32,
        )
        self.sending[pl.ds(head * KEY, KEY)] = total.astype(self.sending.dtype)

    def slice_copy(self, s):
        size = self.got.shape[1]
        part = self.sending.at[pl.ds(s * size, size)]
        return remote(
            part,
            self.got.at[self.link],
            self.slice_sems.at[0, s],
            self.slice_sems.at[1, self.link],
            self.chain(s),
        )

    def prefix_copy(self, s):
        size = self.got.shape[1]
        lines = pl.ds(pl.multiple_of(self.link * size, size), size)
        return remote(
            self.prefix.at[s],
            self.state.at[lines],
            self.prefix_sems.at[0, s],
            self.prefix_sems.at[1, self.link],
            self.chain(s),
        )

    def others(self, what):
        for s in range(self.links):
            pl.when(self.link != s)(lambda: what(s))

    def send_slices(self):
        self.others(lambda s: self.slice_copy(s).start())
        size = self.got.shape[1]
        lines = pl.ds(pl.multiple_of(self.link * size, size), size)
        self.got[self.link] = self.sending[lines]

    def scan(self):
        size = self.got.shape[1]

        def arrived(s):
            part = self.got.at[s]
            remote(
                part, part, self.slice_sems.at[0, s], self.slice_sems.at[1, s], self.chain(s)
            ).wait_recv()

        self.others(arrived)
        step = jnp.exp(
            jnp.full((1, 1), self.log_decay(self.link * size // KEY) * self.count, jnp.float32)
        )
        state = jnp.zeros(self.got.shape[1:], jnp.float32)
        for s in range(self.links):
            self.prefix[s] = state.astype(self.prefix.dtype)
            state = state * step + self.got[s].astype(jnp.float32)
        self.others(lambda s: self.prefix_copy(s).start())
        lines = pl.ds(pl.multiple_of(self.link * size, size), size)
        self.state[lines] = self.prefix[self.link]

    def state_arrived(self):
        size = self.got.shape[1]

        def arrived(s):
            part = self.state.at[pl.ds(s * size, size)]
            remote(
                part, part, self.prefix_sems.at[0, s], self.prefix_sems.at[1, s], self.chain(s)
            ).wait_recv()

        self.others(arrived)

    def inside(self, head, slot, slots):
        columns = pl.ds(head * KEY, KEY)
        decay = self.log_decay(head)

        def rows(first):
            lines = pl.ds(first, 128)
            scores = contract(self.queries[lines, columns], self.keys[:, columns])
            later = lax.broadcasted_iota(jnp.int32, scores.shape, 0) + first
            ahead = later - lax.broadcasted_iota(jnp.int32, scores.shape, 1)
            weight = jnp.exp(decay * jnp.maximum(ahead, 0).astype(jnp.float32))
            scores = jnp.where(ahead >= 0, scores * weight, 0.0).astype(jnp.bfloat16)
            self.within[head, lines] = jnp.dot(
                scores, self.products[1 + head], preferred_element_type=jnp.float32
            )

        self.by_rows(rows, slot, slots)

    def finish_head(self, head, slot, slots):
        columns = pl.ds(head * KEY, KEY)
        decay = self.log_decay(head)

        def rows(first):
            lines = pl.ds(first, 128)
            cross = jnp.dot(
                self.queries[lines, columns],
                self.state[pl.ds(head * KEY, KEY)],
                preferred_element_type=jnp.float32,
            )
            leading = jnp.exp(decay * (self.position(first, 128) + 1.0))
            raw = self.within[head, lines] + cross * leading
            average = jnp.mean(raw, axis=-1, keepdims=True)
            centred = raw - average
            wide = jnp.mean(jnp.square(centred), axis=-1, keepdims=True)
            switch = self.products[7 + head, lines].astype(jnp.float32)
            result = centred * lax.rsqrt(wide + group_eps) * jax.nn.silu(switch)
            self.hidden[lines, pl.ds(head * VAL, VAL)] = result.astype(self.hidden.dtype)

        self.by_rows(rows, slot, slots)


    def glu(self, slot=0, slots=1):
        lead = self.halo_in.shape[0]

        def rows(first):
            lines = pl.ds(first, 128)
            value = self.products[4, lines].astype(jnp.float32)
            switch = self.products[5, lines].astype(jnp.float32)
            gated = (value * jax.nn.sigmoid(switch)).astype(jnp.bfloat16)
            self.padded[pl.ds(pl.multiple_of(first + lead, 8), 128)] = gated.astype(jnp.float32)

        self.by_rows(rows, slot, slots)
        self.halo_out[...] = self.padded[pl.ds(self.count, lead)].astype(jnp.bfloat16)
        self.padded[pl.ds(self.count + lead, 8)] = jnp.zeros(
            (8, self.padded.shape[1]), jnp.float32
        )
        pl.when(self.link < self.links - 1)(lambda: self.halo_copy().start())

    def halo_copy(self):
        following = jnp.minimum(self.link + 1, self.links - 1)
        return remote(
            self.halo_out,
            self.halo_in,
            self.halo_sems.at[0],
            self.halo_sems.at[1],
            self.chain(following),
        )

    def halo(self):
        lead = self.halo_in.shape[0]
        channels = self.padded.shape[1]

        @pl.when(self.link > 0)
        def _():
            self.halo_copy().wait_recv()
            self.padded[pl.ds(0, lead)] = self.halo_in[...].astype(jnp.float32)

        @pl.when(self.link == 0)
        def _():
            self.padded[pl.ds(0, lead)] = jnp.zeros((lead, channels), jnp.float32)

    def convolve(self, slot, slots):
        lead = self.halo_in.shape[0]
        channels = self.padded.shape[1]
        size = 64
        lanes = 128

        def rows(first):
            for part in range(channels // lanes):
                columns = pl.ds(part * lanes, lanes)
                spot = pl.multiple_of(self.rank * channels + part * lanes, lanes)
                weights = self.taps[:, pl.ds(spot, lanes)]
                source = self.padded[pl.ds(first, size + lead + 8), columns]
                total = None
                for low in range(8):
                    group = None
                    for high in range(lead // 8 + 1):
                        tap = high * 8 + low - (lead - KW + 1)
                        if not 0 <= tap < KW:
                            continue
                        term = source[high * 8 : high * 8 + size + 8] * weights[tap : tap + 1]
                        group = term if group is None else group + term
                    if low:
                        group = pltpu.roll(group, size + 8 - low, 0)
                    total = group[:size] if total is None else total + group[:size]
                self.summed[pl.ds(first, size), columns] = total

        self.by_rows(rows, slot, slots, size)

    def finish_convolution(self, slot, slots):
        channels = self.padded.shape[1]
        spot = pl.ds(pl.multiple_of(self.rank * channels, channels), channels)
        gain, shift = self.gain[:, spot], self.shift[:, spot]

        def rows(first):
            lines = pl.ds(first, 128)
            total = self.summed[lines]
            average = jnp.mean(total, axis=-1, keepdims=True)
            centred = total - average
            wide = jnp.mean(jnp.square(centred), axis=-1, keepdims=True)
            normalized = centred * lax.rsqrt(wide + layer_eps) * gain + shift
            switch = self.products[6, lines].astype(jnp.float32)
            result = jax.nn.silu(normalized) * jax.nn.silu(switch)
            target = pl.ds(self.heads * VAL, channels)
            self.hidden[lines, target] = result.astype(self.hidden.dtype)

        self.by_rows(rows, slot, slots)


    def x_copy(self, n):
        zh, zl, y, x, c = self.at
        return remote(
            self.sent.at[n],
            self.crossed.at[n],
            self.out_sems.at[0, n],
            self.out_sems.at[1, n],
            (zh, zl, y, 1 - x, c),
        )

    def near_copy(self, n):
        zh, zl, y, x, c = self.at
        share = self.out.shape[0]
        part = self.half.at[n, pl.ds(pl.multiple_of((1 - c) * share, share), share)]
        return remote(
            part,
            self.here.at[n],
            self.out_sems.at[2, n],
            self.out_sems.at[3, n],
            (zh, zl, y, x, 1 - c),
        )

    def far_copy(self, n, core):
        zh, zl, y, x, c = self.at
        share = self.out.shape[0]
        return remote(
            self.half.at[n, pl.ds(core * share, share)],
            self.there.at[n],
            self.out_sems.at[2 + 2 * core, n],
            self.out_sems.at[5, n],
            (c, zl, y, x, core),
        )

    def multiply(self, j, q, weights):
        x = self.at[3]
        tile = self.sent.shape[2]
        n = j * 4 + q
        pair = self.sent.shape[1]
        lines = pl.ds(pl.multiple_of(q * tile, tile), tile)
        total = contract(self.hidden[...], weights[j, lines])
        low, high = total[:pair], total[pair:]
        self.kept[n] = jnp.where(x == 0, low, high)
        self.sent[n] = jnp.where(x == 0, high, low).astype(self.sent.dtype)
        self.x_copy(n).start()

    def join(self, n):
        zh, zl, y, x, c = self.at
        self.x_copy(n).wait_recv()
        total = self.kept[n] + self.crossed[n].astype(jnp.float32)
        self.half[n] = total.astype(self.half.dtype)

        @pl.when(c == zh)
        def _():
            self.near_copy(n).start()

        @pl.when(c != zh)
        def _():
            self.far_copy(n, 0).start()
            self.far_copy(n, 1).start()

    def close(self, j, q):
        zh, zl, y, x, c = self.at
        n = j * 4 + q
        share = self.out.shape[0]
        wide = self.sent.shape[2] // 2
        part = self.there.at[n]
        remote(
            part, part, self.out_sems.at[4, n], self.out_sems.at[5, n], (zh, zl, y, 1 - x, c)
        ).wait_recv()
        far_part = self.there[n].astype(jnp.float32)

        def store(near_part):
            total = (near_part.astype(jnp.float32) + far_part).astype(self.out.dtype)
            for k in range(2):
                spot = ((2 * q + k) * 2 + j) * wide
                self.out[:, pl.ds(spot, wide)] = total[:, k * wide : (k + 1) * wide]

        @pl.when(c == zh)
        def _():
            store(self.half[n, pl.ds(pl.multiple_of(c * share, share), share)])

        @pl.when(c != zh)
        def _():
            self.near_copy(n).wait_recv()
            store(self.here[n])

    def drain(self):
        zh, zl, y, x, c = self.at
        self.drain_rows()
        self.others(lambda s: self.slice_copy(s).wait_send())
        self.others(lambda s: self.prefix_copy(s).wait_send())
        pl.when(self.link < self.links - 1)(lambda: self.halo_copy().wait_send())
        for n in range(self.sent.shape[0]):
            self.x_copy(n).wait_send()

            @pl.when(c == zh)
            def _():
                self.near_copy(n).wait_send()

            @pl.when(c != zh)
            def _():
                self.far_copy(n, 0).wait_send()
                self.far_copy(n, 1).wait_send()


def layer_kernel(layout, out_layout, *refs):
    blocks, refs = refs[:9], refs[9:]
    first_gather, refs = refs[-12:-6], refs[:-12] + refs[-6:]
    second_gather, refs = refs[-6:], refs[:-6]
    layer = Layer(refs)
    inward, outward = Gather(*first_gather), Gather(*second_gather)
    units = len(layout)
    total = units + 2

    met = meet()
    for k, (which, first) in enumerate(layout):
        inward.load(k, blocks[which].at[:, pl.ds(first, inward.source.shape[2])], None)
    for k, parts in enumerate(out_layout):
        for which, row, column in parts:
            ref = blocks[which]
            lines = pl.ds(row, outward.depth)
            outward.load(k, ref.at[lines], pl.ds(column, ref.shape[1]))

    def at_unit(k, what):
        @pl.when(jnp.logical_and(k >= 0, k < units))
        def _():
            what(inward, k)

        @pl.when(jnp.logical_and(k >= units, k < total))
        def _():
            what(outward, k - units)

    for n in range(3):
        layer.load(n).start()
    met()

    def first_sends(own, ahead):
        for k in range(ahead):
            if k < units:
                inward.begin(k, own)
            else:
                outward.begin(k - units, own)

    pl.when(inward.is_own)(lambda: first_sends(True, OWN_AHEAD))
    pl.when(jnp.logical_not(inward.is_own))(lambda: first_sends(False, FAR_AHEAD))
    layer.near_rows()
    layer.far_strip(0).start()

    def next_sends(i):
        @pl.when(inward.is_own)
        def _():
            at_unit(i + OWN_AHEAD, lambda gather, k: gather.begin(k, True))

        @pl.when(jnp.logical_not(inward.is_own))
        def _():
            at_unit(i + FAR_AHEAD, lambda gather, k: gather.begin(k, False))

    inside, finish_head = layer.inside, layer.finish_head
    key_scale = KEY ** (-0.5)
    after = (
        (lambda n: layer.rotate(0, layer.keys, key_scale, n, 2),) * 2,
        (lambda n: layer.contribute(0), None),
        (lambda n: (layer.contribute(1), layer.send_slices()), None),
        (lambda n: layer.rotate(3, layer.queries, 1.0, n, 2),) * 2,
        (lambda n: inside(0, 0, 1), None),
        (lambda n: layer.glu(), lambda n: inside(1, 0, 1)),
        (lambda n: layer.scan(), lambda n: (layer.halo(), layer.convolve(0, 1))),
        (lambda n: layer.finish_convolution(0, 1), None),
        (
            lambda n: layer.state_arrived(),
            lambda n: (finish_head(0, 0, 1), finish_head(1, 0, 1)),
        ),
    )

    def compute(k, carry):
        inward.complete_own(k)
        inward.complete_far(k)
        layer.project(k, inward.full, 0, 2)
        layer.project(k, inward.full, 1, 2)
        for unit, events in enumerate(after):

            @pl.when(k == unit)
            def _():
                for n, event in enumerate(events):
                    if event is not None:
                        event(n)

        return carry

    def relay(k, number):
        at_unit(k, lambda gather, k: gather.stage(k, number))

    for number in (0, 1, 4):
        for k in range(LEADS[number]):
            relay(k, number)

    layer.tables()

    def ready(i):
        return jnp.clip(2 * (i - START), 0, jnp.clip(i + 1 - BEHIND, 0, units))

    def step(i, carry):
        relay(i + LEADS[0], 0)
        relay(i + LEADS[1], 1)
        pl.when(jnp.logical_and(i >= 0, i < STRIPS - 1))(lambda: layer.far_strip(i + 1).start())
        next_sends(i)

        @pl.when(jnp.logical_and(i >= ROWS_RELAY, i < ROWS_RELAY + STRIPS))
        def _():
            layer.relay_rows(i - ROWS_RELAY)

        relay(i, 2)
        relay(i + LEADS[4], 4)
        relay(i - 1, 3)
        pl.when(i == START + 1)(layer.all_rows)
        lax.fori_loop(ready(i - 1), ready(i), compute, 0)
        return carry

    lax.fori_loop(0, units + 1, step, 0)
    lax.fori_loop(ready(units), units, compute, 0)

    zh = layer.at[0]

    def tiles(j, half, what):
        for m in range(2):
            what(j, half * 2 + m)

    def multiply(j, q):
        layer.multiply(j, q, outward.full)

    def join(j, q):
        layer.join(j * 4 + q)

    for k in range(units + 1 + LEADS[4], total):
        relay(k, 4)
    outward.complete_own(0)
    tiles(0, zh, multiply)
    relay(units, 3)
    outward.complete_own(1)
    tiles(1, zh, multiply)
    relay(units + 1, 2)
    outward.complete_far(0)
    tiles(0, 1 - zh, multiply)
    tiles(0, zh, join)
    tiles(1, zh, join)
    relay(units + 1, 3)
    outward.complete_far(1)
    tiles(1, 1 - zh, multiply)
    tiles(0, 1 - zh, join)
    tiles(1, 1 - zh, join)
    for j in range(2):
        for q in range(4):
            layer.close(j, q)

    def finish(gather):
        def body(k, carry):
            gather.drain(k)
            return carry

        lax.fori_loop(0, gather.source.shape[0], body, 0)

    finish(inward)
    finish(outward)
    layer.drain()


def whole_layer(tokens, norm_gain, taps, gain, shift, blocks):
    depth, width = blocks[0].shape
    share, model = tokens.shape
    layout = []
    for which, block in enumerate(blocks[:7]):
        layout += [(which, first) for first in range(0, block.shape[1], width)]
    units = len(layout)
    shares, dtype = 8, tokens.dtype
    span = 4 * share
    wide = KEY // 2
    frequency = rope_base ** (-np.arange(wide) / wide)
    angles = [np.arange(span)[:, None] * frequency]
    angles += [span * np.arange(shares)[:, None] * frequency]
    angles, turns = (np.stack([np.cos(a), np.sin(a)]).astype(np.float32) for a in angles)
    inner_width = blocks[7].shape[1] + blocks[8].shape[1]
    half_depth = depth // 2
    out_layout = [
        ((7, j * half_depth, 0), (8, j * half_depth, blocks[7].shape[1])) for j in range(2)
    ]
    heads = width // KEY
    channels = blocks[8].shape[1]
    lead = (KW + 7) // 8 * 8
    tile = 2 * half_depth
    tiles = model // tile
    sem = pltpu.SemaphoreType.DMA
    slice_rows = heads * KEY // shares
    return pl.pallas_call(
        lambda *refs: layer_kernel(layout, out_layout, *refs),
        out_shape=jax.ShapeDtypeStruct((share, model), dtype),
        in_specs=[pl.BlockSpec(memory_space=pl.ANY)] * 11
        + [pl.BlockSpec(memory_space=pltpu.VMEM), pl.BlockSpec(memory_space=pl.ANY)]
        + [pl.BlockSpec(memory_space=pltpu.VMEM)] * 3,
        out_specs=pl.BlockSpec(memory_space=pltpu.VMEM),
        scratch_shapes=[
            pltpu.VMEM((share, model), dtype),
            pltpu.VMEM(angles.shape, jnp.float32),
            pltpu.VMEM(taps.shape, jnp.float32),
            pltpu.VMEM((share, model), dtype),
            pltpu.VMEM((span, wide), jnp.float32),
            pltpu.VMEM((span, wide), jnp.float32),
            pltpu.VMEM((span, model), dtype),
            pltpu.VMEM((units, span, width), dtype),
            pltpu.VMEM((span, width), dtype),
            pltpu.VMEM((span, width), dtype),
            pltpu.VMEM((heads, span, VAL), jnp.float32),
            pltpu.VMEM((heads * KEY, VAL), dtype),
            pltpu.VMEM((shares, slice_rows, VAL), dtype),
            pltpu.VMEM((shares, slice_rows, VAL), dtype),
            pltpu.VMEM((heads * KEY, VAL), dtype),
            pltpu.VMEM((span + lead + 8, channels), jnp.float32),
            pltpu.VMEM((lead, channels), dtype),
            pltpu.VMEM((lead, channels), dtype),
            pltpu.VMEM((span, channels), jnp.float32),
            pltpu.VMEM((span, inner_width), dtype),
            pltpu.VMEM((tiles, 2 * share, tile), jnp.float32),
            pltpu.VMEM((tiles, 2 * share, tile), dtype),
            pltpu.VMEM((tiles, 2 * share, tile), dtype),
            pltpu.VMEM((tiles, 2 * share, tile), dtype),
            pltpu.VMEM((tiles, share, tile), dtype),
            pltpu.VMEM((tiles, share, tile), dtype),
            sem((2 + 3 * STRIPS,)),
            sem((4, STRIPS)),
            sem((2, shares)),
            sem((2, shares)),
            sem((2,)),
            sem((6, tiles)),
            sem((3,)),
        ]
        + gather_scratch(units, depth, width, shares, dtype)
        + gather_scratch(2, half_depth, inner_width, shares, dtype),
        compiler_params=pltpu.CompilerParams(
            has_side_effects=True, collective_id=0, vmem_limit_bytes=60 << 20
        ),
        name="layer",
    )(*blocks, tokens, angles, turns, taps, norm_gain, gain, shift)


def local_squares(
    tokens,
    norm_gain,
    query_weight,
    key_weight,
    value_weight,
    retain_gate,
    unit_value,
    unit_gate,
    convolve_gate,
    filter_taps,
    layer_gain,
    layer_shift,
    retain_output,
    convolve_output,
):
    blocks = (key_weight, value_weight, query_weight, unit_value, unit_gate, convolve_gate)
    blocks += (retain_gate, retain_output, convolve_output)
    return whole_layer(
        tokens,
        norm_gain[None],
        filter_taps,
        layer_gain[None],
        layer_shift[None],
        blocks,
    )


def squares(mesh):
    boxes = Mesh(mesh.devices.reshape(2, 2, 2, 2, 2), SQUARE)
    rows, blocks = P(SQUARE, None), P(("zh", "zl", "y"), ("x", "c"))
    return jax.shard_map(
        local_squares,
        mesh=boxes,
        in_specs=(rows, P()) + (blocks,) * 7 + (P(),) * 3 + (blocks,) * 2,
        out_specs=rows,
        check_vma=False,
    )


def solution(mesh):
    sp, tp = mesh.shape["sp"], mesh.shape["tp"]
    if (sp, tp) == (8, 4):
        return squares(mesh)
    planes = Mesh(mesh.devices.reshape(tp, sp // tp, tp), ("hi", "lo", "tp"))
    return jax.shard_map(
        local,
        mesh=planes,
        in_specs=(
            P(("hi", "lo", "tp"), None),
            P(),
            P(("hi", "lo"), "tp"),
            P(("hi", "lo"), "tp"),
            P(("hi", "lo"), "tp"),
            P(("hi", "lo"), "tp"),
            P(("hi", "lo"), "tp"),
            P(("hi", "lo"), "tp"),
            P(("hi", "lo"), "tp"),
            P(),
            P(),
            P(),
            P(("hi", "lo"), "tp"),
            P(("hi", "lo"), "tp"),
        ),
        out_specs=P(("hi", "lo", "tp"), None),
        check_vma=False,
    )
```
